32 devices in a mesh: sp: 16 (over z, y, x), tp: 2 (over core).
Axes of the slice: x: 2, y: 2, z: 4, core: 2. Of those that a mesh axis runs over, the one named last changes fastest.
Arguments:
- hidden: bfloat16 [4096, 2048], P('sp', 'tp'), may hold values from -16 to 16
- query_weight: bfloat16 [2048, 1024], P(None, 'tp'), may hold values from -0.125 to 0.125
- key_weight: bfloat16 [2048, 512], P(None, 'tp'), may hold values from -0.125 to 0.125
- value_weight: bfloat16 [2048, 512], P(None, 'tp'), may hold values from -0.125 to 0.125
- head_gate_weight: bfloat16 [2048, 1024], P(None, 'tp'), may hold values from -0.125 to 0.125
- state_in_weight: bfloat16 [2048, 1024], P(None, 'tp'), may hold values from -0.125 to 0.125
- state_gate_weight: bfloat16 [2048, 1024], P(None, 'tp'), may hold values from -0.125 to 0.125
- sink_logit: float32 [16], P('tp'), may hold values from 1 to 6
- decay_real: float32 [64, 64], P('tp'), may hold values from -0.7 to -0.0049
- decay_frequency: float32 [64, 64], P('tp'), may hold values from 0 to 192
- log_step: float32 [64], P('tp'), may hold values from -20 to 0
- input_real: float32 [64, 64, 16], P('tp'), may hold values from -1028 to 1028
- input_imaginary: float32 [64, 64, 16], P('tp'), may hold values from -1028 to 1028
- output_real: float32 [64, 16, 64], P('tp'), may hold values from -0.5 to 0.5
- output_imaginary: float32 [64, 16, 64], P('tp'), may hold values from -0.5 to 0.5
- skip_weight: float32 [64, 16], P('tp'), may hold values from -3 to 3
- decay_shift: float32 [64, 4096], P('tp', 'sp'), may hold values from -2 to 0
- head_out_weight: bfloat16 [1024, 2048], P('tp'), may hold values from -0.375 to 0.375
- state_out_weight: bfloat16 [1024, 2048], P('tp'), may hold values from -0.375 to 0.375
Outputs:
- layer_out: bfloat16 [4096, 2048], P('sp', 'tp')
The draws below stay inside these ranges and needn't reach their ends.
All inputs are finite; a program needn't handle non-finite values.
Results may differ from the reference program's by a relative error of at most 0.012.
Values may be sent and summed in bfloat16 or wider, within the bound.
A program may use at most 128 MiB of HBM per device.

```python
import math
import jax
import jax.numpy as jnp
from jax import lax

D = 2048
HEAD_DIM = 64
Q_HEADS = 16
KV_HEADS = 8
SSM_GROUPS = 64
GROUP_CH = 16
SSM_STATE = 64
WINDOW = 128
TOK_DEV = 256
TOKENS = 4096
ATT_WIDTH = 1024
KV_WIDTH = 512
SSM_WIDTH = 1024
N_SP = 16


def group_law(key):
    base_key = jax.random.fold_in(key, 101)
    rank_key, slow_key, fast_key, level_key = jax.random.split(base_key, 4)
    fast_count = SSM_GROUPS // 2
    ranks = jax.random.permutation(rank_key, SSM_GROUPS)
    is_fast = ranks < fast_count
    reach = min(100, TOK_DEV // 2)
    slow_log = jax.random.uniform(slow_key, (SSM_GROUPS,), jnp.float32, math.log(7.0 / TOKENS), math.log(30.0 / TOKENS))
    fast_log = jax.random.uniform(fast_key, (SSM_GROUPS,), jnp.float32, math.log(2.0 / reach), math.log(5.0 / reach))
    log_dt = jnp.where(is_fast, fast_log, slow_log)
    level = jax.random.uniform(level_key, (SSM_GROUPS, SSM_STATE), jnp.float32, 0.3, 0.7)
    slow_real = -level * 0.5 / (jnp.exp(slow_log) * TOKENS)[:, None]
    real_part = jnp.where(is_fast[:, None], -level, slow_real)
    return (log_dt, real_part)


def draw_log_step(key, part):
    return group_law(key)[0]


def draw_decay_real(key, part):
    return group_law(key)[1]


def input_draw(key, salt):
    log_dt, real_part = group_law(key)
    draw_key = jax.random.fold_in(key, salt)
    shape = (SSM_GROUPS, SSM_STATE, GROUP_CH)
    raw = jnp.clip(jax.random.normal(draw_key, shape, jnp.float32), -4.0, 4.0)
    scale = (2.0 * GROUP_CH) ** (-0.5) * jnp.sqrt(2.0 * jnp.abs(real_part) / jnp.exp(log_dt)[:, None])
    return raw * scale[:, :, None]


def draw_input_real(key, part):
    return input_draw(key, 202)


def draw_input_imaginary(key, part):
    return input_draw(key, 203)


def draw_decay_shift(key, part):
    rate_key, jitter_key, where_key, amount_key = jax.random.split(jax.random.fold_in(key, 303), 4)
    block_count = TOKENS // TOK_DEV
    block_rate = jnp.exp(jax.random.uniform(rate_key, (block_count,), jnp.float32, math.log(0.2), math.log(0.8))) / TOKENS
    frequency_ratio = jnp.repeat(block_rate, TOK_DEV)
    random_perturbation = jax.random.uniform(jitter_key, (SSM_GROUPS, TOKENS), jnp.float32, 0.5, 1.5)
    places = jax.random.randint(where_key, (SSM_GROUPS, 2), 0, TOKENS)
    total_quantity = jnp.log(jax.random.uniform(amount_key, (SSM_GROUPS, 2), jnp.float32, 0.5, 0.8))
    positions = jnp.arange(TOKENS, dtype=jnp.int32)
    match_count = (places[:, :, None] == positions[None, None, :]).astype(jnp.float32)
    spike_length = jnp.sum(match_count * total_quantity[:, :, None], axis=1)
    return -frequency_ratio[None, :] * random_perturbation + spike_length


def draw_hidden(key, part):
    noise_key = jax.random.fold_in(jax.random.fold_in(key, 404), 0)
    return jnp.clip(jax.random.normal(noise_key, (TOKENS, D), jnp.float32), -6.0, 6.0).astype(jnp.bfloat16)


def block_scale(rng, dims, shards, least, top_value):
    level, own = 1.0, jax.random.fold_in(rng, 6)
    for position, shards_of in shards:
        draws = jnp.exp(jax.random.uniform(jax.random.fold_in(own, position), (shards_of,), jnp.float32, least / len(shards), top_value / len(shards)))
        level = level * jnp.repeat(draws, dims[position] // shards_of).reshape([-1 if axis == position else 1 for axis in range(len(dims))])
    return level


def gaussian(own_key, shape, width, most, cuts=(), held_as=jnp.bfloat16):
    drawn = jax.random.normal(own_key, shape, jnp.float32) * width
    if len(cuts) > 0:
        drawn = block_scale(own_key, shape, cuts, -0.22, 0.18) * drawn
    return jnp.clip(drawn, min=-most, max=most).astype(held_as)


def setup_inputs(seed: int = 0) -> dict:
    key_of = jax.random.split(jax.random.key(seed), 20)
    return {
        "hidden": draw_hidden(jax.random.fold_in(key_of[19], 71), 0),
        "query_weight": gaussian(key_of[1], (D, ATT_WIDTH), D ** -0.5, 0.125, ((1, 2),)),
        "key_weight": gaussian(key_of[2], (D, KV_WIDTH), D ** -0.5, 0.125, ((1, 2),)),
        "value_weight": gaussian(key_of[3], (D, KV_WIDTH), D ** -0.5, 0.125, ((1, 2),)),
        "head_gate_weight": gaussian(key_of[4], (D, ATT_WIDTH), D ** -0.5, 0.125, ((1, 2),)),
        "state_in_weight": gaussian(key_of[5], (D, SSM_WIDTH), D ** -0.5, 0.125, ((1, 2),)),
        "state_gate_weight": gaussian(key_of[6], (D, SSM_WIDTH), D ** -0.5, 0.125, ((1, 2),)),
        "sink_logit": jnp.clip(1.0 + 5.0 * jax.random.uniform(key_of[7], (Q_HEADS,), jnp.float32) ** block_scale(key_of[7], (Q_HEADS,), ((0, 2),), -0.2, 0.2), 1.0, 6.0),
        "decay_real": draw_decay_real(jax.random.fold_in(key_of[19], 71), 0),
        "decay_frequency": jnp.clip(192.0 * jax.random.uniform(key_of[9], (SSM_GROUPS, SSM_STATE), jnp.float32) ** block_scale(key_of[9], (SSM_GROUPS, SSM_STATE), ((0, 2),), -0.2, 0.2), 0.0, 192.0),
        "log_step": draw_log_step(jax.random.fold_in(key_of[19], 71), 0),
        "input_real": draw_input_real(jax.random.fold_in(key_of[19], 71), 0),
        "input_imaginary": draw_input_imaginary(jax.random.fold_in(key_of[19], 71), 0),
        "output_real": gaussian(key_of[13], (SSM_GROUPS, GROUP_CH, SSM_STATE), (2 * SSM_STATE) ** -0.5, 0.5, ((0, 2),), jnp.float32),
        "output_imaginary": gaussian(key_of[14], (SSM_GROUPS, GROUP_CH, SSM_STATE), (2 * SSM_STATE) ** -0.5, 0.5, ((0, 2),), jnp.float32),
        "skip_weight": gaussian(key_of[15], (SSM_GROUPS, GROUP_CH), 0.5, 3.0, ((0, 2),), jnp.float32),
        "decay_shift": draw_decay_shift(jax.random.fold_in(key_of[19], 71), 0),
        "head_out_weight": gaussian(key_of[17], (ATT_WIDTH, D), (ATT_WIDTH // 4) ** -0.5, 0.375, ((0, 2),)),
        "state_out_weight": gaussian(key_of[18], (SSM_WIDTH, D), (SSM_WIDTH // 4) ** -0.5, 0.375, ((0, 2),)),
    }


NEG_FILL = -1e30


def combine(earlier_pair, later_pair):
    prior_real, prior_imag, prior_sum_real, prior_sum_imag = earlier_pair
    after_real, after_imag, after_sum_real, after_sum_imag = later_pair
    return (prior_real * after_real - prior_imag * after_imag,
            prior_real * after_imag + prior_imag * after_real,
            after_real * prior_sum_real - after_imag * prior_sum_imag + after_sum_real,
            after_real * prior_sum_imag + after_imag * prior_sum_real + after_sum_imag)


def band_rows(rows):
    padded = jnp.concatenate([jnp.zeros_like(rows[:1]), rows], axis=0)
    return jnp.concatenate([padded[:-1], padded[1:]], axis=1)


def attention(query_rows_all, key_rows, value_rows, sink_logit):
    blocks = TOKENS // WINDOW
    group_size = Q_HEADS // KV_HEADS
    query_heads = query_rows_all.reshape(blocks, WINDOW, KV_HEADS, group_size, HEAD_DIM).transpose(2, 0, 1, 3, 4)
    key_heads = band_rows(key_rows.reshape(blocks, WINDOW, KV_HEADS, HEAD_DIM)).transpose(2, 0, 1, 3)
    value_heads = band_rows(value_rows.reshape(blocks, WINDOW, KV_HEADS, HEAD_DIM)).transpose(2, 0, 1, 3)
    sink_table = sink_logit.reshape(KV_HEADS, group_size)
    query_index = jnp.arange(WINDOW, dtype=jnp.int32)[:, None]
    column = jnp.arange(2 * WINDOW, dtype=jnp.int32)[None, :]
    distance = WINDOW + query_index - column
    block_start = (jnp.arange(blocks, dtype=jnp.int32) * WINDOW)[:, None, None]
    allowed = (distance >= 0) & (distance < WINDOW) & (block_start - WINDOW + column >= 0)

    def one_head(operands):
        query_part, key_portion_slice, value_part, sink_part = operands
        scores = jnp.einsum('nqgd,nsd->ngqs', query_part.astype(jnp.float32),
                            key_portion_slice.astype(jnp.float32)) * (HEAD_DIM ** -0.5)
        scores = jnp.where(allowed[:, None], scores, NEG_FILL)
        sink_col = sink_part[None, :, None, None]
        maxima = jnp.maximum(jnp.max(scores, axis=-1, keepdims=True), sink_col)
        exponent = jnp.exp(scores - maxima)
        totals = jnp.sum(exponent, axis=-1, keepdims=True) + jnp.exp(sink_col - maxima)
        weights = (exponent / totals).astype(jnp.bfloat16)
        return jnp.einsum('ngqs,nsd->nqgd', weights.astype(jnp.float32), value_part.astype(jnp.float32))

    outputs = lax.map(one_head, (query_heads, key_heads, value_heads, sink_table))
    return outputs.transpose(1, 2, 0, 3, 4).reshape(TOKENS, ATT_WIDTH)


def state_branch(state_input, decay_real, decay_frequency, log_step, input_real, input_imaginary,
                 output_real, output_imaginary, skip_weight, decay_shift):
    highest = lax.Precision.HIGHEST
    stepsize = jnp.exp(log_step)[:, None]
    magnitude = jnp.exp(decay_real * stepsize)
    base_real = magnitude * jnp.cos(decay_frequency * stepsize)
    base_imag = magnitude * jnp.sin(decay_frequency * stepsize)
    denominator = decay_real * decay_real + decay_frequency * decay_frequency
    less_real = base_real - 1.0
    zoh_real = (less_real * decay_real + base_imag * decay_frequency) / denominator
    zoh_imag = (base_imag * decay_real - less_real * decay_frequency) / denominator
    drive_real = zoh_real[..., None] * input_real - zoh_imag[..., None] * input_imaginary
    drive_imag = zoh_real[..., None] * input_imaginary + zoh_imag[..., None] * input_real
    values = state_input.astype(jnp.float32).reshape(N_SP, TOK_DEV, SSM_GROUPS, GROUP_CH)
    shifts = decay_shift.reshape(SSM_GROUPS, N_SP, TOK_DEV).transpose(1, 0, 2)

    def advance(carried, operands):
        carry_real, carry_imag = carried
        block_rows, shift_rows = operands
        push_real = jnp.einsum('tgp,gnp->gnt', block_rows, drive_real, precision=highest)
        push_imag = jnp.einsum('tgp,gnp->gnt', block_rows, drive_imag, precision=highest)
        factor = jnp.exp(shift_rows)[:, None, :]
        cum_real, cum_imag, local_real, local_imag = lax.associative_scan(
            combine, (factor * base_real[..., None], factor * base_imag[..., None], push_real, push_imag), axis=2)
        state_real = local_real + cum_real * carry_real[..., None] - cum_imag * carry_imag[..., None]
        state_imag = local_imag + cum_real * carry_imag[..., None] + cum_imag * carry_real[..., None]
        recurrent = (jnp.einsum('gpn,gnt->tgp', output_real, state_real, precision=highest)
                     - jnp.einsum('gpn,gnt->tgp', output_imaginary, state_imag, precision=highest)
                     + skip_weight[None] * block_rows)
        return (state_real[..., -1], state_imag[..., -1]), recurrent

    zero_state = jnp.zeros((SSM_GROUPS, SSM_STATE), jnp.float32)
    _, outputs = lax.scan(advance, (zero_state, zero_state), (values, shifts))
    return outputs.reshape(TOKENS, SSM_WIDTH)


def reference(hidden, query_weight, key_weight, value_weight, head_gate_weight, state_in_weight,
              state_gate_weight, sink_logit, decay_real, decay_frequency, log_step, input_real,
              input_imaginary, output_real, output_imaginary, skip_weight, decay_shift,
              head_out_weight, state_out_weight):
    def project(weight):
        return jnp.dot(hidden, weight, preferred_element_type=jnp.float32).astype(jnp.bfloat16)

    query_rows_all = project(query_weight)
    key_rows = project(key_weight)
    value_rows = project(value_weight)
    head_gate = project(head_gate_weight)
    state_input = project(state_in_weight)
    state_gate = project(state_gate_weight)
    attended = attention(query_rows_all, key_rows, value_rows, sink_logit)
    head_mixed = (jax.nn.sigmoid(head_gate.astype(jnp.float32)) * attended).astype(jnp.bfloat16)
    recurrent = state_branch(state_input, decay_real, decay_frequency, log_step, input_real,
                             input_imaginary, output_real, output_imaginary, skip_weight, decay_shift)
    state_mixed = (jax.nn.sigmoid(state_gate.astype(jnp.float32)) * jax.nn.gelu(recurrent)).astype(jnp.bfloat16)
    totals = (jnp.dot(head_mixed, head_out_weight, preferred_element_type=jnp.float32)
              + jnp.dot(state_mixed, state_out_weight, preferred_element_type=jnp.float32))
    return totals.astype(jnp.bfloat16)
```

```python
import jax
import jax.numpy as jnp
import numpy as np
from jax import lax
from jax.experimental import pallas as pl
from jax.experimental.pallas import tpu as pltpu
from jax.sharding import PartitionSpec as P

HEAD_DIM = 64
Q_HEADS = 16
KV_HEADS = 8
GROUP_CH = 16
WINDOW = 128
LANES = 128
SEGS = 8
TILE = 256

NEG_FILL = -1e30
MESH = pl.DeviceIdType.MESH
ANY = pl.BlockSpec(memory_space=pl.ANY)
VMEM = pl.BlockSpec(memory_space=pltpu.VMEM)
SMEM = pl.BlockSpec(memory_space=pltpu.SMEM)
BF16 = jnp.bfloat16
F32 = jnp.float32
NT = (((1,), (1,)), ((), ()))


def split(value, pieces):
    out = []
    for _ in range(pieces):
        high = value.astype(BF16)
        out.append(high)
        value = value - high.astype(F32)
    return out


def ndot(a, b):
    return jnp.dot(a, b, preferred_element_type=F32)


def ntdot(a, b):
    return lax.dot_general(a, b, NT, preferred_element_type=F32)


def cmul(ar, ai, br, bi):
    return ar * br - ai * bi, ar * bi + ai * br


REF, FIN, PRE, ONE, TWO, FOUR, ALL = range(7)


def constants(rows, groups, states):
    length = rows // SEGS
    time = np.arange(rows)
    seg, pos = time // length, time % length
    order = (time % SEGS) * length + time // SEGS
    permute = (order[:, None] == time[None]).astype(np.float32)
    same = seg[order][:, None] == seg[None]
    upto = (order[:, None] >= time[None]).astype(np.float32)
    first = (pos < length // 2).astype(np.float32)[None]
    running = same * (upto - first)
    k = np.arange(SEGS)[:, None]
    here = seg[None] == k
    sums = np.concatenate(
        [
            here * first,
            here * (1 - first),
            seg[None] < k,
            here,
            (seg[None] <= k) & (seg[None] > k - 2),
            (seg[None] <= k) & (seg[None] > k - 4),
            np.ones((SEGS, rows)),
        ],
        axis=0,
    ).astype(np.float32)
    column = np.arange(groups * GROUP_CH) // GROUP_CH
    spread = (np.arange(groups)[:, None] == column[None]).astype(np.float32)
    lane = np.arange(groups * states) // states
    widen = (np.arange(groups)[:, None] == lane[None]).astype(np.float32)
    make = lambda x: jnp.asarray(x, BF16)
    return (
        make(permute), make(permute.T), make(running), make(sums),
        make(np.concatenate([spread, spread], axis=0)), make(np.concatenate([widen] * 3, axis=0)),
    )


def per_pair(row, pairs):
    spots = row.shape[1]
    wide = jnp.broadcast_to(row, (pairs, spots))
    r = lax.broadcasted_iota(jnp.int32, (pairs, spots), 0)
    c = lax.broadcasted_iota(jnp.int32, (pairs, spots), 1)
    even = jnp.sum(jnp.where(c == 2 * r, wide, 0.0), axis=1, keepdims=True)
    odd = jnp.sum(jnp.where(c == 2 * r + 1, wide, 0.0), axis=1, keepdims=True)
    low = lax.broadcasted_iota(jnp.int32, (pairs, LANES), 1) < LANES // 2
    return jnp.where(low, even, odd)


def layer_kernel(
    hidden_ref, wq_ref, wk_ref, wv_ref, wg_ref, wsi_ref, wsg_ref, sink_ref, dr_in, df_in, ls_in, ir_in, ii_in,
    or_in, oi_in, skip_in, shift_in, how_ref, sow_ref, permute_in, back_in, running_in, sums_in, spread_in, widen_in,
    out_ref,
    x, w, how, sow, dr, df, ls, ir, ii, orr, oi, skip, shift, permute, back, running, sums, spread, widen,
    drive, readout, pushed, states_ref, u_ref, gate_ref, win, wout, base, power, table, zoh, entry, init,
    proj, keys, values, mixed, head, near, far, acc_me, acc_other, away, landed,
    in_sem, w_sem, x_send, x_recv, near_send, near_recv, far_send, far_recv, halo_send, halo_recv, out_send, out_recv,
):
    tp = lax.axis_index("tp")
    other = 1 - tp
    me = lax.axis_index("sp")
    count = lax.axis_size("sp")
    inner, outer = near.shape[0], far.shape[0]
    mine, plane = lax.rem(me, inner), lax.div(me, inner)
    rows, half_width = hidden_ref.shape
    pairs = drive.shape[0]
    groups = 2 * pairs
    length = rows // SEGS
    per_tile = LANES // GROUP_CH
    tiles = groups // per_tile
    pairs_tile = per_tile // 2

    local = pltpu.make_async_copy
    own_x = local(hidden_ref, x.at[tp], in_sem.at[0])
    small = [
        local(src, dst, in_sem.at[1 + i])
        for i, (src, dst) in enumerate((
            (dr_in, dr), (df_in, df), (ls_in, ls), (shift_in, shift), (running_in, running), (sums_in, sums),
            (spread_in, spread), (widen_in, widen), (ir_in, ir), (ii_in, ii), (or_in, orr), (oi_in, oi),
            (skip_in, skip), (permute_in, permute), (back_in, back), (how_ref, how), (sow_ref, sow),
        ))
    ]
    columns = []
    for ref in (wsi_ref, wk_ref, wv_ref, wq_ref, wg_ref, wsg_ref):
        for c in range(ref.shape[1] // TILE):
            columns.append(ref.at[:, pl.ds(c * TILE, TILE)])
    weights = [local(src, w.at[i], w_sem.at[i]) for i, src in enumerate(columns)]
    own_x.start()
    for copy in small[:-2]:
        copy.start()
    for copy in weights:
        copy.start()
    for copy in small[-2:]:
        copy.start()

    barrier = pltpu.get_barrier_semaphore()
    pl.semaphore_signal(barrier, inc=1, device_id={"tp": other}, device_id_type=MESH)
    for hop in range(1, inner):
        target = plane * inner + lax.rem(mine + hop, inner)
        pl.semaphore_signal(barrier, inc=1, device_id={"sp": target}, device_id_type=MESH)
    for hop in range(1, outer):
        target = lax.rem(plane + hop, outer) * inner + mine
        pl.semaphore_signal(barrier, inc=1, device_id={"sp": target}, device_id_type=MESH)
    for step in (1, count - 1):
        target = lax.rem(me + step, count)
        pl.semaphore_signal(barrier, inc=1, device_id={"sp": target}, device_id_type=MESH)

    zero = jnp.zeros((LANES, TILE), BF16)
    for q in range(pairs):
        drive[q] = zero
        readout[q] = zero
    for copy in small[:3]:
        copy.wait()
    two = lambda ref: jnp.concatenate(
        [ref[pl.ds(0, pairs, stride=2), :], ref[pl.ds(1, pairs, stride=2), :]], axis=1
    )
    decay, frequency = two(dr), two(df)
    stepsize = jnp.exp(per_pair(ls[...], pairs))
    magnitude = jnp.exp(decay * stepsize)
    rotation = frequency * stepsize
    base_r, base_i = magnitude * jnp.cos(rotation), magnitude * jnp.sin(rotation)
    denominator = decay * decay + frequency * frequency
    less = base_r - 1.0
    zoh[0] = (less * decay + base_i * frequency) / denominator
    zoh[1] = (base_i * decay - less * frequency) / denominator
    base[0], base[1] = base_r, base_i
    power_r, power_i = base_r, base_i
    for _ in range(length.bit_length() - 1):
        power_r, power_i = cmul(power_r, power_i, power_r, power_i)
    for d in range(3):
        base[2 + 2 * d], base[3 + 2 * d] = power_r, power_i
        power_r, power_i = cmul(power_r, power_i, power_r, power_i)
    block_r, block_i = power_r, power_i
    run_r, run_i = jnp.ones_like(base_r), jnp.zeros_like(base_r)
    for k in range(SEGS):
        spot = pl.ds(k, pairs, stride=SEGS)
        power[0, spot, :] = run_r
        power[1, spot, :] = run_i
        run_r, run_i = cmul(run_r, run_i, base[2], base[3])

    for copy in small[3:8]:
        copy.wait()
    shifts = split(shift[...], 3)
    relative = sum(ntdot(running[...], piece) for piece in shifts)
    grown = jnp.concatenate(split(jnp.exp(-relative), 2), axis=1)
    win[...] = ndot(grown, spread[...])
    shrunk = jnp.concatenate(split(jnp.exp(relative), 2), axis=1)
    wout[...] = ndot(shrunk, spread[...])
    totals = sum(ntdot(sums[...], piece) for piece in shifts)
    message_shift = totals[ALL * SEGS : (ALL + 1) * SEGS]
    scales = jnp.concatenate(split(jnp.exp(totals), 3), axis=1)
    table[...] = ndot(scales, widen[...])

    for copy in small[8:12]:
        copy.wait()
    row_low = lax.broadcasted_iota(jnp.int32, (2 * GROUP_CH, LANES), 0) < GROUP_CH
    lane_low = lax.broadcasted_iota(jnp.int32, (2 * GROUP_CH, LANES), 1) < LANES // 2
    own_lane = row_low == lane_low
    for q in range(pairs):
        pick = lambda ref: jnp.concatenate([
            jnp.concatenate([ref[2 * q], ref[2 * q]], axis=1),
            jnp.concatenate([ref[2 * q + 1], ref[2 * q + 1]], axis=1),
        ], axis=0)
        spot = pl.ds((q % pairs_tile) * 2 * GROUP_CH, 2 * GROUP_CH)
        in_r, in_i = pick(ir), pick(ii)
        z_r, z_i = zoh[0, q : q + 1, :], zoh[1, q : q + 1, :]
        d_r, d_i = cmul(z_r, z_i, in_r, in_i)
        drive[q, spot, :] = jnp.concatenate(
            [jnp.where(own_lane, d_r, 0.0), jnp.where(own_lane, d_i, 0.0)], axis=1
        ).astype(BF16)
        readout[q, spot, :] = jnp.concatenate(
            [jnp.where(own_lane, pick(orr), 0.0), jnp.where(own_lane, -pick(oi), 0.0)], axis=1
        ).astype(BF16)

    own_x.wait()
    pl.semaphore_wait(barrier, inner + outer + 1)
    swap = pltpu.make_async_remote_copy(
        src_ref=x.at[tp], dst_ref=x.at[tp], send_sem=x_send, recv_sem=x_recv,
        device_id={"tp": other}, device_id_type=MESH,
    )
    swap.start()
    small[12].wait()
    lanes_of = lax.broadcasted_iota(jnp.int32, (GROUP_CH, groups * GROUP_CH), 1) % GROUP_CH
    channel = lax.broadcasted_iota(jnp.int32, (GROUP_CH, groups * GROUP_CH), 0)
    skips = sum(ndot(piece, spread[:groups, :]) for piece in split(skip[...], 3))
    skip_row = jnp.sum(jnp.where(lanes_of == channel, skips, 0.0), axis=0, keepdims=True)
    small[13].wait()
    small[14].wait()
    swap.wait()

    def project(n):
        weights[n].wait()
        return (ndot(x[0], w[n, :half_width, :]) + ndot(x[1], w[n, half_width:, :])).astype(BF16)

    SI, KEY, VALUE = 0, 2, 3
    QUERY, GATE, SGATE = 4, 6, 8

    for c in range(2):
        lanes = pl.ds(c * TILE, TILE)
        u = ndot(permute[...], project(SI + c))
        u_ref[:, lanes] = u.astype(BF16)
        weighted = (u * win[:, lanes]).astype(BF16)
        for t in range(TILE // LANES):
            tile = c * (TILE // LANES) + t
            part = weighted[:, t * LANES : (t + 1) * LANES]
            for i in range(pairs_tile):
                q = tile * pairs_tile + i
                pushed[q] = ndot(part, drive[q])

    bunch = 8

    def wide(ref, index, q):
        return jnp.broadcast_to(ref[index, q : q + 1, :], (SEGS, LANES))

    def scan(first, start, keep):
        br = [wide(base, 0, first + i) for i in range(bunch)]
        bi = [wide(base, 1, first + i) for i in range(bunch)]

        def steps(jj, carry):
            carry = list(carry)
            kept = [[] for _ in range(2 * bunch)]
            for sub in range(2):
                spot = pl.ds(pl.multiple_of((2 * jj + sub) * SEGS, SEGS), SEGS)
                for i in range(bunch):
                    r, m = carry[2 * i], carry[2 * i + 1]
                    p = pushed[first + i, spot, :]
                    new_r = br[i] * r - bi[i] * m + p[:, :LANES]
                    new_m = br[i] * m + bi[i] * r + p[:, LANES:]
                    carry[2 * i], carry[2 * i + 1] = new_r, new_m
                    kept[2 * i].append(new_r)
                    kept[2 * i + 1].append(new_m)
            if keep:
                spot = pl.ds(pl.multiple_of(jj * 2 * SEGS, 2 * SEGS), 2 * SEGS)
                for i in range(bunch):
                    for part in range(2):
                        value = jnp.concatenate(kept[2 * i + part], axis=0).astype(BF16)
                        states_ref[first + i, spot, pl.ds(part * LANES, LANES)] = value
            return tuple(carry)

        return lax.fori_loop(0, length // 2, steps, tuple(start), unroll=2)

    def row(kind, q):
        return table[kind * SEGS : (kind + 1) * SEGS, q * LANES : (q + 1) * LANES]

    sub = lax.broadcasted_iota(jnp.int32, (SEGS, LANES), 0)
    near_me = near.at[mine]
    near_me[2 * pairs :, :] = jnp.concatenate(
        [message_shift, jnp.zeros((SEGS, LANES - groups), F32)], axis=1
    )
    for first in range(0, pairs, bunch):
        ends = scan(first, [jnp.zeros((SEGS, LANES), F32)] * (2 * bunch), False)
        for i in range(bunch):
            q = first + i
            fin = row(FIN, q)
            h_r, h_i = ends[2 * i] * fin, ends[2 * i + 1] * fin
            for d, kind in enumerate((ONE, TWO, FOUR)):
                hop = 1 << d
                weight = jnp.where(sub >= hop, row(kind, q), 0.0)
                a_r, a_i = cmul(
                    pltpu.roll(h_r, hop, 0), pltpu.roll(h_i, hop, 0),
                    wide(base, 2 + 2 * d, q), wide(base, 3 + 2 * d, q),
                )
                h_r, h_i = h_r + weight * a_r, h_i + weight * a_i
            near_me[q : q + 1, :] = h_r[SEGS - 1 :]
            near_me[pairs + q : pairs + q + 1, :] = h_i[SEGS - 1 :]
            ref = row(REF, q)
            entry[0, q] = jnp.where(sub >= 1, pltpu.roll(h_r, 1, 0), 0.0) * ref
            entry[1, q] = jnp.where(sub >= 1, pltpu.roll(h_i, 1, 0), 0.0) * ref

    own_rows = pl.ds(WINDOW, rows)
    keys[own_rows, :] = project(KEY)

    def to_near(target):
        return pltpu.make_async_remote_copy(
            src_ref=near_me, dst_ref=near_me, send_sem=near_send.at[target], recv_sem=near_recv.at[mine],
            device_id={"sp": plane * inner + target}, device_id_type=MESH,
        )

    def from_near(source):
        return pltpu.make_async_remote_copy(
            src_ref=near_me, dst_ref=near.at[source], send_sem=near_send.at[source], recv_sem=near_recv.at[source],
            device_id={"sp": plane * inner + source}, device_id_type=MESH,
        )

    for hop in range(1, inner):
        to_near(lax.rem(mine + hop, inner)).start()
    values[own_rows, :] = project(VALUE)

    def halos(target):
        return [
            pltpu.make_async_remote_copy(
                src_ref=band.at[pl.ds(rows, WINDOW)], dst_ref=band.at[pl.ds(0, WINDOW)],
                send_sem=halo_send.at[k], recv_sem=halo_recv.at[k],
                device_id={"sp": target}, device_id_type=MESH,
            )
            for k, band in enumerate((keys, values))
        ]

    proj[0] = project(QUERY)

    @pl.when(me < count - 1)
    def _():
        for copy in halos(me + 1):
            copy.start()

    @pl.when(me == 0)
    def _():
        keys[:WINDOW, :] = jnp.zeros((WINDOW, keys.shape[1]), BF16)
        values[:WINDOW, :] = jnp.zeros((WINDOW, values.shape[1]), BF16)

    proj[1] = project(QUERY + 1)
    proj[2] = project(GATE)
    proj[3] = project(GATE + 1)

    blocks = rows // WINDOW
    group_size = Q_HEADS // KV_HEADS
    tile_heads = TILE // HEAD_DIM
    q_index = lax.broadcasted_iota(jnp.int32, (WINDOW, 2 * WINDOW), 0)
    k_index = lax.broadcasted_iota(jnp.int32, (WINDOW, 2 * WINDOW), 1)
    distance = WINDOW + q_index - k_index
    in_window = (distance >= 0) & (distance < WINDOW)

    def attend(block):
        here = pl.ds(block * WINDOW, WINDOW)
        band = pl.ds(block * WINDOW, 2 * WINDOW)
        allowed = in_window
        if block == 0:
            allowed = allowed & (k_index >= jnp.where(me == 0, WINDOW, 0))
        key, value = keys[band, :], values[band, :]
        for tile in range(2):
            query = proj[tile, here, :] * jnp.asarray(HEAD_DIM ** -0.5, BF16)
            results = []
            for j in range(tile_heads):
                head_id = tile * tile_heads + j
                kv = head_id // group_size
                k = key[:, kv * HEAD_DIM : (kv + 1) * HEAD_DIM]
                v = value[:, kv * HEAD_DIM : (kv + 1) * HEAD_DIM]
                scores = ntdot(query[:, j * HEAD_DIM : (j + 1) * HEAD_DIM], k)
                scores = jnp.where(allowed, scores, NEG_FILL)
                sink = sink_ref[head_id]
                maxima = jnp.maximum(jnp.max(scores, axis=-1, keepdims=True), sink)
                exponent = jnp.exp(scores - maxima)
                total = jnp.sum(exponent, axis=-1, keepdims=True) + jnp.exp(sink - maxima)
                results.append(ndot(exponent.astype(BF16), v) * (1.0 / total))
            gate = jax.nn.sigmoid(proj[2 + tile, here, :].astype(F32))
            head[here, pl.ds(tile * TILE, TILE)] = (gate * jnp.concatenate(results, axis=1)).astype(BF16)

    for block in range(1, blocks):
        attend(block)

    bd = lambda k: (base[k], base[k + 1])
    for hop in range(1, inner):
        from_near(lax.rem(mine + hop, inner)).wait_recv()
    agg_r = agg_i = jnp.zeros((pairs, LANES), F32)
    agg_s = jnp.zeros((1, LANES), F32)
    pw_r, pw_i = jnp.ones((pairs, LANES), F32), jnp.zeros((pairs, LANES), F32)
    pre = [agg_r, agg_i, agg_s, pw_r, pw_i]
    for i in range(inner):
        now = [agg_r, agg_i, agg_s, pw_r, pw_i]
        if i > 0:
            pre = [jnp.where(mine == i, a, b) for a, b in zip(now, pre)]
        shift_i = near[i, 2 * pairs : 2 * pairs + 1, :]
        a_r, a_i = cmul(agg_r, agg_i, block_r, block_i)
        factor = jnp.exp(per_pair(shift_i, pairs))
        agg_r = factor * a_r + near[i, :pairs, :]
        agg_i = factor * a_i + near[i, pairs : 2 * pairs, :]
        agg_s = agg_s + shift_i
        pw_r, pw_i = cmul(pw_r, pw_i, block_r, block_i)
    plane_r, plane_i = pw_r, pw_i
    far_me = far.at[plane]
    far_me[:pairs, :] = agg_r
    far_me[pairs : 2 * pairs, :] = agg_i
    far_me[2 * pairs :, :] = jnp.broadcast_to(agg_s, (SEGS, LANES))

    def to_far(target):
        return pltpu.make_async_remote_copy(
            src_ref=far_me, dst_ref=far_me, send_sem=far_send.at[target], recv_sem=far_recv.at[plane],
            device_id={"sp": target * inner + mine}, device_id_type=MESH,
        )

    def from_far(source):
        return pltpu.make_async_remote_copy(
            src_ref=far_me, dst_ref=far.at[source], send_sem=far_send.at[source], recv_sem=far_recv.at[source],
            device_id={"sp": source * inner + mine}, device_id_type=MESH,
        )

    before = jnp.exp(per_pair(pre[2], pairs))
    before_r, before_i = before * pre[3], before * pre[4]
    for q in range(pairs):
        spot = pl.ds(q * SEGS, SEGS)
        scale = row(PRE, q) * row(REF, q)
        init[0, q] = power[0, spot, :] * scale
        init[1, q] = power[1, spot, :] * scale

    for target in range(1, outer):
        @pl.when(plane < target)
        def _():
            to_far(target).start()

    for c in range(2):
        gate = project(SGATE + c)
        gate_ref[:, c * TILE : (c + 1) * TILE] = ndot(permute[...], gate).astype(BF16)

    @pl.when(me > 0)
    def _():
        for copy in halos(me):
            copy.wait_recv()

    attend(0)
    small[15].wait()
    width = how.shape[1] // 2
    pieces = away.shape[0]
    step = width // pieces

    def part_of(owner, piece):
        return pl.ds(pl.multiple_of(owner * width + piece * step, LANES), step)

    for piece in range(pieces):
        acc_other[piece] = ndot(head[...], how[:, part_of(other, piece)])
        acc_me[piece] = ndot(head[...], how[:, part_of(tp, piece)])

    carry_r = carry_i = jnp.zeros((pairs, LANES), F32)
    for z in range(outer - 1):
        @pl.when(z < plane)
        def _():
            from_far(z).wait_recv()

    for z in range(outer - 1):
        factor = jnp.exp(per_pair(far[z, 2 * pairs : 2 * pairs + 1, :], pairs))
        a_r, a_i = cmul(carry_r, carry_i, plane_r, plane_i)
        carry_r = jnp.where(z < plane, factor * a_r + far[z, :pairs, :], carry_r)
        carry_i = jnp.where(z < plane, factor * a_i + far[z, pairs : 2 * pairs, :], carry_i)
    in_r, in_i = cmul(carry_r, carry_i, before_r, before_i)
    in_r, in_i = in_r + pre[0], in_i + pre[1]
    zoh[0], zoh[1] = in_r, in_i
    for first in range(0, pairs, bunch):
        start = []
        for i in range(bunch):
            q = first + i
            s_r, s_i = cmul(init[0, q], init[1, q], wide(zoh, 0, q), wide(zoh, 1, q))
            start += [entry[0, q] + s_r, entry[1, q] + s_i]
        scan(first, start, True)
    for tile in range(tiles):
        lanes = pl.ds(tile * LANES, LANES)
        seen = sum(
            ntdot(states_ref[q], readout[q]) for q in range(tile * pairs_tile, (tile + 1) * pairs_tile)
        )
        recurrent = wout[:, lanes] * seen + skip_row[:, tile * LANES : (tile + 1) * LANES] * u_ref[:, lanes].astype(F32)
        gate = jax.nn.sigmoid(gate_ref[:, lanes].astype(F32))
        mixed[:, lanes] = (gate * jax.nn.gelu(recurrent)).astype(BF16)
    state = ndot(back[...], mixed[...]).astype(BF16)
    small[16].wait()

    copies = [
        pltpu.make_async_remote_copy(
            src_ref=away.at[piece], dst_ref=landed.at[piece],
            send_sem=out_send.at[piece], recv_sem=out_recv.at[piece],
            device_id={"tp": other}, device_id_type=MESH,
        )
        for piece in range(pieces)
    ]
    for piece in range(pieces):
        away[piece] = (acc_other[piece] + ndot(state, sow[:, part_of(other, piece)])).astype(BF16)
        if piece > 0:
            copies[piece - 1].start()
    held = acc_me[0] + ndot(state, sow[:, part_of(tp, 0)])
    copies[pieces - 1].start()
    for piece in range(pieces):
        total = held if piece == 0 else acc_me[piece] + ndot(state, sow[:, part_of(tp, piece)])
        copies[piece].wait()
        out_ref[:, pl.ds(piece * step, step)] = (total + landed[piece].astype(F32)).astype(BF16)

    for hop in range(1, inner):
        to_near(lax.rem(mine + hop, inner)).wait_send()
    for target in range(1, outer):
        @pl.when(plane < target)
        def _():
            to_far(target).wait_send()

    @pl.when(me < count - 1)
    def _():
        for copy in halos(me + 1):
            copy.wait_send()


def on_device(
    hidden, query_weight, key_weight, value_weight, head_gate_weight, state_in_weight, state_gate_weight,
    sink_logit, decay_real, decay_frequency, log_step, input_real, input_imaginary, output_real,
    output_imaginary, skip_weight, decay_shift, head_out_weight, state_out_weight,
):
    rows, half = hidden.shape
    groups, states = decay_real.shape
    pairs = groups // 2
    channels = groups * GROUP_CH
    count = lax.axis_size("sp")
    inner = 1 << (count.bit_length() // 2)
    outer = count // inner
    fixed = constants(rows, groups, states)
    tiles = sum(
        v.shape[1] for v in (
            query_weight, key_weight, value_weight, head_gate_weight, state_in_weight, state_gate_weight,
        )
    ) // TILE
    width = head_out_weight.shape[1] // 2
    pieces = 4
    small = (
        decay_real, decay_frequency, log_step.reshape(1, groups), input_real.transpose(0, 2, 1),
        input_imaginary.transpose(0, 2, 1), output_real, output_imaginary, skip_weight.T, decay_shift,
    )
    like = lambda v: pltpu.VMEM(v.shape, v.dtype)
    dma = pltpu.SemaphoreType.DMA
    scratch = [
        pltpu.VMEM((2, rows, half), BF16),
        pltpu.VMEM((tiles, 2 * half, TILE), BF16),
        like(head_out_weight), like(state_out_weight),
        *[like(v) for v in small],
        *[like(v) for v in fixed],
        pltpu.VMEM((pairs, LANES, TILE), BF16),
        pltpu.VMEM((pairs, LANES, TILE), BF16),
        pltpu.VMEM((pairs, rows, TILE), F32),
        pltpu.VMEM((pairs, rows, TILE), BF16),
        pltpu.VMEM((rows, channels), BF16),
        pltpu.VMEM((rows, channels), BF16),
        pltpu.VMEM((rows, channels), F32),
        pltpu.VMEM((rows, channels), F32),
        pltpu.VMEM((8, pairs, LANES), F32),
        pltpu.VMEM((2, pairs * SEGS, LANES), F32),
        pltpu.VMEM((7 * SEGS, groups * states), F32),
        pltpu.VMEM((2, pairs, LANES), F32),
        pltpu.VMEM((2, pairs, SEGS, LANES), F32),
        pltpu.VMEM((2, pairs, SEGS, LANES), F32),
        pltpu.VMEM((4, rows, TILE), BF16),
        pltpu.VMEM((WINDOW + rows, TILE), BF16),
        pltpu.VMEM((WINDOW + rows, TILE), BF16),
        pltpu.VMEM((rows, channels), BF16),
        pltpu.VMEM((rows, channels), BF16),
        pltpu.VMEM((inner, 2 * pairs + SEGS, LANES), F32),
        pltpu.VMEM((outer, 2 * pairs + SEGS, LANES), F32),
        pltpu.VMEM((pieces, rows, width // pieces), F32),
        pltpu.VMEM((pieces, rows, width // pieces), F32),
        pltpu.VMEM((pieces, rows, width // pieces), BF16),
        pltpu.VMEM((pieces, rows, width // pieces), BF16),
        dma((18,)), dma((tiles,)), dma, dma, dma((inner,)), dma((inner,)), dma((outer,)), dma((outer,)),
        dma((2,)), dma((2,)), dma((pieces,)), dma((pieces,)),
    ]
    return pl.pallas_call(
        layer_kernel,
        out_shape=jax.ShapeDtypeStruct((rows, width), BF16),
        in_specs=[ANY] * 7 + [SMEM] + [ANY] * (len(small) + 2 + len(fixed)),
        out_specs=VMEM,
        scratch_shapes=scratch,
        compiler_params=pltpu.CompilerParams(
            vmem_limit_bytes=60 * 1024 * 1024, collective_id=0, has_side_effects=True
        ),
        name="layer",
    )(
        hidden, query_weight, key_weight, value_weight, head_gate_weight, state_in_weight, state_gate_weight,
        sink_logit, *small, head_out_weight, state_out_weight, *fixed,
    )


def solution(mesh):
    in_specs = (
        P("sp", "tp"),
        P(None, "tp"),
        P(None, "tp"),
        P(None, "tp"),
        P(None, "tp"),
        P(None, "tp"),
        P(None, "tp"),
        P("tp"),
        P("tp", None),
        P("tp", None),
        P("tp"),
        P("tp", None, None),
        P("tp", None, None),
        P("tp", None, None),
        P("tp", None, None),
        P("tp", None),
        P("tp", "sp"),
        P("tp", None),
        P("tp", None),
    )
    out_specs = P("sp", "tp")
    return jax.shard_map(
        on_device, mesh=mesh, in_specs=in_specs, out_specs=out_specs, check_vma=False
    )
```

```python
import jax
import jax.numpy as jnp
import numpy as np
from jax import lax
from jax.experimental import pallas as pl
from jax.experimental.pallas import tpu as pltpu
from jax.sharding import PartitionSpec as P

HEAD_DIM = 64
Q_HEADS = 16
KV_HEADS = 8
GROUP_CH = 16
WINDOW = 128
LANES = 128
SEGS = 8
TILE = 256

PREP_MIB, LAYER_MIB, ADD_MIB = 12, 36, 4

NEG_FILL = -1e30
MESH = pl.DeviceIdType.MESH
ANY = pl.BlockSpec(memory_space=pl.ANY)
VMEM = pl.BlockSpec(memory_space=pltpu.VMEM)
SMEM = pl.BlockSpec(memory_space=pltpu.SMEM)
BF16 = jnp.bfloat16
F32 = jnp.float32
NT = (((1,), (1,)), ((), ()))


def split(value, pieces):
    out = []
    for _ in range(pieces):
        high = value.astype(BF16)
        out.append(high)
        value = value - high.astype(F32)
    return out


def ndot(a, b):
    return jnp.dot(a, b, preferred_element_type=F32)


def ntdot(a, b):
    return lax.dot_general(a, b, NT, preferred_element_type=F32)


def cmul(ar, ai, br, bi):
    return ar * br - ai * bi, ar * bi + ai * br


REF, FIN, PRE, ONE, TWO, FOUR, ALL = range(7)


def constants(rows, groups, states):
    length = rows // SEGS
    time = np.arange(rows)
    seg, pos = time // length, time % length
    order = (time % SEGS) * length + time // SEGS
    permute = (order[:, None] == time[None]).astype(np.float32)
    same = seg[order][:, None] == seg[None]
    upto = (order[:, None] >= time[None]).astype(np.float32)
    first = (pos < length // 2).astype(np.float32)[None]
    running = same * (upto - first)
    k = np.arange(SEGS)[:, None]
    here = seg[None] == k
    sums = np.concatenate(
        [
            here * first,
            here * (1 - first),
            seg[None] < k,
            here,
            (seg[None] <= k) & (seg[None] > k - 2),
            (seg[None] <= k) & (seg[None] > k - 4),
            np.ones((SEGS, rows)),
        ],
        axis=0,
    ).astype(np.float32)
    column = np.arange(groups * GROUP_CH) // GROUP_CH
    spread = (np.arange(groups)[:, None] == column[None]).astype(np.float32)
    lane = np.arange(groups * states) // states
    widen = (np.arange(groups)[:, None] == lane[None]).astype(np.float32)
    make = lambda x: jnp.asarray(x, BF16)
    return (
        make(permute), make(permute.T), make(running), make(sums),
        make(np.concatenate([spread, spread], axis=0)), make(np.concatenate([widen] * 3, axis=0)),
    )


def per_pair(row, pairs):
    spots = row.shape[1]
    wide = jnp.broadcast_to(row, (pairs, spots))
    r = lax.broadcasted_iota(jnp.int32, (pairs, spots), 0)
    c = lax.broadcasted_iota(jnp.int32, (pairs, spots), 1)
    even = jnp.sum(jnp.where(c == 2 * r, wide, 0.0), axis=1, keepdims=True)
    odd = jnp.sum(jnp.where(c == 2 * r + 1, wide, 0.0), axis=1, keepdims=True)
    low = lax.broadcasted_iota(jnp.int32, (pairs, LANES), 1) < LANES // 2
    return jnp.where(low, even, odd)


def fetch_all(pairs_of, sems, first=0):
    return [pltpu.make_async_copy(src, dst, sems.at[first + i]) for i, (src, dst) in enumerate(pairs_of)]


def prepare_kernel(
    hidden_ref, wsi_ref, wk_ref, wv_ref, dr_in, df_in, ls_in, shift_in, running_in, sums_in, spread_in, widen_in,
    ir_in, ii_in, or_in, oi_in, skip_in,
    x, w, drive, readout, win, wout, base, power, table, shift_rows, skip_row,
    dr, df, ls, shift, running, sums, spread, widen, ir, ii, orr, oi, skip, zoh,
    in_sem, w_sem, x_send, x_recv,
):
    tp = lax.axis_index("tp")
    other = 1 - tp
    pairs = drive.shape[0]
    groups = 2 * pairs
    rows = win.shape[0]
    length = rows // SEGS
    pairs_tile = LANES // GROUP_CH // 2
    barrier = pltpu.get_barrier_semaphore()
    pl.semaphore_signal(barrier, inc=1, device_id={"tp": other}, device_id_type=MESH)
    own_x = pltpu.make_async_copy(hidden_ref, x.at[tp], in_sem.at[0])
    own_x.start()
    small = fetch_all((
        (dr_in, dr), (df_in, df), (ls_in, ls), (shift_in, shift), (running_in, running), (sums_in, sums),
        (spread_in, spread), (widen_in, widen), (ir_in, ir), (ii_in, ii), (or_in, orr), (oi_in, oi), (skip_in, skip),
    ), in_sem, 1)
    for copy in small:
        copy.start()
    columns = [
        (ref.at[:, pl.ds(c * TILE, TILE)], w.at[i + c])
        for ref, i in ((wsi_ref, 0), (wk_ref, 2), (wv_ref, 3)) for c in range(ref.shape[1] // TILE)
    ]
    weights = fetch_all(columns, w_sem)
    for copy in weights:
        copy.start()
    zero = jnp.zeros((LANES, TILE), BF16)
    for q in range(pairs):
        drive[q] = zero
        readout[q] = zero

    pl.semaphore_wait(barrier, 1)
    own_x.wait()
    swap = pltpu.make_async_remote_copy(
        src_ref=x.at[tp], dst_ref=x.at[tp], send_sem=x_send, recv_sem=x_recv,
        device_id={"tp": other}, device_id_type=MESH,
    )
    swap.start()

    for copy in small:
        copy.wait()
    two = lambda ref: jnp.concatenate(
        [ref[pl.ds(0, pairs, stride=2), :], ref[pl.ds(1, pairs, stride=2), :]], axis=1
    )
    decay, frequency = two(dr), two(df)
    stepsize = jnp.exp(per_pair(ls[...], pairs))
    magnitude = jnp.exp(decay * stepsize)
    rotation = frequency * stepsize
    base_r, base_i = magnitude * jnp.cos(rotation), magnitude * jnp.sin(rotation)
    denominator = decay * decay + frequency * frequency
    less = base_r - 1.0
    zoh[0] = (less * decay + base_i * frequency) / denominator
    zoh[1] = (base_i * decay - less * frequency) / denominator
    base[0], base[1] = base_r, base_i
    power_r, power_i = base_r, base_i
    for _ in range(length.bit_length() - 1):
        power_r, power_i = cmul(power_r, power_i, power_r, power_i)
    for d in range(4):
        base[2 + 2 * d], base[3 + 2 * d] = power_r, power_i
        if d == 0:
            step_r, step_i = power_r, power_i
        power_r, power_i = cmul(power_r, power_i, power_r, power_i)
    run_r, run_i = jnp.ones_like(base_r), jnp.zeros_like(base_r)
    for k in range(SEGS):
        spot = pl.ds(k, pairs, stride=SEGS)
        power[0, spot, :] = run_r
        power[1, spot, :] = run_i
        run_r, run_i = cmul(run_r, run_i, step_r, step_i)

    shifts = split(shift[...], 3)
    relative = sum(ntdot(running[...], piece) for piece in shifts)
    totals = sum(ntdot(sums[...], piece) for piece in shifts)
    grown = jnp.concatenate(split(jnp.exp(-relative), 2), axis=1)
    shrunk = jnp.concatenate(split(jnp.exp(relative), 2), axis=1)
    scales = jnp.concatenate(split(jnp.exp(totals), 3), axis=1)
    win[...] = ndot(grown, spread[...])
    wout[...] = ndot(shrunk, spread[...])
    table[...] = ndot(scales, widen[...])
    shift_rows[...] = jnp.concatenate(
        [totals[ALL * SEGS : (ALL + 1) * SEGS], jnp.zeros((SEGS, LANES - groups), F32)], axis=1
    )
    lanes_of = lax.broadcasted_iota(jnp.int32, (GROUP_CH, groups * GROUP_CH), 1) % GROUP_CH
    channel = lax.broadcasted_iota(jnp.int32, (GROUP_CH, groups * GROUP_CH), 0)
    skips = sum(ndot(piece, spread[:groups, :]) for piece in split(skip[...], 3))
    skip_row[...] = jnp.broadcast_to(
        jnp.sum(jnp.where(lanes_of == channel, skips, 0.0), axis=0, keepdims=True), skip_row.shape
    )

    row_low = lax.broadcasted_iota(jnp.int32, (2 * GROUP_CH, LANES), 0) < GROUP_CH
    lane_low = lax.broadcasted_iota(jnp.int32, (2 * GROUP_CH, LANES), 1) < LANES // 2
    own_lane = row_low == lane_low
    for q in range(pairs):
        pick = lambda ref: jnp.concatenate([
            jnp.concatenate([ref[2 * q], ref[2 * q]], axis=1),
            jnp.concatenate([ref[2 * q + 1], ref[2 * q + 1]], axis=1),
        ], axis=0)
        spot = pl.ds((q % pairs_tile) * 2 * GROUP_CH, 2 * GROUP_CH)
        in_r, in_i = pick(ir), pick(ii)
        z_r, z_i = zoh[0, q : q + 1, :], zoh[1, q : q + 1, :]
        d_r, d_i = cmul(z_r, z_i, in_r, in_i)
        drive[q, spot, :] = jnp.concatenate(
            [jnp.where(own_lane, d_r, 0.0), jnp.where(own_lane, d_i, 0.0)], axis=1
        ).astype(BF16)
        readout[q, spot, :] = jnp.concatenate(
            [jnp.where(own_lane, pick(orr), 0.0), jnp.where(own_lane, -pick(oi), 0.0)], axis=1
        ).astype(BF16)
    swap.wait()
    for copy in weights:
        copy.wait()


def layer_kernel(
    x, w, drive, readout, win, wout, base, power, table, shift_rows, skip_row,
    wq_ref, wg_ref, wsg_ref, sink_in, how_ref, sow_ref, permute_in, back_in,
    total_ref, landed,
    w2, how, sow, permute, back, sink_ref,
    pushed, states_ref, u_ref, gate_ref, carried, entry, init,
    proj, keys, values, mixed, head, near, far, acc_me, acc_other, away,
    in_sem, w_sem, near_send, near_recv, far_send, far_recv, halo_send, halo_recv, out_send, out_recv,
):
    tp = lax.axis_index("tp")
    other = 1 - tp
    me = lax.axis_index("sp")
    count = lax.axis_size("sp")
    inner, outer = near.shape[0], far.shape[0]
    mine, plane = lax.rem(me, inner), lax.div(me, inner)
    rows, half_width = x.shape[1:]
    pairs = drive.shape[0]
    groups = 2 * pairs
    length = rows // SEGS
    per_tile = LANES // GROUP_CH
    tiles = groups // per_tile
    pairs_tile = per_tile // 2

    barrier = pltpu.get_barrier_semaphore()
    for hop in range(1, inner):
        target = plane * inner + lax.rem(mine + hop, inner)
        pl.semaphore_signal(barrier, inc=1, device_id={"sp": target}, device_id_type=MESH)
    for hop in range(1, outer):
        target = lax.rem(plane + hop, outer) * inner + mine
        pl.semaphore_signal(barrier, inc=1, device_id={"sp": target}, device_id_type=MESH)
    for step in (1, count - 1):
        target = lax.rem(me + step, count)
        pl.semaphore_signal(barrier, inc=1, device_id={"sp": target}, device_id_type=MESH)
    pl.semaphore_signal(barrier, inc=1, device_id={"tp": other}, device_id_type=MESH)

    small = fetch_all(((permute_in, permute), (back_in, back), (sink_in, sink_ref), (how_ref, how), (sow_ref, sow)), in_sem)
    columns = [
        (ref.at[:, pl.ds(c * TILE, TILE)], w2.at[2 * i + c])
        for i, ref in enumerate((wq_ref, wg_ref, wsg_ref)) for c in range(2)
    ]
    weights = fetch_all(columns, w_sem)
    for copy in small[:3] + weights + small[3:]:
        copy.start()

    def project(block):
        return (ndot(x[0], block[:half_width, :]) + ndot(x[1], block[half_width:, :])).astype(BF16)

    small[0].wait()
    small[1].wait()
    own_rows = pl.ds(WINDOW, rows)
    fed = [project(w[c]) for c in range(2)]
    keys[own_rows, :] = project(w[2])
    values[own_rows, :] = project(w[3])
    for c in range(2):
        lanes = pl.ds(c * TILE, TILE)
        u = ndot(permute[...], fed[c])
        u_ref[:, lanes] = u.astype(BF16)
        weighted = (u * win[:, lanes]).astype(BF16)
        for t in range(TILE // LANES):
            tile = c * (TILE // LANES) + t
            part = weighted[:, t * LANES : (t + 1) * LANES]
            for i in range(pairs_tile):
                q = tile * pairs_tile + i
                pushed[q] = ndot(part, drive[q])

    pl.semaphore_wait(barrier, inner + outer + 1)

    def halos(target):
        return [
            pltpu.make_async_remote_copy(
                src_ref=band.at[pl.ds(rows, WINDOW)], dst_ref=band.at[pl.ds(0, WINDOW)],
                send_sem=halo_send.at[k], recv_sem=halo_recv.at[k],
                device_id={"sp": target}, device_id_type=MESH,
            )
            for k, band in enumerate((keys, values))
        ]

    @pl.when(me < count - 1)
    def _():
        for copy in halos(me + 1):
            copy.start()

    @pl.when(me == 0)
    def _():
        keys[:WINDOW, :] = jnp.zeros((WINDOW, keys.shape[1]), BF16)
        values[:WINDOW, :] = jnp.zeros((WINDOW, values.shape[1]), BF16)

    bunch = 8

    def wide(ref, index, q):
        return jnp.broadcast_to(ref[index, q : q + 1, :], (SEGS, LANES))

    def scan(first, start, keep):
        br = [wide(base, 0, first + i) for i in range(bunch)]
        bi = [wide(base, 1, first + i) for i in range(bunch)]

        def steps(jj, carry):
            carry = list(carry)
            kept = [[] for _ in range(2 * bunch)]
            for sub in range(2):
                spot = pl.ds(pl.multiple_of((2 * jj + sub) * SEGS, SEGS), SEGS)
                for i in range(bunch):
                    r, m = carry[2 * i], carry[2 * i + 1]
                    p = pushed[first + i, spot, :]
                    new_r = br[i] * r - bi[i] * m + p[:, :LANES]
                    new_m = br[i] * m + bi[i] * r + p[:, LANES:]
                    carry[2 * i], carry[2 * i + 1] = new_r, new_m
                    kept[2 * i].append(new_r)
                    kept[2 * i + 1].append(new_m)
            if keep:
                spot = pl.ds(pl.multiple_of(jj * 2 * SEGS, 2 * SEGS), 2 * SEGS)
                for i in range(bunch):
                    for part in range(2):
                        value = jnp.concatenate(kept[2 * i + part], axis=0).astype(BF16)
                        states_ref[first + i, spot, pl.ds(part * LANES, LANES)] = value
            return tuple(carry)

        return lax.fori_loop(0, length // 2, steps, tuple(start), unroll=2)

    def row(kind, q):
        return table[kind * SEGS : (kind + 1) * SEGS, q * LANES : (q + 1) * LANES]

    sub = lax.broadcasted_iota(jnp.int32, (SEGS, LANES), 0)
    near_me = near.at[mine]
    near_me[2 * pairs :, :] = shift_rows[...]
    for first in range(0, pairs, bunch):
        ends = scan(first, [jnp.zeros((SEGS, LANES), F32)] * (2 * bunch), False)
        for i in range(bunch):
            q = first + i
            fin = row(FIN, q)
            h_r, h_i = ends[2 * i] * fin, ends[2 * i + 1] * fin
            for d, kind in enumerate((ONE, TWO, FOUR)):
                hop = 1 << d
                weight = jnp.where(sub >= hop, row(kind, q), 0.0)
                a_r, a_i = cmul(
                    pltpu.roll(h_r, hop, 0), pltpu.roll(h_i, hop, 0),
                    wide(base, 2 + 2 * d, q), wide(base, 3 + 2 * d, q),
                )
                h_r, h_i = h_r + weight * a_r, h_i + weight * a_i
            near_me[q : q + 1, :] = h_r[SEGS - 1 :]
            near_me[pairs + q : pairs + q + 1, :] = h_i[SEGS - 1 :]
            ref = row(REF, q)
            entry[0, q] = jnp.where(sub >= 1, pltpu.roll(h_r, 1, 0), 0.0) * ref
            entry[1, q] = jnp.where(sub >= 1, pltpu.roll(h_i, 1, 0), 0.0) * ref

    def to_near(target):
        return pltpu.make_async_remote_copy(
            src_ref=near_me, dst_ref=near_me, send_sem=near_send.at[target], recv_sem=near_recv.at[mine],
            device_id={"sp": plane * inner + target}, device_id_type=MESH,
        )

    def from_near(source):
        return pltpu.make_async_remote_copy(
            src_ref=near_me, dst_ref=near.at[source], send_sem=near_send.at[source], recv_sem=near_recv.at[source],
            device_id={"sp": plane * inner + source}, device_id_type=MESH,
        )

    for copy in weights[:4]:
        copy.wait()
    for hop in range(1, inner):
        to_near(lax.rem(mine + hop, inner)).start()
    for n in range(4):
        proj[n] = project(w2[n])

    small[2].wait()
    blocks = rows // WINDOW
    group_size = Q_HEADS // KV_HEADS
    tile_heads = TILE // HEAD_DIM
    q_index = lax.broadcasted_iota(jnp.int32, (WINDOW, 2 * WINDOW), 0)
    k_index = lax.broadcasted_iota(jnp.int32, (WINDOW, 2 * WINDOW), 1)
    distance = WINDOW + q_index - k_index
    in_window = (distance >= 0) & (distance < WINDOW)

    def attend(block):
        here = pl.ds(block * WINDOW, WINDOW)
        band = pl.ds(block * WINDOW, 2 * WINDOW)
        allowed = in_window
        if block == 0:
            allowed = allowed & (k_index >= jnp.where(me == 0, WINDOW, 0))
        key, value = keys[band, :], values[band, :]
        for tile in range(2):
            query = proj[tile, here, :] * jnp.asarray(HEAD_DIM ** -0.5, BF16)
            results = []
            for j in range(tile_heads):
                head_id = tile * tile_heads + j
                kv = head_id // group_size
                k = key[:, kv * HEAD_DIM : (kv + 1) * HEAD_DIM]
                v = value[:, kv * HEAD_DIM : (kv + 1) * HEAD_DIM]
                scores = ntdot(query[:, j * HEAD_DIM : (j + 1) * HEAD_DIM], k)
                scores = jnp.where(allowed, scores, NEG_FILL)
                sink = sink_ref[head_id]
                maxima = jnp.maximum(jnp.max(scores, axis=-1, keepdims=True), sink)
                exponent = jnp.exp(scores - maxima)
                total = jnp.sum(exponent, axis=-1, keepdims=True) + jnp.exp(sink - maxima)
                results.append(ndot(exponent.astype(BF16), v) * (1.0 / total))
            gate = jax.nn.sigmoid(proj[2 + tile, here, :].astype(F32))
            head[here, pl.ds(tile * TILE, TILE)] = (gate * jnp.concatenate(results, axis=1)).astype(BF16)

    for block in range(1, blocks):
        attend(block)

    for hop in range(1, inner):
        from_near(lax.rem(mine + hop, inner)).wait_recv()
    block_r, block_i = base[8], base[9]
    agg_r = agg_i = jnp.zeros((pairs, LANES), F32)
    agg_s = jnp.zeros((1, LANES), F32)
    pw_r, pw_i = jnp.ones((pairs, LANES), F32), jnp.zeros((pairs, LANES), F32)
    pre = [agg_r, agg_i, agg_s, pw_r, pw_i]
    for i in range(inner):
        now = [agg_r, agg_i, agg_s, pw_r, pw_i]
        if i > 0:
            pre = [jnp.where(mine == i, a, b) for a, b in zip(now, pre)]
        shift_i = near[i, 2 * pairs : 2 * pairs + 1, :]
        a_r, a_i = cmul(agg_r, agg_i, block_r, block_i)
        factor = jnp.exp(per_pair(shift_i, pairs))
        agg_r = factor * a_r + near[i, :pairs, :]
        agg_i = factor * a_i + near[i, pairs : 2 * pairs, :]
        agg_s = agg_s + shift_i
        pw_r, pw_i = cmul(pw_r, pw_i, block_r, block_i)
    plane_r, plane_i = pw_r, pw_i
    far_me = far.at[plane]
    far_me[:pairs, :] = agg_r
    far_me[pairs : 2 * pairs, :] = agg_i
    far_me[2 * pairs :, :] = jnp.broadcast_to(agg_s, (SEGS, LANES))

    def to_far(target):
        return pltpu.make_async_remote_copy(
            src_ref=far_me, dst_ref=far_me, send_sem=far_send.at[target], recv_sem=far_recv.at[plane],
            device_id={"sp": target * inner + mine}, device_id_type=MESH,
        )

    def from_far(source):
        return pltpu.make_async_remote_copy(
            src_ref=far_me, dst_ref=far.at[source], send_sem=far_send.at[source], recv_sem=far_recv.at[source],
            device_id={"sp": source * inner + mine}, device_id_type=MESH,
        )

    before = jnp.exp(per_pair(pre[2], pairs))
    before_r, before_i = before * pre[3], before * pre[4]
    for q in range(pairs):
        spot = pl.ds(q * SEGS, SEGS)
        scale = row(PRE, q) * row(REF, q)
        init[0, q] = power[0, spot, :] * scale
        init[1, q] = power[1, spot, :] * scale

    for copy in weights[4:]:
        copy.wait()
    for target in range(1, outer):
        @pl.when(plane < target)
        def _():
            to_far(target).start()

    gates = [project(w2[4 + c]) for c in range(2)]
    for c in range(2):
        gate_ref[:, c * TILE : (c + 1) * TILE] = ndot(permute[...], gates[c]).astype(BF16)

    @pl.when(me > 0)
    def _():
        for copy in halos(me):
            copy.wait_recv()

    attend(0)
    small[3].wait()
    small[4].wait()
    width = how.shape[1] // 2
    pieces = away.shape[0]
    step = width // pieces

    def part_of(owner, piece):
        return pl.ds(pl.multiple_of(owner * width + piece * step, LANES), step)

    for piece in range(pieces):
        acc_other[piece] = ndot(head[...], how[:, part_of(other, piece)])
        acc_me[piece] = ndot(head[...], how[:, part_of(tp, piece)])

    carry_r = carry_i = jnp.zeros((pairs, LANES), F32)
    for z in range(outer - 1):
        @pl.when(z < plane)
        def _():
            from_far(z).wait_recv()

    for z in range(outer - 1):
        factor = jnp.exp(per_pair(far[z, 2 * pairs : 2 * pairs + 1, :], pairs))
        a_r, a_i = cmul(carry_r, carry_i, plane_r, plane_i)
        carry_r = jnp.where(z < plane, factor * a_r + far[z, :pairs, :], carry_r)
        carry_i = jnp.where(z < plane, factor * a_i + far[z, pairs : 2 * pairs, :], carry_i)
    in_r, in_i = cmul(carry_r, carry_i, before_r, before_i)
    carried[0], carried[1] = in_r + pre[0], in_i + pre[1]
    for first in range(0, pairs, bunch):
        start = []
        for i in range(bunch):
            q = first + i
            s_r, s_i = cmul(init[0, q], init[1, q], wide(carried, 0, q), wide(carried, 1, q))
            start += [entry[0, q] + s_r, entry[1, q] + s_i]
        scan(first, start, True)
    for tile in range(tiles):
        lanes = pl.ds(tile * LANES, LANES)
        seen = sum(
            ntdot(states_ref[q], readout[q]) for q in range(tile * pairs_tile, (tile + 1) * pairs_tile)
        )
        recurrent = wout[:, lanes] * seen + skip_row[:1, lanes] * u_ref[:, lanes].astype(F32)
        gate = jax.nn.sigmoid(gate_ref[:, lanes].astype(F32))
        mixed[:, lanes] = (gate * jax.nn.gelu(recurrent)).astype(BF16)
    state = ndot(back[...], mixed[...]).astype(BF16)

    copies = [
        pltpu.make_async_remote_copy(
            src_ref=away.at[piece], dst_ref=landed.at[piece],
            send_sem=out_send.at[piece], recv_sem=out_recv.at[piece],
            device_id={"tp": other}, device_id_type=MESH,
        )
        for piece in range(pieces)
    ]
    for piece in range(pieces):
        away[piece] = (acc_other[piece] + ndot(state, sow[:, part_of(other, piece)])).astype(BF16)
        if piece > 0:
            copies[piece - 1].start()
    total_ref[0] = acc_me[0] + ndot(state, sow[:, part_of(tp, 0)])
    copies[pieces - 1].start()
    for piece in range(1, pieces):
        total_ref[piece] = acc_me[piece] + ndot(state, sow[:, part_of(tp, piece)])

    for hop in range(1, inner):
        to_near(lax.rem(mine + hop, inner)).wait_send()
    for target in range(1, outer):
        @pl.when(plane < target)
        def _():
            to_far(target).wait_send()

    @pl.when(me < count - 1)
    def _():
        for copy in halos(me + 1):
            copy.wait_send()
    for copy in copies:
        copy.wait()


def add_kernel(total_ref, landed_ref, out_ref, stage, sem):
    pieces, _, step = landed_ref.shape
    copies = [
        pltpu.make_async_copy(stage.at[piece], out_ref.at[:, pl.ds(piece * step, step)], sem.at[piece])
        for piece in range(pieces)
    ]
    for piece in range(pieces):
        stage[piece] = (total_ref[piece] + landed_ref[piece].astype(F32)).astype(BF16)
        copies[piece].start()
    for copy in copies:
        copy.wait()


def on_device(
    hidden, query_weight, key_weight, value_weight, head_gate_weight, state_in_weight, state_gate_weight,
    sink_logit, decay_real, decay_frequency, log_step, input_real, input_imaginary, output_real,
    output_imaginary, skip_weight, decay_shift, head_out_weight, state_out_weight,
):
    rows, half = hidden.shape
    groups, states = decay_real.shape
    pairs = groups // 2
    channels = groups * GROUP_CH
    count = lax.axis_size("sp")
    inner = 1 << (count.bit_length() // 2)
    outer = count // inner
    permute, back, running, sums, spread, widen = constants(rows, groups, states)
    width = head_out_weight.shape[1] // 2
    pieces = 4
    like = lambda v: pltpu.VMEM(v.shape, v.dtype)
    pin = lambda v: pltpu.with_memory_space_constraint(v, pltpu.HBM)
    shaped = jax.ShapeDtypeStruct
    dma = pltpu.SemaphoreType.DMA
    mib = 1024 * 1024
    small = (
        decay_real, decay_frequency, log_step.reshape(1, groups), decay_shift, running, sums, spread, widen,
        input_real.transpose(0, 2, 1), input_imaginary.transpose(0, 2, 1), output_real, output_imaginary,
        skip_weight.T,
    )
    first_tiles = (state_in_weight.shape[1] + key_weight.shape[1] + value_weight.shape[1]) // TILE
    prepared = (
        shaped((2, rows, half), BF16),
        shaped((first_tiles, 2 * half, TILE), BF16),
        shaped((pairs, LANES, TILE), BF16),
        shaped((pairs, LANES, TILE), BF16),
        shaped((rows, channels), F32),
        shaped((rows, channels), F32),
        shaped((10, pairs, LANES), F32),
        shaped((2, pairs * SEGS, LANES), F32),
        shaped((7 * SEGS, groups * states), F32),
        shaped((SEGS, LANES), F32),
        shaped((SEGS, channels), F32),
    )
    ready = pl.pallas_call(
        prepare_kernel,
        out_shape=prepared,
        in_specs=[ANY] * (4 + len(small)),
        out_specs=(VMEM,) * len(prepared),
        scratch_shapes=[
            *[like(v) for v in small],
            pltpu.VMEM((2, pairs, LANES), F32),
            dma((1 + len(small),)), dma((first_tiles,)), dma, dma,
        ],
        compiler_params=pltpu.CompilerParams(
            vmem_limit_bytes=PREP_MIB * mib, collective_id=0, has_side_effects=True
        ),
        name="prepare",
    )(*map(pin, (hidden, state_in_weight, key_weight, value_weight, *small)))
    total, landed = pl.pallas_call(
        layer_kernel,
        out_shape=(
            shaped((pieces, rows, width // pieces), F32),
            shaped((pieces, rows, width // pieces), BF16),
        ),
        in_specs=[VMEM] * len(prepared) + [ANY] * 8,
        out_specs=(VMEM, VMEM),
        scratch_shapes=[
            pltpu.VMEM((6, 2 * half, TILE), BF16),
            like(head_out_weight), like(state_out_weight), like(permute), like(back),
            pltpu.SMEM(sink_logit.shape, F32),
            pltpu.VMEM((pairs, rows, TILE), F32),
            pltpu.VMEM((pairs, rows, TILE), BF16),
            pltpu.VMEM((rows, channels), BF16),
            pltpu.VMEM((rows, channels), BF16),
            pltpu.VMEM((2, pairs, LANES), F32),
            pltpu.VMEM((2, pairs, SEGS, LANES), F32),
            pltpu.VMEM((2, pairs, SEGS, LANES), F32),
            pltpu.VMEM((4, rows, TILE), BF16),
            pltpu.VMEM((WINDOW + rows, TILE), BF16),
            pltpu.VMEM((WINDOW + rows, TILE), BF16),
            pltpu.VMEM((rows, channels), BF16),
            pltpu.VMEM((rows, channels), BF16),
            pltpu.VMEM((inner, 2 * pairs + SEGS, LANES), F32),
            pltpu.VMEM((outer, 2 * pairs + SEGS, LANES), F32),
            pltpu.VMEM((pieces, rows, width // pieces), F32),
            pltpu.VMEM((pieces, rows, width // pieces), F32),
            pltpu.VMEM((pieces, rows, width // pieces), BF16),
            dma((5,)), dma((6,)), dma((inner,)), dma((inner,)), dma((outer,)), dma((outer,)),
            dma((2,)), dma((2,)), dma((pieces,)), dma((pieces,)),
        ],
        compiler_params=pltpu.CompilerParams(
            vmem_limit_bytes=LAYER_MIB * mib, collective_id=1, has_side_effects=True
        ),
        name="layer",
    )(
        *ready,
        *map(pin, (
            query_weight, head_gate_weight, state_gate_weight, sink_logit, head_out_weight, state_out_weight,
            permute, back,
        )),
    )
    return pl.pallas_call(
        add_kernel,
        out_shape=shaped((rows, width), BF16),
        in_specs=[VMEM, VMEM],
        out_specs=ANY,
        scratch_shapes=[pltpu.VMEM((pieces, rows, width // pieces), BF16), dma((pieces,))],
        compiler_params=pltpu.CompilerParams(vmem_limit_bytes=ADD_MIB * mib),
        name="add",
    )(total, landed)


def solution(mesh):
    in_specs = (
        P("sp", "tp"),
        P(None, "tp"),
        P(None, "tp"),
        P(None, "tp"),
        P(None, "tp"),
        P(None, "tp"),
        P(None, "tp"),
        P("tp"),
        P("tp", None),
        P("tp", None),
        P("tp"),
        P("tp", None, None),
        P("tp", None, None),
        P("tp", None, None),
        P("tp", None, None),
        P("tp", None),
        P("tp", "sp"),
        P("tp", None),
        P("tp", None),
    )
    out_specs = P("sp", "tp")
    return jax.shard_map(
        on_device, mesh=mesh, in_specs=in_specs, out_specs=out_specs, check_vma=False
    )
```

```python
import jax
import jax.numpy as jnp
import numpy as np
from jax import lax
from jax.experimental import pallas as pl
from jax.experimental.pallas import tpu as pltpu
from jax.sharding import PartitionSpec as P

HEAD_DIM = 64
Q_HEADS = 16
KV_HEADS = 8
GROUP_CH = 16
WINDOW = 128
LANES = 128
SEGS = 8
TILE = 256

PREP_MIB, LAYER_MIB, CLOSE_MIB = 12, 36, 6

NEG_FILL = -1e30
MESH = pl.DeviceIdType.MESH
ANY = pl.BlockSpec(memory_space=pl.ANY)
VMEM = pl.BlockSpec(memory_space=pltpu.VMEM)
SMEM = pl.BlockSpec(memory_space=pltpu.SMEM)
BF16 = jnp.bfloat16
F32 = jnp.float32
NT = (((1,), (1,)), ((), ()))


def split(value, pieces):
    out = []
    for _ in range(pieces):
        high = value.astype(BF16)
        out.append(high)
        value = value - high.astype(F32)
    return out


def ndot(a, b):
    return jnp.dot(a, b, preferred_element_type=F32)


def ntdot(a, b):
    return lax.dot_general(a, b, NT, preferred_element_type=F32)


def cmul(ar, ai, br, bi):
    return ar * br - ai * bi, ar * bi + ai * br


REF, FIN, PRE, ONE, TWO, FOUR, ALL = range(7)


def constants(rows, groups, states):
    length = rows // SEGS
    time = np.arange(rows)
    seg, pos = time // length, time % length
    order = (time % SEGS) * length + time // SEGS
    permute = (order[:, None] == time[None]).astype(np.float32)
    same = seg[order][:, None] == seg[None]
    upto = (order[:, None] >= time[None]).astype(np.float32)
    first = (pos < length // 2).astype(np.float32)[None]
    running = same * (upto - first)
    k = np.arange(SEGS)[:, None]
    here = seg[None] == k
    sums = np.concatenate(
        [
            here * first,
            here * (1 - first),
            seg[None] < k,
            here,
            (seg[None] <= k) & (seg[None] > k - 2),
            (seg[None] <= k) & (seg[None] > k - 4),
            np.ones((SEGS, rows)),
        ],
        axis=0,
    ).astype(np.float32)
    column = np.arange(groups * GROUP_CH) // GROUP_CH
    spread = (np.arange(groups)[:, None] == column[None]).astype(np.float32)
    lane = np.arange(groups * states) // states
    widen = (np.arange(groups)[:, None] == lane[None]).astype(np.float32)
    make = lambda x: jnp.asarray(x, BF16)
    return (
        make(permute), make(permute.T), make(running), make(sums),
        make(np.concatenate([spread, spread], axis=0)), make(np.concatenate([widen] * 3, axis=0)),
    )


def per_pair(row, pairs):
    spots = row.shape[1]
    wide = jnp.broadcast_to(row, (pairs, spots))
    r = lax.broadcasted_iota(jnp.int32, (pairs, spots), 0)
    c = lax.broadcasted_iota(jnp.int32, (pairs, spots), 1)
    even = jnp.sum(jnp.where(c == 2 * r, wide, 0.0), axis=1, keepdims=True)
    odd = jnp.sum(jnp.where(c == 2 * r + 1, wide, 0.0), axis=1, keepdims=True)
    low = lax.broadcasted_iota(jnp.int32, (pairs, LANES), 1) < LANES // 2
    return jnp.where(low, even, odd)


def fetch_all(pairs_of, sems, first=0):
    return [pltpu.make_async_copy(src, dst, sems.at[first + i]) for i, (src, dst) in enumerate(pairs_of)]


def prepare_kernel(
    hidden_ref, wsi_ref, wk_ref, wv_ref, dr_in, df_in, ls_in, shift_in, running_in, sums_in, spread_in, widen_in,
    ir_in, ii_in, permute_in,
    x, w, drive, win, shrunk, base, power, table, shift_rows, permute, spread,
    dr, df, ls, shift, running, sums, widen, ir, ii, zoh,
    in_sem, w_sem, x_send, x_recv,
):
    tp = lax.axis_index("tp")
    other = 1 - tp
    pairs = drive.shape[0]
    groups = 2 * pairs
    rows = win.shape[0]
    length = rows // SEGS
    pairs_tile = LANES // GROUP_CH // 2
    barrier = pltpu.get_barrier_semaphore()
    pl.semaphore_signal(barrier, inc=1, device_id={"tp": other}, device_id_type=MESH)
    own_x = pltpu.make_async_copy(hidden_ref, x.at[tp], in_sem.at[0])
    own_x.start()
    small = fetch_all((
        (dr_in, dr), (df_in, df), (ls_in, ls), (shift_in, shift), (running_in, running), (sums_in, sums),
        (spread_in, spread), (widen_in, widen), (ir_in, ir), (ii_in, ii), (permute_in, permute),
    ), in_sem, 1)
    for copy in small:
        copy.start()
    columns = [
        (ref.at[:, pl.ds(c * TILE, TILE)], w.at[i + c])
        for ref, i in ((wsi_ref, 0), (wk_ref, 2), (wv_ref, 3)) for c in range(ref.shape[1] // TILE)
    ]
    weights = fetch_all(columns, w_sem)
    for copy in weights:
        copy.start(priority=1)
    zero = jnp.zeros((LANES, TILE), BF16)
    for q in range(pairs):
        drive[q] = zero

    pl.semaphore_wait(barrier, 1)
    own_x.wait()
    swap = pltpu.make_async_remote_copy(
        src_ref=x.at[tp], dst_ref=x.at[tp], send_sem=x_send, recv_sem=x_recv,
        device_id={"tp": other}, device_id_type=MESH,
    )
    swap.start()

    for copy in small[:7]:
        copy.wait()
    two = lambda ref: jnp.concatenate(
        [ref[pl.ds(0, pairs, stride=2), :], ref[pl.ds(1, pairs, stride=2), :]], axis=1
    )
    decay, frequency = two(dr), two(df)
    stepsize = jnp.exp(per_pair(ls[...], pairs))
    magnitude = jnp.exp(decay * stepsize)
    rotation = frequency * stepsize
    base_r, base_i = magnitude * jnp.cos(rotation), magnitude * jnp.sin(rotation)
    denominator = decay * decay + frequency * frequency
    less = base_r - 1.0
    zoh[0] = (less * decay + base_i * frequency) / denominator
    zoh[1] = (base_i * decay - less * frequency) / denominator
    base[0], base[1] = base_r, base_i
    power_r, power_i = base_r, base_i
    for _ in range(length.bit_length() - 1):
        power_r, power_i = cmul(power_r, power_i, power_r, power_i)
    for d in range(4):
        base[2 + 2 * d], base[3 + 2 * d] = power_r, power_i
        if d == 0:
            step_r, step_i = power_r, power_i
        power_r, power_i = cmul(power_r, power_i, power_r, power_i)
    run_r, run_i = jnp.ones_like(base_r), jnp.zeros_like(base_r)
    for k in range(SEGS):
        spot = pl.ds(k, pairs, stride=SEGS)
        power[0, spot, :] = run_r
        power[1, spot, :] = run_i
        run_r, run_i = cmul(run_r, run_i, step_r, step_i)

    shifts = split(shift[...], 3)
    relative = sum(ntdot(running[...], piece) for piece in shifts)
    totals = sum(ntdot(sums[...], piece) for piece in shifts)
    grown = jnp.concatenate(split(jnp.exp(-relative), 2), axis=1)
    shrunk[...] = jnp.concatenate(split(jnp.exp(relative), 2), axis=1)
    win[...] = ndot(grown, spread[...])
    shift_rows[...] = jnp.concatenate(
        [totals[ALL * SEGS : (ALL + 1) * SEGS], jnp.zeros((SEGS, LANES - groups), F32)], axis=1
    )
    scales = jnp.concatenate(split(jnp.exp(totals), 3), axis=1)
    for copy in small[7:]:
        copy.wait()
    table[...] = ndot(scales, widen[...])

    row_low = lax.broadcasted_iota(jnp.int32, (2 * GROUP_CH, LANES), 0) < GROUP_CH
    lane_low = lax.broadcasted_iota(jnp.int32, (2 * GROUP_CH, LANES), 1) < LANES // 2
    own_lane = row_low == lane_low
    for q in range(pairs):
        pick = lambda ref: jnp.concatenate([
            jnp.concatenate([ref[2 * q], ref[2 * q]], axis=1),
            jnp.concatenate([ref[2 * q + 1], ref[2 * q + 1]], axis=1),
        ], axis=0)
        spot = pl.ds((q % pairs_tile) * 2 * GROUP_CH, 2 * GROUP_CH)
        in_r, in_i = pick(ir), pick(ii)
        z_r, z_i = zoh[0, q : q + 1, :], zoh[1, q : q + 1, :]
        d_r, d_i = cmul(z_r, z_i, in_r, in_i)
        drive[q, spot, :] = jnp.concatenate(
            [jnp.where(own_lane, d_r, 0.0), jnp.where(own_lane, d_i, 0.0)], axis=1
        ).astype(BF16)
    swap.wait()
    for copy in weights:
        copy.wait()


def layer_kernel(
    x, w, drive, win, shrunk, base, power, table, shift_rows, permute, spread,
    wq_ref, wg_ref, wsg_ref, sink_in, how_ref, sow_ref, back_in, or_in, oi_in, skip_in,
    acc, state_x, sow_x,
    w2, how, how_x, sow, back, sink_ref, orr, oi, skip, readout, wout, skip_row,
    pushed, states_ref, u_ref, gate_ref, carried, entry, init,
    proj, keys, values, mixed, head, head_x, state, near, far,
    in_sem, w_sem, near_send, near_recv, far_send, far_recv, halo_send, halo_recv, x_send, x_recv,
):
    tp = lax.axis_index("tp")
    other = 1 - tp
    me = lax.axis_index("sp")
    count = lax.axis_size("sp")
    inner, outer = near.shape[0], far.shape[0]
    mine, plane = lax.rem(me, inner), lax.div(me, inner)
    rows, half_width = x.shape[1:]
    pairs = drive.shape[0]
    groups = 2 * pairs
    length = rows // SEGS
    per_tile = LANES // GROUP_CH
    tiles = groups // per_tile
    pairs_tile = per_tile // 2

    barrier = pltpu.get_barrier_semaphore()
    for hop in range(1, inner):
        target = plane * inner + lax.rem(mine + hop, inner)
        pl.semaphore_signal(barrier, inc=1, device_id={"sp": target}, device_id_type=MESH)
    for hop in range(1, outer):
        target = lax.rem(plane + hop, outer) * inner + mine
        pl.semaphore_signal(barrier, inc=1, device_id={"sp": target}, device_id_type=MESH)
    for step in (1, count - 1):
        target = lax.rem(me + step, count)
        pl.semaphore_signal(barrier, inc=1, device_id={"sp": target}, device_id_type=MESH)
    pl.semaphore_signal(barrier, inc=1, device_id={"tp": other}, device_id_type=MESH)

    pieces, _, step = acc.shape
    width = pieces * step
    half_of = lambda ref, owner: ref.at[:, pl.ds(pl.multiple_of(owner * width, LANES), width)]
    small = fetch_all((
        (sink_in, sink_ref), (or_in, orr), (oi_in, oi), (skip_in, skip), (back_in, back),
        (half_of(how_ref, tp), how), (half_of(sow_ref, tp), sow),
    ), in_sem)
    columns = [
        (ref.at[:, pl.ds(c * TILE, TILE)], w2.at[2 * i + c])
        for i, ref in enumerate((wq_ref, wg_ref, wsg_ref)) for c in range(2)
    ]
    weights = fetch_all(columns, w_sem)
    for copy in small[:5] + weights + small[5:]:
        copy.start()

    def cross(k, src, dst):
        return pltpu.make_async_remote_copy(
            src_ref=src, dst_ref=dst, send_sem=x_send.at[k], recv_sem=x_recv.at[k],
            device_id={"tp": other}, device_id_type=MESH,
        )

    crossing = [cross(0, half_of(how_ref, other), how_x), cross(1, half_of(sow_ref, other), sow_x)]
    head_cross, state_cross = cross(2, head, head_x), cross(3, state, state_x)

    def project(block):
        return (ndot(x[0], block[:half_width, :]) + ndot(x[1], block[half_width:, :])).astype(BF16)

    own_rows = pl.ds(WINDOW, rows)
    fed = [project(w[c]) for c in range(2)]
    us = [ndot(permute[...], part) for part in fed]
    keys[own_rows, :] = project(w[2])
    for c in range(2):
        lanes = pl.ds(c * TILE, TILE)
        u_ref[:, lanes] = us[c].astype(BF16)
        weighted = (us[c] * win[:, lanes]).astype(BF16)
        for t in range(TILE // LANES):
            tile = c * (TILE // LANES) + t
            part = weighted[:, t * LANES : (t + 1) * LANES]
            for i in range(pairs_tile):
                q = tile * pairs_tile + i
                pushed[q] = ndot(part, drive[q])
    values[own_rows, :] = project(w[3])

    bunch = 8

    def wide(ref, index, q):
        return jnp.broadcast_to(ref[index, q : q + 1, :], (SEGS, LANES))

    def scan(first, start, keep):
        br = [wide(base, 0, first + i) for i in range(bunch)]
        bi = [wide(base, 1, first + i) for i in range(bunch)]

        def steps(jj, carry):
            carry = list(carry)
            kept = [[] for _ in range(2 * bunch)]
            for sub in range(2):
                spot = pl.ds(pl.multiple_of((2 * jj + sub) * SEGS, SEGS), SEGS)
                for i in range(bunch):
                    r, m = carry[2 * i], carry[2 * i + 1]
                    p = pushed[first + i, spot, :]
                    new_r = br[i] * r - bi[i] * m + p[:, :LANES]
                    new_m = br[i] * m + bi[i] * r + p[:, LANES:]
                    carry[2 * i], carry[2 * i + 1] = new_r, new_m
                    kept[2 * i].append(new_r)
                    kept[2 * i + 1].append(new_m)
            if keep:
                spot = pl.ds(pl.multiple_of(jj * 2 * SEGS, 2 * SEGS), 2 * SEGS)
                for i in range(bunch):
                    for part in range(2):
                        value = jnp.concatenate(kept[2 * i + part], axis=0).astype(BF16)
                        states_ref[first + i, spot, pl.ds(part * LANES, LANES)] = value
            return tuple(carry)

        return lax.fori_loop(0, length // 2, steps, tuple(start), unroll=2)

    def row(kind, q):
        return table[kind * SEGS : (kind + 1) * SEGS, q * LANES : (q + 1) * LANES]

    sub = lax.broadcasted_iota(jnp.int32, (SEGS, LANES), 0)
    near_me = near.at[mine]
    near_me[2 * pairs :, :] = shift_rows[...]
    for first in range(0, pairs, bunch):
        ends = scan(first, [jnp.zeros((SEGS, LANES), F32)] * (2 * bunch), False)
        for i in range(bunch):
            q = first + i
            fin = row(FIN, q)
            h_r, h_i = ends[2 * i] * fin, ends[2 * i + 1] * fin
            for d, kind in enumerate((ONE, TWO, FOUR)):
                hop = 1 << d
                weight = jnp.where(sub >= hop, row(kind, q), 0.0)
                a_r, a_i = cmul(
                    pltpu.roll(h_r, hop, 0), pltpu.roll(h_i, hop, 0),
                    wide(base, 2 + 2 * d, q), wide(base, 3 + 2 * d, q),
                )
                h_r, h_i = h_r + weight * a_r, h_i + weight * a_i
            near_me[q : q + 1, :] = h_r[SEGS - 1 :]
            near_me[pairs + q : pairs + q + 1, :] = h_i[SEGS - 1 :]
            ref = row(REF, q)
            entry[0, q] = jnp.where(sub >= 1, pltpu.roll(h_r, 1, 0), 0.0) * ref
            entry[1, q] = jnp.where(sub >= 1, pltpu.roll(h_i, 1, 0), 0.0) * ref

    blocks = rows // WINDOW
    group_size = Q_HEADS // KV_HEADS
    tile_heads = TILE // HEAD_DIM
    q_index = lax.broadcasted_iota(jnp.int32, (WINDOW, 2 * WINDOW), 0)
    k_index = lax.broadcasted_iota(jnp.int32, (WINDOW, 2 * WINDOW), 1)
    distance = WINDOW + q_index - k_index
    in_window = (distance >= 0) & (distance < WINDOW)

    def attend(block):
        here = pl.ds(block * WINDOW, WINDOW)
        band = pl.ds(block * WINDOW, 2 * WINDOW)
        allowed = in_window
        if block == 0:
            allowed = allowed & (k_index >= jnp.where(me == 0, WINDOW, 0))
        key, value = keys[band, :], values[band, :]
        for tile in range(2):
            query = proj[tile, here, :] * jnp.asarray(HEAD_DIM ** -0.5, BF16)
            results = []
            for j in range(tile_heads):
                head_id = tile * tile_heads + j
                kv = head_id // group_size
                k = key[:, kv * HEAD_DIM : (kv + 1) * HEAD_DIM]
                v = value[:, kv * HEAD_DIM : (kv + 1) * HEAD_DIM]
                scores = ntdot(query[:, j * HEAD_DIM : (j + 1) * HEAD_DIM], k)
                scores = jnp.where(allowed, scores, NEG_FILL)
                sink = sink_ref[head_id]
                maxima = jnp.maximum(jnp.max(scores, axis=-1, keepdims=True), sink)
                exponent = jnp.exp(scores - maxima)
                total = jnp.sum(exponent, axis=-1, keepdims=True) + jnp.exp(sink - maxima)
                results.append(ndot(exponent.astype(BF16), v) * (1.0 / total))
            gate = jax.nn.sigmoid(proj[2 + tile, here, :].astype(F32))
            head[here, pl.ds(tile * TILE, TILE)] = (gate * jnp.concatenate(results, axis=1)).astype(BF16)

    def middle():
        for copy in weights[:4] + small[:1]:
            copy.wait()
        for n in range(4):
            proj[n] = project(w2[n])
        for block in range(1, blocks):
            attend(block)

    pl.when(me == 0)(middle)

    def to_near(target):
        return pltpu.make_async_remote_copy(
            src_ref=near_me, dst_ref=near_me, send_sem=near_send.at[target], recv_sem=near_recv.at[mine],
            device_id={"sp": plane * inner + target}, device_id_type=MESH,
        )

    def from_near(source):
        return pltpu.make_async_remote_copy(
            src_ref=near_me, dst_ref=near.at[source], send_sem=near_send.at[source], recv_sem=near_recv.at[source],
            device_id={"sp": plane * inner + source}, device_id_type=MESH,
        )

    pl.semaphore_wait(barrier, inner + outer + 1)
    for hop in range(1, inner):
        to_near(lax.rem(mine + hop, inner)).start()

    def halos(target):
        return [
            pltpu.make_async_remote_copy(
                src_ref=band.at[pl.ds(rows, WINDOW)], dst_ref=band.at[pl.ds(0, WINDOW)],
                send_sem=halo_send.at[k], recv_sem=halo_recv.at[k],
                device_id={"sp": target}, device_id_type=MESH,
            )
            for k, band in enumerate((keys, values))
        ]

    @pl.when(me < count - 1)
    def _():
        for copy in halos(me + 1):
            copy.start()

    @pl.when(me == 0)
    def _():
        keys[:WINDOW, :] = jnp.zeros((WINDOW, keys.shape[1]), BF16)
        values[:WINDOW, :] = jnp.zeros((WINDOW, values.shape[1]), BF16)

    for copy in crossing:
        copy.start()

    pl.when(me != 0)(middle)

    for copy in small[1:4]:
        copy.wait()
    wout[...] = ndot(shrunk[...], spread[...])
    lanes_of = lax.broadcasted_iota(jnp.int32, (GROUP_CH, groups * GROUP_CH), 1) % GROUP_CH
    channel = lax.broadcasted_iota(jnp.int32, (GROUP_CH, groups * GROUP_CH), 0)
    skips = sum(ndot(piece, spread[:groups, :]) for piece in split(skip[...], 3))
    skip_row[...] = jnp.broadcast_to(
        jnp.sum(jnp.where(lanes_of == channel, skips, 0.0), axis=0, keepdims=True), skip_row.shape
    )
    row_low = lax.broadcasted_iota(jnp.int32, (2 * GROUP_CH, LANES), 0) < GROUP_CH
    lane_low = lax.broadcasted_iota(jnp.int32, (2 * GROUP_CH, LANES), 1) < LANES // 2
    own_lane = row_low == lane_low
    zero = jnp.zeros((LANES, TILE), BF16)
    for q in range(pairs):
        pick = lambda ref: jnp.concatenate([
            jnp.concatenate([ref[2 * q], ref[2 * q]], axis=1),
            jnp.concatenate([ref[2 * q + 1], ref[2 * q + 1]], axis=1),
        ], axis=0)
        readout[q] = zero
        readout[q, pl.ds((q % pairs_tile) * 2 * GROUP_CH, 2 * GROUP_CH), :] = jnp.concatenate(
            [jnp.where(own_lane, pick(orr), 0.0), jnp.where(own_lane, -pick(oi), 0.0)], axis=1
        ).astype(BF16)

    for hop in range(1, inner):
        from_near(lax.rem(mine + hop, inner)).wait_recv()
    block_r, block_i = base[8], base[9]
    agg_r = agg_i = jnp.zeros((pairs, LANES), F32)
    agg_s = jnp.zeros((1, LANES), F32)
    pw_r, pw_i = jnp.ones((pairs, LANES), F32), jnp.zeros((pairs, LANES), F32)
    pre = [agg_r, agg_i, agg_s, pw_r, pw_i]
    for i in range(inner):
        now = [agg_r, agg_i, agg_s, pw_r, pw_i]
        if i > 0:
            pre = [jnp.where(mine == i, a, b) for a, b in zip(now, pre)]
        shift_i = near[i, 2 * pairs : 2 * pairs + 1, :]
        a_r, a_i = cmul(agg_r, agg_i, block_r, block_i)
        factor = jnp.exp(per_pair(shift_i, pairs))
        agg_r = factor * a_r + near[i, :pairs, :]
        agg_i = factor * a_i + near[i, pairs : 2 * pairs, :]
        agg_s = agg_s + shift_i
        pw_r, pw_i = cmul(pw_r, pw_i, block_r, block_i)
    plane_r, plane_i = pw_r, pw_i
    far_me = far.at[plane]
    far_me[:pairs, :] = agg_r
    far_me[pairs : 2 * pairs, :] = agg_i
    far_me[2 * pairs :, :] = jnp.broadcast_to(agg_s, (SEGS, LANES))

    def to_far(target):
        return pltpu.make_async_remote_copy(
            src_ref=far_me, dst_ref=far_me, send_sem=far_send.at[target], recv_sem=far_recv.at[plane],
            device_id={"sp": target * inner + mine}, device_id_type=MESH,
        )

    def from_far(source):
        return pltpu.make_async_remote_copy(
            src_ref=far_me, dst_ref=far.at[source], send_sem=far_send.at[source], recv_sem=far_recv.at[source],
            device_id={"sp": source * inner + mine}, device_id_type=MESH,
        )

    before = jnp.exp(per_pair(pre[2], pairs))
    before_r, before_i = before * pre[3], before * pre[4]
    for q in range(pairs):
        spot = pl.ds(q * SEGS, SEGS)
        scale = row(PRE, q) * row(REF, q)
        init[0, q] = power[0, spot, :] * scale
        init[1, q] = power[1, spot, :] * scale

    for copy in weights[4:]:
        copy.wait()
    for target in range(1, outer):
        @pl.when(plane < target)
        def _():
            to_far(target).start()

    gates = [project(w2[4 + c]) for c in range(2)]
    for c in range(2):
        gate_ref[:, c * TILE : (c + 1) * TILE] = ndot(permute[...], gates[c]).astype(BF16)

    @pl.when(me > 0)
    def _():
        for copy in halos(me):
            copy.wait_recv()

    attend(0)
    head_cross.start()
    small[4].wait()
    small[5].wait()
    small[6].wait()
    part_of = lambda piece: pl.ds(piece * step, step)
    for piece in range(pieces):
        acc[piece] = ndot(head[...], how[:, part_of(piece)])

    carry_r = carry_i = jnp.zeros((pairs, LANES), F32)
    for z in range(outer - 1):
        @pl.when(z < plane)
        def _():
            from_far(z).wait_recv()

    for z in range(outer - 1):
        factor = jnp.exp(per_pair(far[z, 2 * pairs : 2 * pairs + 1, :], pairs))
        a_r, a_i = cmul(carry_r, carry_i, plane_r, plane_i)
        carry_r = jnp.where(z < plane, factor * a_r + far[z, :pairs, :], carry_r)
        carry_i = jnp.where(z < plane, factor * a_i + far[z, pairs : 2 * pairs, :], carry_i)
    in_r, in_i = cmul(carry_r, carry_i, before_r, before_i)
    carried[0], carried[1] = in_r + pre[0], in_i + pre[1]
    for first in range(0, pairs, bunch):
        start = []
        for i in range(bunch):
            q = first + i
            s_r, s_i = cmul(init[0, q], init[1, q], wide(carried, 0, q), wide(carried, 1, q))
            start += [entry[0, q] + s_r, entry[1, q] + s_i]
        scan(first, start, True)
    for tile in range(tiles):
        lanes = pl.ds(tile * LANES, LANES)
        seen = sum(
            ntdot(states_ref[q], readout[q]) for q in range(tile * pairs_tile, (tile + 1) * pairs_tile)
        )
        recurrent = wout[:, lanes] * seen + skip_row[:1, lanes] * u_ref[:, lanes].astype(F32)
        gate = jax.nn.sigmoid(gate_ref[:, lanes].astype(F32))
        mixed[:, lanes] = (gate * jax.nn.gelu(recurrent)).astype(BF16)
    state[...] = ndot(back[...], mixed[...]).astype(BF16)
    state_cross.start()
    crossing[0].wait()
    head_cross.wait()
    for piece in range(pieces):
        acc[piece] += (
            ndot(state[...], sow[:, part_of(piece)]) + ndot(head_x[...], how_x[:, part_of(piece)])
        )
    crossing[1].wait()

    for hop in range(1, inner):
        to_near(lax.rem(mine + hop, inner)).wait_send()
    for target in range(1, outer):
        @pl.when(plane < target)
        def _():
            to_far(target).wait_send()

    @pl.when(me < count - 1)
    def _():
        for copy in halos(me + 1):
            copy.wait_send()
    state_cross.wait()


def close_kernel(acc, state_x, sow_x, out_ref, stage, sem):
    pieces, _, step = acc.shape
    copies = [
        pltpu.make_async_copy(stage.at[piece], out_ref.at[:, pl.ds(piece * step, step)], sem.at[piece])
        for piece in range(pieces)
    ]
    for piece in range(pieces):
        stage[piece] = (acc[piece] + ndot(state_x[...], sow_x[:, pl.ds(piece * step, step)])).astype(BF16)
        copies[piece].start()
    for copy in copies:
        copy.wait()


def on_device(
    hidden, query_weight, key_weight, value_weight, head_gate_weight, state_in_weight, state_gate_weight,
    sink_logit, decay_real, decay_frequency, log_step, input_real, input_imaginary, output_real,
    output_imaginary, skip_weight, decay_shift, head_out_weight, state_out_weight,
):
    rows, half = hidden.shape
    groups, states = decay_real.shape
    pairs = groups // 2
    channels = groups * GROUP_CH
    count = lax.axis_size("sp")
    inner = 1 << (count.bit_length() // 2)
    outer = count // inner
    permute, back, running, sums, spread, widen = constants(rows, groups, states)
    width = head_out_weight.shape[1] // 2
    pieces = 4
    like = lambda v: pltpu.VMEM(v.shape, v.dtype)
    pin = lambda v: pltpu.with_memory_space_constraint(v, pltpu.HBM)
    shaped = jax.ShapeDtypeStruct
    dma = pltpu.SemaphoreType.DMA
    mib = 1024 * 1024
    small = (
        decay_real, decay_frequency, log_step.reshape(1, groups), decay_shift, running, sums, spread, widen,
        input_real.transpose(0, 2, 1), input_imaginary.transpose(0, 2, 1), permute,
    )
    late = (output_real, output_imaginary, skip_weight.T)
    first_tiles = (state_in_weight.shape[1] + key_weight.shape[1] + value_weight.shape[1]) // TILE
    prepared = (
        shaped((2, rows, half), BF16),
        shaped((first_tiles, 2 * half, TILE), BF16),
        shaped((pairs, LANES, TILE), BF16),
        shaped((rows, channels), F32),
        shaped((rows, 2 * groups), BF16),
        shaped((10, pairs, LANES), F32),
        shaped((2, pairs * SEGS, LANES), F32),
        shaped((7 * SEGS, groups * states), F32),
        shaped((SEGS, LANES), F32),
        shaped(permute.shape, BF16),
        shaped(spread.shape, BF16),
    )
    ready = pl.pallas_call(
        prepare_kernel,
        out_shape=prepared,
        in_specs=[ANY] * (4 + len(small)),
        out_specs=(VMEM,) * len(prepared),
        scratch_shapes=[
            *[like(v) for v in small if v is not permute and v is not spread],
            pltpu.VMEM((2, pairs, LANES), F32),
            dma((1 + len(small),)), dma((first_tiles,)), dma, dma,
        ],
        compiler_params=pltpu.CompilerParams(
            vmem_limit_bytes=PREP_MIB * mib, collective_id=0, has_side_effects=True
        ),
        name="prepare",
    )(*map(pin, (hidden, state_in_weight, key_weight, value_weight, *small)))
    closing = pl.pallas_call(
        layer_kernel,
        out_shape=(
            shaped((pieces, rows, width // pieces), F32),
            shaped((rows, channels), BF16),
            shaped((state_out_weight.shape[0], width), BF16),
        ),
        in_specs=[VMEM] * len(prepared) + [ANY] * (7 + len(late)),
        out_specs=(VMEM,) * 3,
        scratch_shapes=[
            pltpu.VMEM((6, 2 * half, TILE), BF16),
            *[pltpu.VMEM((head_out_weight.shape[0], width), BF16)] * 3,
            like(back),
            pltpu.SMEM(sink_logit.shape, F32),
            *[like(v) for v in late],
            pltpu.VMEM((pairs, LANES, TILE), BF16),
            pltpu.VMEM((rows, channels), F32),
            pltpu.VMEM((SEGS, channels), F32),
            pltpu.VMEM((pairs, rows, TILE), F32),
            pltpu.VMEM((pairs, rows, TILE), BF16),
            pltpu.VMEM((rows, channels), BF16),
            pltpu.VMEM((rows, channels), BF16),
            pltpu.VMEM((2, pairs, LANES), F32),
            pltpu.VMEM((2, pairs, SEGS, LANES), F32),
            pltpu.VMEM((2, pairs, SEGS, LANES), F32),
            pltpu.VMEM((4, rows, TILE), BF16),
            pltpu.VMEM((WINDOW + rows, TILE), BF16),
            pltpu.VMEM((WINDOW + rows, TILE), BF16),
            *[pltpu.VMEM((rows, channels), BF16)] * 4,
            pltpu.VMEM((inner, 2 * pairs + SEGS, LANES), F32),
            pltpu.VMEM((outer, 2 * pairs + SEGS, LANES), F32),
            dma((7,)), dma((6,)), dma((inner,)), dma((inner,)), dma((outer,)), dma((outer,)),
            dma((2,)), dma((2,)), dma((4,)), dma((4,)),
        ],
        compiler_params=pltpu.CompilerParams(
            vmem_limit_bytes=LAYER_MIB * mib, collective_id=1, has_side_effects=True
        ),
        name="layer",
    )(
        *ready,
        *map(pin, (
            query_weight, head_gate_weight, state_gate_weight, sink_logit, head_out_weight, state_out_weight,
            back, *late,
        )),
    )
    return pl.pallas_call(
        close_kernel,
        out_shape=shaped((rows, width), BF16),
        in_specs=[VMEM] * 3,
        out_specs=ANY,
        scratch_shapes=[pltpu.VMEM((pieces, rows, width // pieces), BF16), dma((pieces,))],
        compiler_params=pltpu.CompilerParams(vmem_limit_bytes=CLOSE_MIB * mib),
        name="close",
    )(*closing)


def solution(mesh):
    in_specs = (
        P("sp", "tp"),
        P(None, "tp"),
        P(None, "tp"),
        P(None, "tp"),
        P(None, "tp"),
        P(None, "tp"),
        P(None, "tp"),
        P("tp"),
        P("tp", None),
        P("tp", None),
        P("tp"),
        P("tp", None, None),
        P("tp", None, None),
        P("tp", None, None),
        P("tp", None, None),
        P("tp", None),
        P("tp", "sp"),
        P("tp", None),
        P("tp", None),
    )
    out_specs = P("sp", "tp")
    return jax.shard_map(
        on_device, mesh=mesh, in_specs=in_specs, out_specs=out_specs, check_vma=False
    )
```

```python
import jax
import jax.numpy as jnp
import numpy as np
from jax import lax
from jax.experimental import pallas as pl
from jax.experimental.pallas import tpu as pltpu
from jax.sharding import PartitionSpec as P

HEAD_DIM = 64
Q_HEADS = 16
KV_HEADS = 8
GROUP_CH = 16
WINDOW = 128
LANES = 128
SEGS = 8
TILE = 256

PREP_MIB, LAYER_MIB, CLOSE_MIB = 12, 36, 6

NEG_FILL = -1e30
MESH = pl.DeviceIdType.MESH
ANY = pl.BlockSpec(memory_space=pl.ANY)
VMEM = pl.BlockSpec(memory_space=pltpu.VMEM)
SMEM = pl.BlockSpec(memory_space=pltpu.SMEM)
BF16 = jnp.bfloat16
F32 = jnp.float32
NT = (((1,), (1,)), ((), ()))


def split(value, pieces):
    out = []
    for _ in range(pieces):
        high = value.astype(BF16)
        out.append(high)
        value = value - high.astype(F32)
    return out


def ndot(a, b):
    return jnp.dot(a, b, preferred_element_type=F32)


def ntdot(a, b):
    return lax.dot_general(a, b, NT, preferred_element_type=F32)


def cmul(ar, ai, br, bi):
    return ar * br - ai * bi, ar * bi + ai * br


REF, FIN, PRE, ONE, TWO, FOUR, ALL = range(7)


def constants(rows, groups, states):
    length = rows // SEGS
    time = np.arange(rows)
    seg, pos = time // length, time % length
    order = (time % SEGS) * length + time // SEGS
    permute = (order[:, None] == time[None]).astype(np.float32)
    same = seg[order][:, None] == seg[None]
    upto = (order[:, None] >= time[None]).astype(np.float32)
    first = (pos < length // 2).astype(np.float32)[None]
    running = same * (upto - first)
    k = np.arange(SEGS)[:, None]
    here = seg[None] == k
    sums = np.concatenate(
        [
            here * first,
            here * (1 - first),
            seg[None] < k,
            here,
            (seg[None] <= k) & (seg[None] > k - 2),
            (seg[None] <= k) & (seg[None] > k - 4),
            np.ones((SEGS, rows)),
        ],
        axis=0,
    ).astype(np.float32)
    column = np.arange(groups * GROUP_CH) // GROUP_CH
    spread = (np.arange(groups)[:, None] == column[None]).astype(np.float32)
    lane = np.arange(groups * states) // states
    widen = (np.arange(groups)[:, None] == lane[None]).astype(np.float32)
    make = lambda x: jnp.asarray(x, BF16)
    return (
        make(permute), make(permute.T), make(running), make(sums),
        make(np.concatenate([spread, spread], axis=0)), make(np.concatenate([widen] * 3, axis=0)),
    )


def per_pair(row, pairs):
    spots = row.shape[1]
    wide = jnp.broadcast_to(row, (pairs, spots))
    r = lax.broadcasted_iota(jnp.int32, (pairs, spots), 0)
    c = lax.broadcasted_iota(jnp.int32, (pairs, spots), 1)
    even = jnp.sum(jnp.where(c == 2 * r, wide, 0.0), axis=1, keepdims=True)
    odd = jnp.sum(jnp.where(c == 2 * r + 1, wide, 0.0), axis=1, keepdims=True)
    low = lax.broadcasted_iota(jnp.int32, (pairs, LANES), 1) < LANES // 2
    return jnp.where(low, even, odd)


def fetch_all(pairs_of, sems, first=0):
    return [pltpu.make_async_copy(src, dst, sems.at[first + i]) for i, (src, dst) in enumerate(pairs_of)]


def pack_shift(rows):
    high, low = split(rows, 2)
    return jnp.concatenate([high, low], axis=0)


def unpack_shift(packed):
    wide = packed.astype(F32)
    return wide[:1] + wide[SEGS : SEGS + 1]


def prepare_kernel(
    hidden_ref, wsi_ref, wk_ref, wv_ref, dr_in, df_in, ls_in, shift_in, running_in, sums_in, spread_in, widen_in,
    ir_in, ii_in, permute_in,
    x, w, drive, win, shrunk, base, power, table, shift_rows, permute, spread,
    dr, df, ls, shift, running, sums, widen, ir, ii, zoh,
    in_sem, w_sem, x_send, x_recv,
):
    tp = lax.axis_index("tp")
    other = 1 - tp
    pairs = drive.shape[0]
    groups = 2 * pairs
    rows = win.shape[0]
    length = rows // SEGS
    pairs_tile = LANES // GROUP_CH // 2
    barrier = pltpu.get_barrier_semaphore()
    pl.semaphore_signal(barrier, inc=1, device_id={"tp": other}, device_id_type=MESH)
    own_x = pltpu.make_async_copy(hidden_ref, x.at[tp], in_sem.at[0])
    own_x.start()
    small = fetch_all((
        (dr_in, dr), (df_in, df), (ls_in, ls), (shift_in, shift), (running_in, running), (sums_in, sums),
        (spread_in, spread), (widen_in, widen), (ir_in, ir), (ii_in, ii), (permute_in, permute),
    ), in_sem, 1)
    for copy in small:
        copy.start()
    columns = [
        (ref.at[:, pl.ds(c * TILE, TILE)], w.at[i + c])
        for ref, i in ((wsi_ref, 0), (wk_ref, 2), (wv_ref, 3)) for c in range(ref.shape[1] // TILE)
    ]
    weights = fetch_all(columns, w_sem)
    for copy in weights:
        copy.start(priority=1)
    zero = jnp.zeros((LANES, TILE), BF16)
    for q in range(pairs):
        drive[q] = zero

    pl.semaphore_wait(barrier, 1)
    own_x.wait()
    swap = pltpu.make_async_remote_copy(
        src_ref=x.at[tp], dst_ref=x.at[tp], send_sem=x_send, recv_sem=x_recv,
        device_id={"tp": other}, device_id_type=MESH,
    )
    swap.start()

    for copy in small[:7]:
        copy.wait()
    two = lambda ref: jnp.concatenate(
        [ref[pl.ds(0, pairs, stride=2), :], ref[pl.ds(1, pairs, stride=2), :]], axis=1
    )
    decay, frequency = two(dr), two(df)
    stepsize = jnp.exp(per_pair(ls[...], pairs))
    magnitude = jnp.exp(decay * stepsize)
    rotation = frequency * stepsize
    base_r, base_i = magnitude * jnp.cos(rotation), magnitude * jnp.sin(rotation)
    denominator = decay * decay + frequency * frequency
    less = base_r - 1.0
    zoh[0] = (less * decay + base_i * frequency) / denominator
    zoh[1] = (base_i * decay - less * frequency) / denominator
    base[0], base[1] = base_r, base_i
    power_r, power_i = base_r, base_i
    for _ in range(length.bit_length() - 1):
        power_r, power_i = cmul(power_r, power_i, power_r, power_i)
    for d in range(4):
        base[2 + 2 * d], base[3 + 2 * d] = power_r, power_i
        if d == 0:
            step_r, step_i = power_r, power_i
        power_r, power_i = cmul(power_r, power_i, power_r, power_i)
    run_r, run_i = jnp.ones_like(base_r), jnp.zeros_like(base_r)
    for k in range(SEGS):
        spot = pl.ds(k, pairs, stride=SEGS)
        power[0, spot, :] = run_r
        power[1, spot, :] = run_i
        run_r, run_i = cmul(run_r, run_i, step_r, step_i)

    shifts = split(shift[...], 3)
    relative = sum(ntdot(running[...], piece) for piece in shifts)
    totals = sum(ntdot(sums[...], piece) for piece in shifts)
    grown = jnp.concatenate(split(jnp.exp(-relative), 2), axis=1)
    shrunk[...] = jnp.concatenate(split(jnp.exp(relative), 2), axis=1)
    win[...] = ndot(grown, spread[...])
    shift_rows[...] = jnp.concatenate(
        [totals[ALL * SEGS : (ALL + 1) * SEGS], jnp.zeros((SEGS, LANES - groups), F32)], axis=1
    )
    scales = jnp.concatenate(split(jnp.exp(totals), 3), axis=1)
    for copy in small[7:]:
        copy.wait()
    table[...] = ndot(scales, widen[...])

    row_low = lax.broadcasted_iota(jnp.int32, (2 * GROUP_CH, LANES), 0) < GROUP_CH
    lane_low = lax.broadcasted_iota(jnp.int32, (2 * GROUP_CH, LANES), 1) < LANES // 2
    own_lane = row_low == lane_low
    for q in range(pairs):
        pick = lambda ref: jnp.concatenate([
            jnp.concatenate([ref[2 * q], ref[2 * q]], axis=1),
            jnp.concatenate([ref[2 * q + 1], ref[2 * q + 1]], axis=1),
        ], axis=0)
        spot = pl.ds((q % pairs_tile) * 2 * GROUP_CH, 2 * GROUP_CH)
        in_r, in_i = pick(ir), pick(ii)
        z_r, z_i = zoh[0, q : q + 1, :], zoh[1, q : q + 1, :]
        d_r, d_i = cmul(z_r, z_i, in_r, in_i)
        drive[q, spot, :] = jnp.concatenate(
            [jnp.where(own_lane, d_r, 0.0), jnp.where(own_lane, d_i, 0.0)], axis=1
        ).astype(BF16)
    swap.wait()
    for copy in weights:
        copy.wait()


def layer_kernel(
    x, w, drive, win, shrunk, base, power, table, shift_rows, permute, spread,
    wq_ref, wg_ref, wsg_ref, sink_in, how_ref, sow_ref, back_in, or_in, oi_in, skip_in,
    acc, state_x, sow_x, head_x, how_x,
    w2, how, sow, back, sink_ref, orr, oi, skip, readout, wout, skip_row,
    pushed, states_ref, u_ref, gate_ref, carried, before, entry, init,
    proj, keys, values, mixed, head, state, near, far,
    in_sem, w_sem, near_send, near_recv, far_send, first_send, far_recv, halo_send, halo_recv, x_send, x_recv,
):
    tp = lax.axis_index("tp")
    other = 1 - tp
    me = lax.axis_index("sp")
    count = lax.axis_size("sp")
    inner, outer = near.shape[0], far.shape[0]
    mine, plane = lax.rem(me, inner), lax.div(me, inner)
    rows, half_width = x.shape[1:]
    pairs = drive.shape[0]
    groups = 2 * pairs
    length = rows // SEGS
    per_tile = LANES // GROUP_CH
    tiles = groups // per_tile
    pairs_tile = per_tile // 2

    barrier = pltpu.get_barrier_semaphore()
    for hop in range(1, inner):
        target = plane * inner + lax.rem(mine + hop, inner)
        pl.semaphore_signal(barrier, inc=1, device_id={"sp": target}, device_id_type=MESH)

    @pl.when(me > 0)
    def _():
        for hop in range(1, outer):
            target = lax.rem(plane + hop, outer) * inner + mine
            target = jnp.where(target == 0, 1, target)
            pl.semaphore_signal(barrier, inc=1, device_id={"sp": target}, device_id_type=MESH)
        pl.semaphore_signal(barrier, inc=1, device_id={"sp": me - 1}, device_id_type=MESH)

    pl.semaphore_signal(barrier, inc=1, device_id={"tp": other}, device_id_type=MESH)

    pieces, _, step = acc.shape
    width = pieces * step
    half_of = lambda ref, owner: ref.at[:, pl.ds(pl.multiple_of(owner * width, LANES), width)]
    small = fetch_all((
        (sink_in, sink_ref), (or_in, orr), (oi_in, oi), (skip_in, skip), (back_in, back),
        (half_of(how_ref, tp), how), (half_of(sow_ref, tp), sow),
    ), in_sem)
    columns = [
        (ref.at[:, pl.ds(c * TILE, TILE)], w2.at[2 * i + c])
        for i, ref in enumerate((wq_ref, wg_ref, wsg_ref)) for c in range(2)
    ]
    weights = fetch_all(columns, w_sem)
    for copy in small[:5] + weights + small[5:]:
        copy.start()

    def cross(k, src, dst):
        return pltpu.make_async_remote_copy(
            src_ref=src, dst_ref=dst, send_sem=x_send.at[k], recv_sem=x_recv.at[k],
            device_id={"tp": other}, device_id_type=MESH,
        )

    crossing = [cross(0, half_of(how_ref, other), how_x), cross(1, half_of(sow_ref, other), sow_x)]
    head_cross, state_cross = cross(2, head, head_x), cross(3, state, state_x)

    def project(block):
        return (ndot(x[0], block[:half_width, :]) + ndot(x[1], block[half_width:, :])).astype(BF16)

    own_rows = pl.ds(WINDOW, rows)
    keys[own_rows, :] = project(w[2])
    values[own_rows, :] = project(w[3])
    fed = [project(w[c]) for c in range(2)]

    def halos(target):
        return [
            pltpu.make_async_remote_copy(
                src_ref=band.at[pl.ds(rows, WINDOW)], dst_ref=band.at[pl.ds(0, WINDOW)],
                send_sem=halo_send.at[k], recv_sem=halo_recv.at[k],
                device_id={"sp": target}, device_id_type=MESH,
            )
            for k, band in enumerate((keys, values))
        ]

    signals = inner + jnp.where(me < count - 1, 1, 0) + jnp.where(me > 0, outer - 2, 0)
    signals = signals + jnp.where(mine > 0, 1, 0) + jnp.where(me == 1, outer - 1, 0)

    def send_halos():
        @pl.when(me < count - 1)
        def _():
            for copy in halos(me + 1):
                copy.start()

    us = [ndot(permute[...], part) for part in fed]
    for c in range(2):
        lanes = pl.ds(c * TILE, TILE)
        u_ref[:, lanes] = us[c].astype(BF16)
        weighted = (us[c] * win[:, lanes]).astype(BF16)
        for t in range(TILE // LANES):
            tile = c * (TILE // LANES) + t
            part = weighted[:, t * LANES : (t + 1) * LANES]
            for i in range(pairs_tile):
                q = tile * pairs_tile + i
                pushed[q] = ndot(part, drive[q])

    bunch = 8

    def wide(ref, index, q):
        return jnp.broadcast_to(ref[index, q : q + 1, :], (SEGS, LANES))

    def scan(first, start, keep):
        br = [wide(base, 0, first + i) for i in range(bunch)]
        bi = [wide(base, 1, first + i) for i in range(bunch)]

        def steps(jj, carry):
            carry = list(carry)
            kept = [[] for _ in range(2 * bunch)]
            for sub in range(2):
                spot = pl.ds(pl.multiple_of((2 * jj + sub) * SEGS, SEGS), SEGS)
                for i in range(bunch):
                    r, m = carry[2 * i], carry[2 * i + 1]
                    p = pushed[first + i, spot, :]
                    new_r = br[i] * r - bi[i] * m + p[:, :LANES]
                    new_m = br[i] * m + bi[i] * r + p[:, LANES:]
                    carry[2 * i], carry[2 * i + 1] = new_r, new_m
                    kept[2 * i].append(new_r)
                    kept[2 * i + 1].append(new_m)
            if keep:
                spot = pl.ds(pl.multiple_of(jj * 2 * SEGS, 2 * SEGS), 2 * SEGS)
                for i in range(bunch):
                    for part in range(2):
                        value = jnp.concatenate(kept[2 * i + part], axis=0).astype(BF16)
                        states_ref[first + i, spot, pl.ds(part * LANES, LANES)] = value
            return tuple(carry)

        return lax.fori_loop(0, length // 2, steps, tuple(start), unroll=2)

    def row(kind, q):
        return table[kind * SEGS : (kind + 1) * SEGS, q * LANES : (q + 1) * LANES]

    sub = lax.broadcasted_iota(jnp.int32, (SEGS, LANES), 0)
    near_me = near.at[mine]
    near_me[2 * pairs :, :] = pack_shift(shift_rows[...])
    for first in range(0, pairs, bunch):
        ends = scan(first, [jnp.zeros((SEGS, LANES), F32)] * (2 * bunch), False)
        for i in range(bunch):
            q = first + i
            fin = row(FIN, q)
            h_r, h_i = ends[2 * i] * fin, ends[2 * i + 1] * fin
            for d, kind in enumerate((ONE, TWO, FOUR)):
                hop = 1 << d
                weight = jnp.where(sub >= hop, row(kind, q), 0.0)
                a_r, a_i = cmul(
                    pltpu.roll(h_r, hop, 0), pltpu.roll(h_i, hop, 0),
                    wide(base, 2 + 2 * d, q), wide(base, 3 + 2 * d, q),
                )
                h_r, h_i = h_r + weight * a_r, h_i + weight * a_i
            carried[0, q : q + 1, :] = h_r[SEGS - 1 :]
            carried[1, q : q + 1, :] = h_i[SEGS - 1 :]
            ref = row(REF, q)
            entry[0, q] = jnp.where(sub >= 1, pltpu.roll(h_r, 1, 0), 0.0) * ref
            entry[1, q] = jnp.where(sub >= 1, pltpu.roll(h_i, 1, 0), 0.0) * ref

    blocks = rows // WINDOW
    group_size = Q_HEADS // KV_HEADS
    tile_heads = TILE // HEAD_DIM
    q_index = lax.broadcasted_iota(jnp.int32, (WINDOW, 2 * WINDOW), 0)
    k_index = lax.broadcasted_iota(jnp.int32, (WINDOW, 2 * WINDOW), 1)
    distance = WINDOW + q_index - k_index
    in_window = (distance >= 0) & (distance < WINDOW)

    def attend(block):
        here = pl.ds(block * WINDOW, WINDOW)
        band = pl.ds(block * WINDOW, 2 * WINDOW)
        allowed = in_window
        if block == 0:
            allowed = allowed & (k_index >= jnp.where(me == 0, WINDOW, 0))
        key, value = keys[band, :], values[band, :]
        for tile in range(2):
            query = proj[tile, here, :] * jnp.asarray(HEAD_DIM ** -0.5, BF16)
            results = []
            for j in range(tile_heads):
                head_id = tile * tile_heads + j
                kv = head_id // group_size
                k = key[:, kv * HEAD_DIM : (kv + 1) * HEAD_DIM]
                v = value[:, kv * HEAD_DIM : (kv + 1) * HEAD_DIM]
                scores = ntdot(query[:, j * HEAD_DIM : (j + 1) * HEAD_DIM], k)
                scores = jnp.where(allowed, scores, NEG_FILL)
                sink = sink_ref[head_id]
                maxima = jnp.maximum(jnp.max(scores, axis=-1, keepdims=True), sink)
                exponent = jnp.exp(scores - maxima)
                total = jnp.sum(exponent, axis=-1, keepdims=True) + jnp.exp(sink - maxima)
                results.append(ndot(exponent.astype(BF16), v) * (1.0 / total))
            gate = jax.nn.sigmoid(proj[2 + tile, here, :].astype(F32))
            head[here, pl.ds(tile * TILE, TILE)] = (gate * jnp.concatenate(results, axis=1)).astype(BF16)

    def last_part():
        for copy in weights[4:]:
            copy.wait()
        gates = [project(w2[4 + c]) for c in range(2)]
        for c in range(2):
            gate_ref[:, c * TILE : (c + 1) * TILE] = ndot(permute[...], gates[c]).astype(BF16)

    @pl.when(me == 0)
    def _():
        keys[:WINDOW, :] = jnp.zeros((WINDOW, keys.shape[1]), BF16)
        values[:WINDOW, :] = jnp.zeros((WINDOW, values.shape[1]), BF16)

    near_me[:pairs, :] = carried[0].astype(BF16)
    near_me[pairs : 2 * pairs, :] = carried[1].astype(BF16)

    def to_near(target):
        return pltpu.make_async_remote_copy(
            src_ref=near_me, dst_ref=near_me, send_sem=near_send.at[target], recv_sem=near_recv.at[mine],
            device_id={"sp": plane * inner + target}, device_id_type=MESH,
        )

    def from_near(source):
        return pltpu.make_async_remote_copy(
            src_ref=near_me, dst_ref=near.at[source], send_sem=near_send.at[source], recv_sem=near_recv.at[source],
            device_id={"sp": plane * inner + source}, device_id_type=MESH,
        )

    pl.semaphore_wait(barrier, signals)
    for hop in range(1, inner):
        to_near(lax.rem(mine + hop, inner)).start()

    crowded = mine == inner - 1
    pl.when(jnp.logical_not(crowded))(send_halos)
    for copy in weights[:4] + small[:1]:
        copy.wait()
    for n in range(4):
        proj[n] = project(w2[n])
    pl.when(crowded)(send_halos)
    for block in range(1, blocks):
        attend(block)

    for copy in small[1:4]:
        copy.wait()
    wout[...] = ndot(shrunk[...], spread[...])
    lanes_of = lax.broadcasted_iota(jnp.int32, (GROUP_CH, groups * GROUP_CH), 1) % GROUP_CH
    channel = lax.broadcasted_iota(jnp.int32, (GROUP_CH, groups * GROUP_CH), 0)
    skips = sum(ndot(piece, spread[:groups, :]) for piece in split(skip[...], 3))
    skip_row[...] = jnp.broadcast_to(
        jnp.sum(jnp.where(lanes_of == channel, skips, 0.0), axis=0, keepdims=True), skip_row.shape
    )
    row_low = lax.broadcasted_iota(jnp.int32, (2 * GROUP_CH, LANES), 0) < GROUP_CH
    lane_low = lax.broadcasted_iota(jnp.int32, (2 * GROUP_CH, LANES), 1) < LANES // 2
    own_lane = row_low == lane_low
    zero = jnp.zeros((LANES, TILE), BF16)
    for q in range(pairs):
        pick = lambda ref: jnp.concatenate([
            jnp.concatenate([ref[2 * q], ref[2 * q]], axis=1),
            jnp.concatenate([ref[2 * q + 1], ref[2 * q + 1]], axis=1),
        ], axis=0)
        readout[q] = zero
        readout[q, pl.ds((q % pairs_tile) * 2 * GROUP_CH, 2 * GROUP_CH), :] = jnp.concatenate(
            [jnp.where(own_lane, pick(orr), 0.0), jnp.where(own_lane, -pick(oi), 0.0)], axis=1
        ).astype(BF16)

    def near_arrive():
        for hop in range(1, inner):
            from_near(lax.rem(mine + hop, inner)).wait_recv()

    far_me = far.at[plane]

    @pl.when(me == 0)
    def _():
        before[...] = jnp.zeros(before.shape, F32)

    @pl.when(me > 0)
    def _():
        near_arrive()

        block_r, block_i = base[8], base[9]
        agg_r = agg_i = jnp.zeros((pairs, LANES), F32)
        agg_s = jnp.zeros((1, LANES), F32)
        pw_r, pw_i = jnp.ones((pairs, LANES), F32), jnp.zeros((pairs, LANES), F32)
        pre = [agg_r, agg_i, agg_s, pw_r, pw_i]
        for i in range(inner):
            now = [agg_r, agg_i, agg_s, pw_r, pw_i]
            if i > 0:
                pre = [jnp.where(mine == i, a, b) for a, b in zip(now, pre)]
            shift_i = unpack_shift(near[i, 2 * pairs :, :])
            a_r, a_i = cmul(agg_r, agg_i, block_r, block_i)
            factor = jnp.exp(per_pair(shift_i, pairs))
            agg_r = factor * a_r + near[i, :pairs, :].astype(F32)
            agg_i = factor * a_i + near[i, pairs : 2 * pairs, :].astype(F32)
            agg_s = agg_s + shift_i
            pw_r, pw_i = cmul(pw_r, pw_i, block_r, block_i)
        far_me[:pairs, :] = agg_r.astype(BF16)
        far_me[pairs : 2 * pairs, :] = agg_i.astype(BF16)
        far_me[2 * pairs :, :] = pack_shift(jnp.broadcast_to(agg_s, (SEGS, LANES)))
        scale = jnp.exp(per_pair(pre[2], pairs))
        for k, value in enumerate((pre[0], pre[1], scale * pre[3], scale * pre[4], pw_r, pw_i)):
            before[k] = value

    def to_far(target, place, sem):
        return pltpu.make_async_remote_copy(
            src_ref=far_me, dst_ref=far_me, send_sem=sem.at[target], recv_sem=far_recv.at[plane],
            device_id={"sp": target * inner + place}, device_id_type=MESH,
        )

    def far_sends(act):
        for target in range(1, outer):
            @pl.when((plane < target) & (me > 0))
            def _():
                act(to_far(target, mine, far_send))

            @pl.when(me == 1)
            def _():
                act(to_far(target, 0, first_send))

    def from_far(source):
        return pltpu.make_async_remote_copy(
            src_ref=far_me, dst_ref=far.at[source], send_sem=far_send.at[source], recv_sem=far_recv.at[source],
            device_id={"sp": source * inner + mine}, device_id_type=MESH,
        )

    for q in range(pairs):
        spot = pl.ds(q * SEGS, SEGS)
        scale = row(PRE, q) * row(REF, q)
        init[0, q] = power[0, spot, :] * scale
        init[1, q] = power[1, spot, :] * scale

    far_sends(lambda copy: copy.start())
    for copy in crossing:
        copy.start()

    last_part()

    def first_block():
        @pl.when(me > 0)
        def _():
            for copy in halos(me):
                copy.wait_recv()

        attend(0)

    def head_out():
        head_cross.start()
        for piece in range(pieces):
            acc[piece] = ndot(head[...], how[:, part_of(piece)])

    for copy in small[4:]:
        copy.wait()
    part_of = lambda piece: pl.ds(piece * step, step)

    soon = (lax.rem(me, 2) == 1) | (me == 0)

    @pl.when(soon)
    def _():
        first_block()
        head_out()

    carry_r = carry_i = jnp.zeros((pairs, LANES), F32)
    for z in range(outer - 1):
        @pl.when(z < plane)
        def _():
            from_far(z).wait_recv()

    for z in range(outer - 1):
        factor = jnp.exp(per_pair(unpack_shift(far[z, 2 * pairs :, :]), pairs))
        a_r, a_i = cmul(carry_r, carry_i, before[4], before[5])
        carry_r = jnp.where(z < plane, factor * a_r + far[z, :pairs, :].astype(F32), carry_r)
        carry_i = jnp.where(z < plane, factor * a_i + far[z, pairs : 2 * pairs, :].astype(F32), carry_i)
    in_r, in_i = cmul(carry_r, carry_i, before[2], before[3])
    carried[0], carried[1] = in_r + before[0], in_i + before[1]
    for first in range(0, pairs, bunch):
        start = []
        for i in range(bunch):
            q = first + i
            s_r, s_i = cmul(init[0, q], init[1, q], wide(carried, 0, q), wide(carried, 1, q))
            start += [entry[0, q] + s_r, entry[1, q] + s_i]
        scan(first, start, True)
    for tile in range(tiles):
        lanes = pl.ds(tile * LANES, LANES)
        seen = sum(
            ntdot(states_ref[q], readout[q]) for q in range(tile * pairs_tile, (tile + 1) * pairs_tile)
        )
        recurrent = wout[:, lanes] * seen + skip_row[:1, lanes] * u_ref[:, lanes].astype(F32)
        gate = jax.nn.sigmoid(gate_ref[:, lanes].astype(F32))
        mixed[:, lanes] = (gate * jax.nn.gelu(recurrent)).astype(BF16)
    state[...] = ndot(back[...], mixed[...]).astype(BF16)
    state_cross.start()

    @pl.when(jnp.logical_not(soon))
    def _():
        first_block()
        head_out()

    for piece in range(pieces):
        acc[piece] += ndot(state[...], sow[:, part_of(piece)])
    for copy in crossing:
        copy.wait()
    pl.when(me == 0)(near_arrive)
    for hop in range(1, inner):
        to_near(lax.rem(mine + hop, inner)).wait_send()
    far_sends(lambda copy: copy.wait_send())

    @pl.when(me < count - 1)
    def _():
        for copy in halos(me + 1):
            copy.wait_send()
    head_cross.wait()
    state_cross.wait()


def close_kernel(acc, state_x, sow_x, head_x, how_x, out_ref, stage, sem):
    pieces, _, step = acc.shape
    copies = [
        pltpu.make_async_copy(stage.at[piece], out_ref.at[:, pl.ds(piece * step, step)], sem.at[piece])
        for piece in range(pieces)
    ]
    for piece in range(pieces):
        lanes = pl.ds(piece * step, step)
        stage[piece] = (
            acc[piece] + ndot(head_x[...], how_x[:, lanes]) + ndot(state_x[...], sow_x[:, lanes])
        ).astype(BF16)
        copies[piece].start()
    for copy in copies:
        copy.wait()


def on_device(
    hidden, query_weight, key_weight, value_weight, head_gate_weight, state_in_weight, state_gate_weight,
    sink_logit, decay_real, decay_frequency, log_step, input_real, input_imaginary, output_real,
    output_imaginary, skip_weight, decay_shift, head_out_weight, state_out_weight,
):
    rows, half = hidden.shape
    groups, states = decay_real.shape
    pairs = groups // 2
    channels = groups * GROUP_CH
    count = lax.axis_size("sp")
    inner = 1 << (count.bit_length() // 2)
    outer = count // inner
    permute, back, running, sums, spread, widen = constants(rows, groups, states)
    width = head_out_weight.shape[1] // 2
    pieces = 4
    like = lambda v: pltpu.VMEM(v.shape, v.dtype)
    pin = lambda v: pltpu.with_memory_space_constraint(v, pltpu.HBM)
    shaped = jax.ShapeDtypeStruct
    dma = pltpu.SemaphoreType.DMA
    mib = 1024 * 1024
    small = (
        decay_real, decay_frequency, log_step.reshape(1, groups), decay_shift, running, sums, spread, widen,
        input_real.transpose(0, 2, 1), input_imaginary.transpose(0, 2, 1), permute,
    )
    late = (output_real, output_imaginary, skip_weight.T)
    first_tiles = (state_in_weight.shape[1] + key_weight.shape[1] + value_weight.shape[1]) // TILE
    prepared = (
        shaped((2, rows, half), BF16),
        shaped((first_tiles, 2 * half, TILE), BF16),
        shaped((pairs, LANES, TILE), BF16),
        shaped((rows, channels), F32),
        shaped((rows, 2 * groups), BF16),
        shaped((10, pairs, LANES), F32),
        shaped((2, pairs * SEGS, LANES), F32),
        shaped((7 * SEGS, groups * states), F32),
        shaped((SEGS, LANES), F32),
        shaped(permute.shape, BF16),
        shaped(spread.shape, BF16),
    )
    ready = pl.pallas_call(
        prepare_kernel,
        out_shape=prepared,
        in_specs=[ANY] * (4 + len(small)),
        out_specs=(VMEM,) * len(prepared),
        scratch_shapes=[
            *[like(v) for v in small if v is not permute and v is not spread],
            pltpu.VMEM((2, pairs, LANES), F32),
            dma((1 + len(small),)), dma((first_tiles,)), dma, dma,
        ],
        compiler_params=pltpu.CompilerParams(
            vmem_limit_bytes=PREP_MIB * mib, collective_id=0, has_side_effects=True
        ),
        name="prepare",
    )(*map(pin, (hidden, state_in_weight, key_weight, value_weight, *small)))
    closing = pl.pallas_call(
        layer_kernel,
        out_shape=(
            shaped((pieces, rows, width // pieces), F32),
            shaped((rows, channels), BF16),
            shaped((state_out_weight.shape[0], width), BF16),
            shaped((rows, head_out_weight.shape[0]), BF16),
            shaped((head_out_weight.shape[0], width), BF16),
        ),
        in_specs=[VMEM] * len(prepared) + [ANY] * (7 + len(late)),
        out_specs=(VMEM,) * 5,
        scratch_shapes=[
            pltpu.VMEM((6, 2 * half, TILE), BF16),
            *[pltpu.VMEM((head_out_weight.shape[0], width), BF16)] * 2,
            like(back),
            pltpu.SMEM(sink_logit.shape, F32),
            *[like(v) for v in late],
            pltpu.VMEM((pairs, LANES, TILE), BF16),
            pltpu.VMEM((rows, channels), F32),
            pltpu.VMEM((SEGS, channels), F32),
            pltpu.VMEM((pairs, rows, TILE), F32),
            pltpu.VMEM((pairs, rows, TILE), BF16),
            pltpu.VMEM((rows, channels), BF16),
            pltpu.VMEM((rows, channels), BF16),
            pltpu.VMEM((2, pairs, LANES), F32),
            pltpu.VMEM((6, pairs, LANES), F32),
            pltpu.VMEM((2, pairs, SEGS, LANES), F32),
            pltpu.VMEM((2, pairs, SEGS, LANES), F32),
            pltpu.VMEM((4, rows, TILE), BF16),
            pltpu.VMEM((WINDOW + rows, TILE), BF16),
            pltpu.VMEM((WINDOW + rows, TILE), BF16),
            *[pltpu.VMEM((rows, channels), BF16)] * 3,
            pltpu.VMEM((inner, 2 * pairs + 2 * SEGS, LANES), BF16),
            pltpu.VMEM((outer, 2 * pairs + 2 * SEGS, LANES), BF16),
            dma((7,)), dma((6,)), dma((inner,)), dma((inner,)), *[dma((outer,))] * 3,
            dma((2,)), dma((2,)), dma((4,)), dma((4,)),
        ],
        compiler_params=pltpu.CompilerParams(
            vmem_limit_bytes=LAYER_MIB * mib, collective_id=1, has_side_effects=True
        ),
        name="layer",
    )(
        *ready,
        *map(pin, (
            query_weight, head_gate_weight, state_gate_weight, sink_logit, head_out_weight, state_out_weight,
            back, *late,
        )),
    )
    return pl.pallas_call(
        close_kernel,
        out_shape=shaped((rows, width), BF16),
        in_specs=[VMEM] * 5,
        out_specs=ANY,
        scratch_shapes=[pltpu.VMEM((pieces, rows, width // pieces), BF16), dma((pieces,))],
        compiler_params=pltpu.CompilerParams(vmem_limit_bytes=CLOSE_MIB * mib),
        name="close",
    )(*closing)


def solution(mesh):
    in_specs = (
        P("sp", "tp"),
        P(None, "tp"),
        P(None, "tp"),
        P(None, "tp"),
        P(None, "tp"),
        P(None, "tp"),
        P(None, "tp"),
        P("tp"),
        P("tp", None),
        P("tp", None),
        P("tp"),
        P("tp", None, None),
        P("tp", None, None),
        P("tp", None, None),
        P("tp", None, None),
        P("tp", None),
        P("tp", "sp"),
        P("tp", None),
        P("tp", None),
    )
    out_specs = P("sp", "tp")
    return jax.shard_map(
        on_device, mesh=mesh, in_specs=in_specs, out_specs=out_specs, check_vma=False
    )
```

```python
import jax
import jax.numpy as jnp
import numpy as np
from jax import lax
from jax.experimental import pallas as pl
from jax.experimental.pallas import tpu as pltpu
from jax.sharding import PartitionSpec as P

HEAD_DIM = 64
Q_HEADS = 16
KV_HEADS = 8
GROUP_CH = 16
WINDOW = 128
LANES = 128
SEGS = 8
TILE = 256

PREP_MIB, LAYER_MIB, CLOSE_MIB = 12, 36, 6

NEG_FILL = -1e30
MESH = pl.DeviceIdType.MESH
ANY = pl.BlockSpec(memory_space=pl.ANY)
VMEM = pl.BlockSpec(memory_space=pltpu.VMEM)
SMEM = pl.BlockSpec(memory_space=pltpu.SMEM)
BF16 = jnp.bfloat16
F32 = jnp.float32
NT = (((1,), (1,)), ((), ()))


def split(value, pieces):
    out = []
    for _ in range(pieces):
        high = value.astype(BF16)
        out.append(high)
        value = value - high.astype(F32)
    return out


def ndot(a, b):
    return jnp.dot(a, b, preferred_element_type=F32)


def ntdot(a, b):
    return lax.dot_general(a, b, NT, preferred_element_type=F32)


def cmul(ar, ai, br, bi):
    return ar * br - ai * bi, ar * bi + ai * br


REF, FIN, PRE, ONE, TWO, FOUR, ALL = range(7)


def constants(rows, groups, states):
    length = rows // SEGS
    time = np.arange(rows)
    seg, pos = time // length, time % length
    order = (time % SEGS) * length + time // SEGS
    permute = (order[:, None] == time[None]).astype(np.float32)
    same = seg[order][:, None] == seg[None]
    upto = (order[:, None] >= time[None]).astype(np.float32)
    first = (pos < length // 2).astype(np.float32)[None]
    running = same * (upto - first)
    k = np.arange(SEGS)[:, None]
    here = seg[None] == k
    sums = np.concatenate(
        [
            here * first,
            here * (1 - first),
            seg[None] < k,
            here,
            (seg[None] <= k) & (seg[None] > k - 2),
            (seg[None] <= k) & (seg[None] > k - 4),
            np.ones((SEGS, rows)),
        ],
        axis=0,
    ).astype(np.float32)
    column = np.arange(groups * GROUP_CH) // GROUP_CH
    spread = (np.arange(groups)[:, None] == column[None]).astype(np.float32)
    lane = np.arange(groups * states) // states
    widen = (np.arange(groups)[:, None] == lane[None]).astype(np.float32)
    make = lambda x: jnp.asarray(x, BF16)
    return (
        make(permute), make(permute.T), make(running), make(sums),
        make(np.concatenate([spread, spread], axis=0)), make(np.concatenate([widen] * 3, axis=0)),
    )


def per_pair(row, pairs):
    spots = row.shape[1]
    wide = jnp.broadcast_to(row, (pairs, spots))
    r = lax.broadcasted_iota(jnp.int32, (pairs, spots), 0)
    c = lax.broadcasted_iota(jnp.int32, (pairs, spots), 1)
    even = jnp.sum(jnp.where(c == 2 * r, wide, 0.0), axis=1, keepdims=True)
    odd = jnp.sum(jnp.where(c == 2 * r + 1, wide, 0.0), axis=1, keepdims=True)
    low = lax.broadcasted_iota(jnp.int32, (pairs, LANES), 1) < LANES // 2
    return jnp.where(low, even, odd)


def fetch_all(pairs_of, sems, first=0):
    return [pltpu.make_async_copy(src, dst, sems.at[first + i]) for i, (src, dst) in enumerate(pairs_of)]


def pack_shift(rows):
    high, low = split(rows, 2)
    return jnp.concatenate([high, low], axis=0)


def unpack_shift(packed):
    wide = packed.astype(F32)
    return wide[:1] + wide[SEGS : SEGS + 1]


def prepare_kernel(
    hidden_ref, wsi_ref, wk_ref, wv_ref, dr_in, df_in, ls_in, shift_in, running_in, sums_in, spread_in, widen_in,
    ir_in, ii_in, permute_in,
    x, w, drive, win, shrunk, base, power, table, shift_rows, permute, spread,
    dr, df, ls, shift, running, sums, widen, ir, ii, zoh,
    in_sem, w_sem, x_send, x_recv,
):
    tp = lax.axis_index("tp")
    other = 1 - tp
    pairs = drive.shape[0]
    groups = 2 * pairs
    rows = win.shape[0]
    length = rows // SEGS
    pairs_tile = LANES // GROUP_CH // 2
    barrier = pltpu.get_barrier_semaphore()
    pl.semaphore_signal(barrier, inc=1, device_id={"tp": other}, device_id_type=MESH)
    own_x = pltpu.make_async_copy(hidden_ref, x.at[tp], in_sem.at[0])
    own_x.start()
    small = fetch_all((
        (dr_in, dr), (df_in, df), (ls_in, ls), (shift_in, shift), (running_in, running), (sums_in, sums),
        (spread_in, spread), (widen_in, widen), (ir_in, ir), (ii_in, ii), (permute_in, permute),
    ), in_sem, 1)
    for copy in small:
        copy.start()
    columns = [
        (ref.at[:, pl.ds(c * TILE, TILE)], w.at[i + c])
        for ref, i in ((wsi_ref, 0), (wk_ref, 2), (wv_ref, 3)) for c in range(ref.shape[1] // TILE)
    ]
    weights = fetch_all(columns, w_sem)
    for copy in weights:
        copy.start(priority=1)
    zero = jnp.zeros((LANES, TILE), BF16)
    for q in range(pairs):
        drive[q] = zero

    pl.semaphore_wait(barrier, 1)
    own_x.wait()
    swap = pltpu.make_async_remote_copy(
        src_ref=x.at[tp], dst_ref=x.at[tp], send_sem=x_send, recv_sem=x_recv,
        device_id={"tp": other}, device_id_type=MESH,
    )
    swap.start()

    for copy in small[:7]:
        copy.wait()
    two = lambda ref: jnp.concatenate(
        [ref[pl.ds(0, pairs, stride=2), :], ref[pl.ds(1, pairs, stride=2), :]], axis=1
    )
    decay, frequency = two(dr), two(df)
    stepsize = jnp.exp(per_pair(ls[...], pairs))
    magnitude = jnp.exp(decay * stepsize)
    rotation = frequency * stepsize
    base_r, base_i = magnitude * jnp.cos(rotation), magnitude * jnp.sin(rotation)
    denominator = decay * decay + frequency * frequency
    less = base_r - 1.0
    zoh[0] = (less * decay + base_i * frequency) / denominator
    zoh[1] = (base_i * decay - less * frequency) / denominator
    base[0], base[1] = base_r, base_i
    power_r, power_i = base_r, base_i
    for _ in range(length.bit_length() - 1):
        power_r, power_i = cmul(power_r, power_i, power_r, power_i)
    for d in range(4):
        base[2 + 2 * d], base[3 + 2 * d] = power_r, power_i
        if d == 0:
            step_r, step_i = power_r, power_i
        power_r, power_i = cmul(power_r, power_i, power_r, power_i)
    run_r, run_i = jnp.ones_like(base_r), jnp.zeros_like(base_r)
    for k in range(SEGS):
        spot = pl.ds(k, pairs, stride=SEGS)
        power[0, spot, :] = run_r
        power[1, spot, :] = run_i
        run_r, run_i = cmul(run_r, run_i, step_r, step_i)

    shifts = split(shift[...], 3)
    relative = sum(ntdot(running[...], piece) for piece in shifts)
    totals = sum(ntdot(sums[...], piece) for piece in shifts)
    grown = jnp.concatenate(split(jnp.exp(-relative), 2), axis=1)
    shrunk[...] = jnp.concatenate(split(jnp.exp(relative), 2), axis=1)
    win[...] = ndot(grown, spread[...])
    shift_rows[...] = jnp.concatenate(
        [totals[ALL * SEGS : (ALL + 1) * SEGS], jnp.zeros((SEGS, LANES - groups), F32)], axis=1
    )
    scales = jnp.concatenate(split(jnp.exp(totals), 3), axis=1)
    for copy in small[7:]:
        copy.wait()
    table[...] = ndot(scales, widen[...])

    row_low = lax.broadcasted_iota(jnp.int32, (2 * GROUP_CH, LANES), 0) < GROUP_CH
    lane_low = lax.broadcasted_iota(jnp.int32, (2 * GROUP_CH, LANES), 1) < LANES // 2
    own_lane = row_low == lane_low
    for q in range(pairs):
        pick = lambda ref: jnp.concatenate([
            jnp.concatenate([ref[2 * q], ref[2 * q]], axis=1),
            jnp.concatenate([ref[2 * q + 1], ref[2 * q + 1]], axis=1),
        ], axis=0)
        spot = pl.ds((q % pairs_tile) * 2 * GROUP_CH, 2 * GROUP_CH)
        in_r, in_i = pick(ir), pick(ii)
        z_r, z_i = zoh[0, q : q + 1, :], zoh[1, q : q + 1, :]
        d_r, d_i = cmul(z_r, z_i, in_r, in_i)
        drive[q, spot, :] = jnp.concatenate(
            [jnp.where(own_lane, d_r, 0.0), jnp.where(own_lane, d_i, 0.0)], axis=1
        ).astype(BF16)
    swap.wait()
    for copy in weights:
        copy.wait()


def layer_kernel(
    x, w, drive, win, shrunk, base, power, table, shift_rows, permute, spread,
    wq_ref, wg_ref, wsg_ref, sink_in, how_ref, sow_ref, back_in, or_in, oi_in, skip_in,
    acc, state_x, sow_x, head_x, how_x,
    w2, how, sow, back, sink_ref, orr, oi, skip, readout, wout, skip_row,
    pushed, states_ref, u_ref, gate_ref, carried, before, entry, init,
    proj, keys, values, mixed, head, state, near, far,
    in_sem, w_sem, near_send, near_recv, far_send, first_send, far_recv, halo_send, halo_recv, x_send, x_recv,
):
    tp = lax.axis_index("tp")
    other = 1 - tp
    me = lax.axis_index("sp")
    count = lax.axis_size("sp")
    inner, outer = near.shape[0], far.shape[0]
    mine, plane = lax.rem(me, inner), lax.div(me, inner)
    rows, half_width = x.shape[1:]
    pairs = drive.shape[0]
    groups = 2 * pairs
    length = rows // SEGS
    per_tile = LANES // GROUP_CH
    tiles = groups // per_tile
    pairs_tile = per_tile // 2

    barrier = pltpu.get_barrier_semaphore()
    for hop in range(1, inner):
        target = plane * inner + lax.rem(mine + hop, inner)
        pl.semaphore_signal(barrier, inc=1, device_id={"sp": target}, device_id_type=MESH)

    @pl.when(me > 0)
    def _():
        for hop in range(1, outer):
            target = lax.rem(plane + hop, outer) * inner + mine
            target = jnp.where(target == 0, 2, target)
            pl.semaphore_signal(barrier, inc=1, device_id={"sp": target}, device_id_type=MESH)
        pl.semaphore_signal(barrier, inc=1, device_id={"sp": me - 1}, device_id_type=MESH)

    pl.semaphore_signal(barrier, inc=1, device_id={"tp": other}, device_id_type=MESH)

    pieces, _, step = acc.shape
    width = pieces * step
    half_of = lambda ref, owner: ref.at[:, pl.ds(pl.multiple_of(owner * width, LANES), width)]
    small = fetch_all((
        (sink_in, sink_ref), (or_in, orr), (oi_in, oi), (skip_in, skip), (back_in, back),
        (half_of(how_ref, tp), how), (half_of(sow_ref, tp), sow),
    ), in_sem)
    columns = [
        (ref.at[:, pl.ds(c * TILE, TILE)], w2.at[2 * i + c])
        for i, ref in enumerate((wq_ref, wg_ref, wsg_ref)) for c in range(2)
    ]
    weights = fetch_all(columns, w_sem)
    for copy in small[:5] + weights + small[5:]:
        copy.start()

    def cross(k, src, dst):
        return pltpu.make_async_remote_copy(
            src_ref=src, dst_ref=dst, send_sem=x_send.at[k], recv_sem=x_recv.at[k],
            device_id={"tp": other}, device_id_type=MESH,
        )

    crossing = [cross(0, half_of(how_ref, other), how_x), cross(1, half_of(sow_ref, other), sow_x)]
    head_cross, state_cross = cross(2, head, head_x), cross(3, state, state_x)

    def project(block):
        return (ndot(x[0], block[:half_width, :]) + ndot(x[1], block[half_width:, :])).astype(BF16)

    own_rows = pl.ds(WINDOW, rows)
    keys[own_rows, :] = project(w[2])
    values[own_rows, :] = project(w[3])
    fed = [project(w[c]) for c in range(2)]

    def halos(target):
        return [
            pltpu.make_async_remote_copy(
                src_ref=band.at[pl.ds(rows, WINDOW)], dst_ref=band.at[pl.ds(0, WINDOW)],
                send_sem=halo_send.at[k], recv_sem=halo_recv.at[k],
                device_id={"sp": target}, device_id_type=MESH,
            )
            for k, band in enumerate((keys, values))
        ]

    signals = inner + jnp.where(me < count - 1, 1, 0) + jnp.where(me > 0, outer - 2, 0)
    signals = signals + jnp.where(mine > 0, 1, 0) + jnp.where(me == 2, outer - 1, 0)

    def send_halos():
        @pl.when(me < count - 1)
        def _():
            for copy in halos(me + 1):
                copy.start()

    us = [ndot(permute[...], part) for part in fed]
    for c in range(2):
        lanes = pl.ds(c * TILE, TILE)
        u_ref[:, lanes] = us[c].astype(BF16)
        weighted = (us[c] * win[:, lanes]).astype(BF16)
        for t in range(TILE // LANES):
            tile = c * (TILE // LANES) + t
            part = weighted[:, t * LANES : (t + 1) * LANES]
            for i in range(pairs_tile):
                q = tile * pairs_tile + i
                pushed[q] = ndot(part, drive[q])

    bunch = 8

    def wide(ref, index, q):
        return jnp.broadcast_to(ref[index, q : q + 1, :], (SEGS, LANES))

    def scan(first, start, keep):
        br = [wide(base, 0, first + i) for i in range(bunch)]
        bi = [wide(base, 1, first + i) for i in range(bunch)]

        def steps(jj, carry):
            carry = list(carry)
            kept = [[] for _ in range(2 * bunch)]
            for sub in range(2):
                spot = pl.ds(pl.multiple_of((2 * jj + sub) * SEGS, SEGS), SEGS)
                for i in range(bunch):
                    r, m = carry[2 * i], carry[2 * i + 1]
                    p = pushed[first + i, spot, :]
                    new_r = br[i] * r - bi[i] * m + p[:, :LANES]
                    new_m = br[i] * m + bi[i] * r + p[:, LANES:]
                    carry[2 * i], carry[2 * i + 1] = new_r, new_m
                    kept[2 * i].append(new_r)
                    kept[2 * i + 1].append(new_m)
            if keep:
                spot = pl.ds(pl.multiple_of(jj * 2 * SEGS, 2 * SEGS), 2 * SEGS)
                for i in range(bunch):
                    for part in range(2):
                        value = jnp.concatenate(kept[2 * i + part], axis=0).astype(BF16)
                        states_ref[first + i, spot, pl.ds(part * LANES, LANES)] = value
            return tuple(carry)

        return lax.fori_loop(0, length // 2, steps, tuple(start), unroll=2)

    def row(kind, q):
        return table[kind * SEGS : (kind + 1) * SEGS, q * LANES : (q + 1) * LANES]

    sub = lax.broadcasted_iota(jnp.int32, (SEGS, LANES), 0)
    near_me = near.at[mine]
    near_me[2 * pairs :, :] = pack_shift(shift_rows[...])
    for first in range(0, pairs, bunch):
        ends = scan(first, [jnp.zeros((SEGS, LANES), F32)] * (2 * bunch), False)
        for i in range(bunch):
            q = first + i
            fin = row(FIN, q)
            h_r, h_i = ends[2 * i] * fin, ends[2 * i + 1] * fin
            for d, kind in enumerate((ONE, TWO, FOUR)):
                hop = 1 << d
                weight = jnp.where(sub >= hop, row(kind, q), 0.0)
                a_r, a_i = cmul(
                    pltpu.roll(h_r, hop, 0), pltpu.roll(h_i, hop, 0),
                    wide(base, 2 + 2 * d, q), wide(base, 3 + 2 * d, q),
                )
                h_r, h_i = h_r + weight * a_r, h_i + weight * a_i
            carried[0, q : q + 1, :] = h_r[SEGS - 1 :]
            carried[1, q : q + 1, :] = h_i[SEGS - 1 :]
            ref = row(REF, q)
            entry[0, q] = jnp.where(sub >= 1, pltpu.roll(h_r, 1, 0), 0.0) * ref
            entry[1, q] = jnp.where(sub >= 1, pltpu.roll(h_i, 1, 0), 0.0) * ref

    blocks = rows // WINDOW
    group_size = Q_HEADS // KV_HEADS
    tile_heads = TILE // HEAD_DIM
    q_index = lax.broadcasted_iota(jnp.int32, (WINDOW, 2 * WINDOW), 0)
    k_index = lax.broadcasted_iota(jnp.int32, (WINDOW, 2 * WINDOW), 1)
    distance = WINDOW + q_index - k_index
    in_window = (distance >= 0) & (distance < WINDOW)

    def attend(block):
        here = pl.ds(block * WINDOW, WINDOW)
        band = pl.ds(block * WINDOW, 2 * WINDOW)
        allowed = in_window
        if block == 0:
            allowed = allowed & (k_index >= jnp.where(me == 0, WINDOW, 0))
        key, value = keys[band, :], values[band, :]
        for tile in range(2):
            query = proj[tile, here, :] * jnp.asarray(HEAD_DIM ** -0.5, BF16)
            results = []
            for j in range(tile_heads):
                head_id = tile * tile_heads + j
                kv = head_id // group_size
                k = key[:, kv * HEAD_DIM : (kv + 1) * HEAD_DIM]
                v = value[:, kv * HEAD_DIM : (kv + 1) * HEAD_DIM]
                scores = ntdot(query[:, j * HEAD_DIM : (j + 1) * HEAD_DIM], k)
                scores = jnp.where(allowed, scores, NEG_FILL)
                sink = sink_ref[head_id]
                maxima = jnp.maximum(jnp.max(scores, axis=-1, keepdims=True), sink)
                exponent = jnp.exp(scores - maxima)
                total = jnp.sum(exponent, axis=-1, keepdims=True) + jnp.exp(sink - maxima)
                results.append(ndot(exponent.astype(BF16), v) * (1.0 / total))
            gate = jax.nn.sigmoid(proj[2 + tile, here, :].astype(F32))
            head[here, pl.ds(tile * TILE, TILE)] = (gate * jnp.concatenate(results, axis=1)).astype(BF16)

    def last_part():
        for copy in weights[4:]:
            copy.wait()
        gates = [project(w2[4 + c]) for c in range(2)]
        for c in range(2):
            gate_ref[:, c * TILE : (c + 1) * TILE] = ndot(permute[...], gates[c]).astype(BF16)

    @pl.when(me == 0)
    def _():
        keys[:WINDOW, :] = jnp.zeros((WINDOW, keys.shape[1]), BF16)
        values[:WINDOW, :] = jnp.zeros((WINDOW, values.shape[1]), BF16)

    near_me[:pairs, :] = carried[0].astype(BF16)
    near_me[pairs : 2 * pairs, :] = carried[1].astype(BF16)

    def to_near(target):
        return pltpu.make_async_remote_copy(
            src_ref=near_me, dst_ref=near_me, send_sem=near_send.at[target], recv_sem=near_recv.at[mine],
            device_id={"sp": plane * inner + target}, device_id_type=MESH,
        )

    def from_near(source):
        return pltpu.make_async_remote_copy(
            src_ref=near_me, dst_ref=near.at[source], send_sem=near_send.at[source], recv_sem=near_recv.at[source],
            device_id={"sp": plane * inner + source}, device_id_type=MESH,
        )

    pl.semaphore_wait(barrier, signals)
    for hop in range(1, inner):
        to_near(lax.rem(mine + hop, inner)).start()

    crowded = mine == inner - 1
    pl.when(jnp.logical_not(crowded))(send_halos)
    for copy in weights[:4] + small[:1]:
        copy.wait()
    for n in range(4):
        proj[n] = project(w2[n])
    pl.when(crowded)(send_halos)
    for block in range(1, blocks):
        attend(block)

    for copy in small[1:4]:
        copy.wait()
    wout[...] = ndot(shrunk[...], spread[...])
    lanes_of = lax.broadcasted_iota(jnp.int32, (GROUP_CH, groups * GROUP_CH), 1) % GROUP_CH
    channel = lax.broadcasted_iota(jnp.int32, (GROUP_CH, groups * GROUP_CH), 0)
    skips = sum(ndot(piece, spread[:groups, :]) for piece in split(skip[...], 3))
    skip_row[...] = jnp.broadcast_to(
        jnp.sum(jnp.where(lanes_of == channel, skips, 0.0), axis=0, keepdims=True), skip_row.shape
    )
    row_low = lax.broadcasted_iota(jnp.int32, (2 * GROUP_CH, LANES), 0) < GROUP_CH
    lane_low = lax.broadcasted_iota(jnp.int32, (2 * GROUP_CH, LANES), 1) < LANES // 2
    own_lane = row_low == lane_low
    zero = jnp.zeros((LANES, TILE), BF16)
    for q in range(pairs):
        pick = lambda ref: jnp.concatenate([
            jnp.concatenate([ref[2 * q], ref[2 * q]], axis=1),
            jnp.concatenate([ref[2 * q + 1], ref[2 * q + 1]], axis=1),
        ], axis=0)
        readout[q] = zero
        readout[q, pl.ds((q % pairs_tile) * 2 * GROUP_CH, 2 * GROUP_CH), :] = jnp.concatenate(
            [jnp.where(own_lane, pick(orr), 0.0), jnp.where(own_lane, -pick(oi), 0.0)], axis=1
        ).astype(BF16)

    def near_arrive():
        for hop in range(1, inner):
            from_near(lax.rem(mine + hop, inner)).wait_recv()

    far_me = far.at[plane]

    @pl.when(me == 0)
    def _():
        before[...] = jnp.zeros(before.shape, F32)

    @pl.when(me > 0)
    def _():
        near_arrive()

        block_r, block_i = base[8], base[9]
        agg_r = agg_i = jnp.zeros((pairs, LANES), F32)
        agg_s = jnp.zeros((1, LANES), F32)
        pw_r, pw_i = jnp.ones((pairs, LANES), F32), jnp.zeros((pairs, LANES), F32)
        pre = [agg_r, agg_i, agg_s, pw_r, pw_i]
        for i in range(inner):
            now = [agg_r, agg_i, agg_s, pw_r, pw_i]
            if i > 0:
                pre = [jnp.where(mine == i, a, b) for a, b in zip(now, pre)]
            shift_i = unpack_shift(near[i, 2 * pairs :, :])
            a_r, a_i = cmul(agg_r, agg_i, block_r, block_i)
            factor = jnp.exp(per_pair(shift_i, pairs))
            agg_r = factor * a_r + near[i, :pairs, :].astype(F32)
            agg_i = factor * a_i + near[i, pairs : 2 * pairs, :].astype(F32)
            agg_s = agg_s + shift_i
            pw_r, pw_i = cmul(pw_r, pw_i, block_r, block_i)
        far_me[:pairs, :] = agg_r.astype(BF16)
        far_me[pairs : 2 * pairs, :] = agg_i.astype(BF16)
        far_me[2 * pairs :, :] = pack_shift(jnp.broadcast_to(agg_s, (SEGS, LANES)))
        scale = jnp.exp(per_pair(pre[2], pairs))
        for k, value in enumerate((pre[0], pre[1], scale * pre[3], scale * pre[4], pw_r, pw_i)):
            before[k] = value

    def to_far(target, place, sem):
        return pltpu.make_async_remote_copy(
            src_ref=far_me, dst_ref=far_me, send_sem=sem.at[target], recv_sem=far_recv.at[plane],
            device_id={"sp": target * inner + place}, device_id_type=MESH,
        )

    def far_sends(act):
        for target in range(1, outer):
            @pl.when(me == 2)
            def _():
                act(to_far(target, 0, first_send))

            @pl.when((plane < target) & (me > 0))
            def _():
                act(to_far(target, mine, far_send))

    def from_far(source):
        return pltpu.make_async_remote_copy(
            src_ref=far_me, dst_ref=far.at[source], send_sem=far_send.at[source], recv_sem=far_recv.at[source],
            device_id={"sp": source * inner + mine}, device_id_type=MESH,
        )

    for q in range(pairs):
        spot = pl.ds(q * SEGS, SEGS)
        scale = row(PRE, q) * row(REF, q)
        init[0, q] = power[0, spot, :] * scale
        init[1, q] = power[1, spot, :] * scale

    far_sends(lambda copy: copy.start())
    for copy in crossing:
        copy.start()

    last_part()

    def first_block():
        @pl.when(me > 0)
        def _():
            for copy in halos(me):
                copy.wait_recv()

        attend(0)

    def head_out():
        head_cross.start()
        for piece in range(pieces):
            acc[piece] = ndot(head[...], how[:, part_of(piece)])

    for copy in small[4:]:
        copy.wait()
    part_of = lambda piece: pl.ds(piece * step, step)

    soon = halo_comes_soon(me)

    @pl.when(soon)
    def _():
        first_block()
        head_out()

    carry_r = carry_i = jnp.zeros((pairs, LANES), F32)
    for z in range(outer - 1):
        @pl.when(z < plane)
        def _():
            from_far(z).wait_recv()

    for z in range(outer - 1):
        factor = jnp.exp(per_pair(unpack_shift(far[z, 2 * pairs :, :]), pairs))
        a_r, a_i = cmul(carry_r, carry_i, before[4], before[5])
        carry_r = jnp.where(z < plane, factor * a_r + far[z, :pairs, :].astype(F32), carry_r)
        carry_i = jnp.where(z < plane, factor * a_i + far[z, pairs : 2 * pairs, :].astype(F32), carry_i)
    in_r, in_i = cmul(carry_r, carry_i, before[2], before[3])
    carried[0], carried[1] = in_r + before[0], in_i + before[1]
    for first in range(0, pairs, bunch):
        start = []
        for i in range(bunch):
            q = first + i
            s_r, s_i = cmul(init[0, q], init[1, q], wide(carried, 0, q), wide(carried, 1, q))
            start += [entry[0, q] + s_r, entry[1, q] + s_i]
        scan(first, start, True)
    for tile in range(tiles):
        lanes = pl.ds(tile * LANES, LANES)
        seen = sum(
            ntdot(states_ref[q], readout[q]) for q in range(tile * pairs_tile, (tile + 1) * pairs_tile)
        )
        recurrent = wout[:, lanes] * seen + skip_row[:1, lanes] * u_ref[:, lanes].astype(F32)
        gate = jax.nn.sigmoid(gate_ref[:, lanes].astype(F32))
        mixed[:, lanes] = (gate * jax.nn.gelu(recurrent)).astype(BF16)
    state[...] = ndot(back[...], mixed[...]).astype(BF16)
    state_cross.start()

    @pl.when(jnp.logical_not(soon))
    def _():
        first_block()
        head_out()

    for piece in range(pieces):
        acc[piece] += ndot(state[...], sow[:, part_of(piece)])
    for copy in crossing:
        copy.wait()

    @pl.when(soon)
    def _():
        head_cross.wait()
        for piece in range(pieces):
            acc[piece] += ndot(head_x[...], how_x[:, part_of(piece)])
        state_cross.wait()

    @pl.when(jnp.logical_not(soon))
    def _():
        state_cross.wait()
        for piece in range(pieces):
            acc[piece] += ndot(state_x[...], sow_x[:, part_of(piece)])
        head_cross.wait()

    pl.when(me == 0)(near_arrive)
    for hop in range(1, inner):
        to_near(lax.rem(mine + hop, inner)).wait_send()
    far_sends(lambda copy: copy.wait_send())

    @pl.when(me < count - 1)
    def _():
        for copy in halos(me + 1):
            copy.wait_send()


def halo_comes_soon(me):
    return (lax.rem(me, 2) == 1) | (me == 0)


def close_kernel(acc, state_x, sow_x, head_x, how_x, out_ref, stage, sem):
    pieces, _, step = acc.shape
    copies = [
        pltpu.make_async_copy(stage.at[piece], out_ref.at[:, pl.ds(piece * step, step)], sem.at[piece])
        for piece in range(pieces)
    ]

    def close(gated, weight):
        for piece in range(pieces):
            stage[piece] = (acc[piece] + ndot(gated[...], weight[:, pl.ds(piece * step, step)])).astype(BF16)
            copies[piece].start()

    soon = halo_comes_soon(lax.axis_index("sp"))
    pl.when(soon)(lambda: close(state_x, sow_x))
    pl.when(jnp.logical_not(soon))(lambda: close(head_x, how_x))
    for copy in copies:
        copy.wait()


def on_device(
    hidden, query_weight, key_weight, value_weight, head_gate_weight, state_in_weight, state_gate_weight,
    sink_logit, decay_real, decay_frequency, log_step, input_real, input_imaginary, output_real,
    output_imaginary, skip_weight, decay_shift, head_out_weight, state_out_weight,
):
    rows, half = hidden.shape
    groups, states = decay_real.shape
    pairs = groups // 2
    channels = groups * GROUP_CH
    count = lax.axis_size("sp")
    inner = 1 << (count.bit_length() // 2)
    outer = count // inner
    permute, back, running, sums, spread, widen = constants(rows, groups, states)
    width = head_out_weight.shape[1] // 2
    pieces = 4
    like = lambda v: pltpu.VMEM(v.shape, v.dtype)
    pin = lambda v: pltpu.with_memory_space_constraint(v, pltpu.HBM)
    shaped = jax.ShapeDtypeStruct
    dma = pltpu.SemaphoreType.DMA
    mib = 1024 * 1024
    small = (
        decay_real, decay_frequency, log_step.reshape(1, groups), decay_shift, running, sums, spread, widen,
        input_real.transpose(0, 2, 1), input_imaginary.transpose(0, 2, 1), permute,
    )
    late = (output_real, output_imaginary, skip_weight.T)
    first_tiles = (state_in_weight.shape[1] + key_weight.shape[1] + value_weight.shape[1]) // TILE
    prepared = (
        shaped((2, rows, half), BF16),
        shaped((first_tiles, 2 * half, TILE), BF16),
        shaped((pairs, LANES, TILE), BF16),
        shaped((rows, channels), F32),
        shaped((rows, 2 * groups), BF16),
        shaped((10, pairs, LANES), F32),
        shaped((2, pairs * SEGS, LANES), F32),
        shaped((7 * SEGS, groups * states), F32),
        shaped((SEGS, LANES), F32),
        shaped(permute.shape, BF16),
        shaped(spread.shape, BF16),
    )
    ready = pl.pallas_call(
        prepare_kernel,
        out_shape=prepared,
        in_specs=[ANY] * (4 + len(small)),
        out_specs=(VMEM,) * len(prepared),
        scratch_shapes=[
            *[like(v) for v in small if v is not permute and v is not spread],
            pltpu.VMEM((2, pairs, LANES), F32),
            dma((1 + len(small),)), dma((first_tiles,)), dma, dma,
        ],
        compiler_params=pltpu.CompilerParams(
            vmem_limit_bytes=PREP_MIB * mib, collective_id=0, has_side_effects=True
        ),
        name="prepare",
    )(*map(pin, (hidden, state_in_weight, key_weight, value_weight, *small)))
    closing = pl.pallas_call(
        layer_kernel,
        out_shape=(
            shaped((pieces, rows, width // pieces), F32),
            shaped((rows, channels), BF16),
            shaped((state_out_weight.shape[0], width), BF16),
            shaped((rows, head_out_weight.shape[0]), BF16),
            shaped((head_out_weight.shape[0], width), BF16),
        ),
        in_specs=[VMEM] * len(prepared) + [ANY] * (7 + len(late)),
        out_specs=(VMEM,) * 5,
        scratch_shapes=[
            pltpu.VMEM((6, 2 * half, TILE), BF16),
            *[pltpu.VMEM((head_out_weight.shape[0], width), BF16)] * 2,
            like(back),
            pltpu.SMEM(sink_logit.shape, F32),
            *[like(v) for v in late],
            pltpu.VMEM((pairs, LANES, TILE), BF16),
            pltpu.VMEM((rows, channels), F32),
            pltpu.VMEM((SEGS, channels), F32),
            pltpu.VMEM((pairs, rows, TILE), F32),
            pltpu.VMEM((pairs, rows, TILE), BF16),
            pltpu.VMEM((rows, channels), BF16),
            pltpu.VMEM((rows, channels), BF16),
            pltpu.VMEM((2, pairs, LANES), F32),
            pltpu.VMEM((6, pairs, LANES), F32),
            pltpu.VMEM((2, pairs, SEGS, LANES), F32),
            pltpu.VMEM((2, pairs, SEGS, LANES), F32),
            pltpu.VMEM((4, rows, TILE), BF16),
            pltpu.VMEM((WINDOW + rows, TILE), BF16),
            pltpu.VMEM((WINDOW + rows, TILE), BF16),
            *[pltpu.VMEM((rows, channels), BF16)] * 3,
            pltpu.VMEM((inner, 2 * pairs + 2 * SEGS, LANES), BF16),
            pltpu.VMEM((outer, 2 * pairs + 2 * SEGS, LANES), BF16),
            dma((7,)), dma((6,)), dma((inner,)), dma((inner,)), *[dma((outer,))] * 3,
            dma((2,)), dma((2,)), dma((4,)), dma((4,)),
        ],
        compiler_params=pltpu.CompilerParams(
            vmem_limit_bytes=LAYER_MIB * mib, collective_id=1, has_side_effects=True
        ),
        name="layer",
    )(
        *ready,
        *map(pin, (
            query_weight, head_gate_weight, state_gate_weight, sink_logit, head_out_weight, state_out_weight,
            back, *late,
        )),
    )
    return pl.pallas_call(
        close_kernel,
        out_shape=shaped((rows, width), BF16),
        in_specs=[VMEM] * 5,
        out_specs=ANY,
        scratch_shapes=[pltpu.VMEM((pieces, rows, width // pieces), BF16), dma((pieces,))],
        compiler_params=pltpu.CompilerParams(vmem_limit_bytes=CLOSE_MIB * mib),
        name="close",
    )(*closing)


def solution(mesh):
    in_specs = (
        P("sp", "tp"),
        P(None, "tp"),
        P(None, "tp"),
        P(None, "tp"),
        P(None, "tp"),
        P(None, "tp"),
        P(None, "tp"),
        P("tp"),
        P("tp", None),
        P("tp", None),
        P("tp"),
        P("tp", None, None),
        P("tp", None, None),
        P("tp", None, None),
        P("tp", None, None),
        P("tp", None),
        P("tp", "sp"),
        P("tp", None),
        P("tp", None),
    )
    out_specs = P("sp", "tp")
    return jax.shard_map(
        on_device, mesh=mesh, in_specs=in_specs, out_specs=out_specs, check_vma=False
    )
```

```python
import jax
import jax.numpy as jnp
import numpy as np
from jax import lax
from jax.experimental import pallas as pl
from jax.experimental.pallas import tpu as pltpu
from jax.sharding import PartitionSpec as P

HEAD_DIM = 64
Q_HEADS = 16
KV_HEADS = 8
GROUP_CH = 16
WINDOW = 128
LANES = 128
SEGS = 8
TILE = 256

PREP_MIB, LAYER_MIB, CLOSE_MIB = 12, 36, 6

NEG_FILL = -1e30
MESH = pl.DeviceIdType.MESH
ANY = pl.BlockSpec(memory_space=pl.ANY)
VMEM = pl.BlockSpec(memory_space=pltpu.VMEM)
SMEM = pl.BlockSpec(memory_space=pltpu.SMEM)
BF16 = jnp.bfloat16
F32 = jnp.float32
NT = (((1,), (1,)), ((), ()))


def split(value, pieces):
    out = []
    for _ in range(pieces):
        high = value.astype(BF16)
        out.append(high)
        value = value - high.astype(F32)
    return out


def ndot(a, b):
    return jnp.dot(a, b, preferred_element_type=F32)


def ntdot(a, b):
    return lax.dot_general(a, b, NT, preferred_element_type=F32)


def cmul(ar, ai, br, bi):
    return ar * br - ai * bi, ar * bi + ai * br


REF, FIN, PRE, ONE, TWO, FOUR, ALL = range(7)


def constants(rows, groups, states):
    length = rows // SEGS
    time = np.arange(rows)
    seg, pos = time // length, time % length
    order = (time % SEGS) * length + time // SEGS
    permute = (order[:, None] == time[None]).astype(np.float32)
    same = seg[order][:, None] == seg[None]
    upto = (order[:, None] >= time[None]).astype(np.float32)
    first = (pos < length // 2).astype(np.float32)[None]
    running = same * (upto - first)
    k = np.arange(SEGS)[:, None]
    here = seg[None] == k
    sums = np.concatenate(
        [
            here * first,
            here * (1 - first),
            seg[None] < k,
            here,
            (seg[None] <= k) & (seg[None] > k - 2),
            (seg[None] <= k) & (seg[None] > k - 4),
            np.ones((SEGS, rows)),
        ],
        axis=0,
    ).astype(np.float32)
    column = np.arange(groups * GROUP_CH) // GROUP_CH
    spread = (np.arange(groups)[:, None] == column[None]).astype(np.float32)
    lane = np.arange(groups * states) // states
    widen = (np.arange(groups)[:, None] == lane[None]).astype(np.float32)
    make = lambda x: jnp.asarray(x, BF16)
    return (
        make(permute), make(permute.T), make(running), make(sums),
        make(np.concatenate([spread, spread], axis=0)), make(np.concatenate([widen] * 3, axis=0)),
    )


def per_pair(row, pairs):
    spots = row.shape[1]
    wide = jnp.broadcast_to(row, (pairs, spots))
    r = lax.broadcasted_iota(jnp.int32, (pairs, spots), 0)
    c = lax.broadcasted_iota(jnp.int32, (pairs, spots), 1)
    even = jnp.sum(jnp.where(c == 2 * r, wide, 0.0), axis=1, keepdims=True)
    odd = jnp.sum(jnp.where(c == 2 * r + 1, wide, 0.0), axis=1, keepdims=True)
    low = lax.broadcasted_iota(jnp.int32, (pairs, LANES), 1) < LANES // 2
    return jnp.where(low, even, odd)


def fetch_all(pairs_of, sems, first=0):
    return [pltpu.make_async_copy(src, dst, sems.at[first + i]) for i, (src, dst) in enumerate(pairs_of)]


def pack_shift(rows):
    high, low = split(rows, 2)
    return jnp.concatenate([high, low], axis=0)


def unpack_shift(packed):
    wide = packed.astype(F32)
    return wide[:1] + wide[SEGS : SEGS + 1]


def prepare_kernel(
    hidden_ref, wsi_ref, wk_ref, wv_ref, dr_in, df_in, ls_in, shift_in, running_in, sums_in, spread_in, widen_in,
    ir_in, ii_in, permute_in,
    x, w, drive, win, shrunk, base, power, table, shift_rows, permute, spread,
    dr, df, ls, shift, running, sums, widen, ir, ii, zoh,
    in_sem, w_sem, x_send, x_recv,
):
    tp = lax.axis_index("tp")
    other = 1 - tp
    pairs = drive.shape[0]
    groups = 2 * pairs
    rows = win.shape[0]
    length = rows // SEGS
    pairs_tile = LANES // GROUP_CH // 2
    barrier = pltpu.get_barrier_semaphore()
    pl.semaphore_signal(barrier, inc=1, device_id={"tp": other}, device_id_type=MESH)
    own_x = pltpu.make_async_copy(hidden_ref, x.at[tp], in_sem.at[0])
    own_x.start()
    small = fetch_all((
        (dr_in, dr), (df_in, df), (ls_in, ls), (shift_in, shift), (running_in, running), (sums_in, sums),
        (spread_in, spread), (widen_in, widen), (ir_in, ir), (ii_in, ii), (permute_in, permute),
    ), in_sem, 1)
    for copy in small:
        copy.start()
    columns = [
        (ref.at[:, pl.ds(c * TILE, TILE)], w.at[i + c])
        for ref, i in ((wsi_ref, 0), (wk_ref, 2), (wv_ref, 3)) for c in range(ref.shape[1] // TILE)
    ]
    weights = fetch_all(columns, w_sem)
    for copy in weights:
        copy.start(priority=1)
    zero = jnp.zeros((LANES, TILE), BF16)
    for q in range(pairs):
        drive[q] = zero

    pl.semaphore_wait(barrier, 1)
    own_x.wait()
    swap = pltpu.make_async_remote_copy(
        src_ref=x.at[tp], dst_ref=x.at[tp], send_sem=x_send, recv_sem=x_recv,
        device_id={"tp": other}, device_id_type=MESH,
    )
    swap.start()

    for copy in small[:7]:
        copy.wait()
    two = lambda ref: jnp.concatenate(
        [ref[pl.ds(0, pairs, stride=2), :], ref[pl.ds(1, pairs, stride=2), :]], axis=1
    )
    decay, frequency = two(dr), two(df)
    stepsize = jnp.exp(per_pair(ls[...], pairs))
    magnitude = jnp.exp(decay * stepsize)
    rotation = frequency * stepsize
    base_r, base_i = magnitude * jnp.cos(rotation), magnitude * jnp.sin(rotation)
    denominator = decay * decay + frequency * frequency
    less = base_r - 1.0
    zoh[0] = (less * decay + base_i * frequency) / denominator
    zoh[1] = (base_i * decay - less * frequency) / denominator
    base[0], base[1] = base_r, base_i
    power_r, power_i = base_r, base_i
    for _ in range(length.bit_length() - 1):
        power_r, power_i = cmul(power_r, power_i, power_r, power_i)
    for d in range(4):
        base[2 + 2 * d], base[3 + 2 * d] = power_r, power_i
        if d == 0:
            step_r, step_i = power_r, power_i
        power_r, power_i = cmul(power_r, power_i, power_r, power_i)
    run_r, run_i = jnp.ones_like(base_r), jnp.zeros_like(base_r)
    for k in range(SEGS):
        spot = pl.ds(k, pairs, stride=SEGS)
        power[0, spot, :] = run_r
        power[1, spot, :] = run_i
        run_r, run_i = cmul(run_r, run_i, step_r, step_i)

    shifts = split(shift[...], 3)
    relative = sum(ntdot(running[...], piece) for piece in shifts)
    totals = sum(ntdot(sums[...], piece) for piece in shifts)
    grown = jnp.concatenate(split(jnp.exp(-relative), 2), axis=1)
    shrunk[...] = jnp.concatenate(split(jnp.exp(relative), 2), axis=1)
    win[...] = ndot(grown, spread[...])
    shift_rows[...] = jnp.concatenate(
        [totals[ALL * SEGS : (ALL + 1) * SEGS], jnp.zeros((SEGS, LANES - groups), F32)], axis=1
    )
    scales = jnp.concatenate(split(jnp.exp(totals), 3), axis=1)
    for copy in small[7:]:
        copy.wait()
    table[...] = ndot(scales, widen[...])

    row_low = lax.broadcasted_iota(jnp.int32, (2 * GROUP_CH, LANES), 0) < GROUP_CH
    lane_low = lax.broadcasted_iota(jnp.int32, (2 * GROUP_CH, LANES), 1) < LANES // 2
    own_lane = row_low == lane_low
    for q in range(pairs):
        pick = lambda ref: jnp.concatenate([
            jnp.concatenate([ref[2 * q], ref[2 * q]], axis=1),
            jnp.concatenate([ref[2 * q + 1], ref[2 * q + 1]], axis=1),
        ], axis=0)
        spot = pl.ds((q % pairs_tile) * 2 * GROUP_CH, 2 * GROUP_CH)
        in_r, in_i = pick(ir), pick(ii)
        z_r, z_i = zoh[0, q : q + 1, :], zoh[1, q : q + 1, :]
        d_r, d_i = cmul(z_r, z_i, in_r, in_i)
        drive[q, spot, :] = jnp.concatenate(
            [jnp.where(own_lane, d_r, 0.0), jnp.where(own_lane, d_i, 0.0)], axis=1
        ).astype(BF16)
    swap.wait()
    for copy in weights:
        copy.wait()


def layer_kernel(
    x, w, drive, win, shrunk, base, power, table, shift_rows, permute, spread,
    wq_ref, wg_ref, wsg_ref, sink_in, how_ref, sow_ref, back_in, or_in, oi_in, skip_in,
    acc, state_x, sow_x, head_x, how_x,
    w2, how, sow, back, sink_ref, orr, oi, skip, readout, wout, skip_row,
    pushed, states_ref, u_ref, gate_ref, carried, before, entry, init,
    proj, keys, values, mixed, head, state, near, far,
    in_sem, w_sem, near_send, near_recv, far_send, first_send, far_recv, halo_send, halo_recv, x_send, x_recv,
):
    tp = lax.axis_index("tp")
    other = 1 - tp
    me = lax.axis_index("sp")
    count = lax.axis_size("sp")
    inner, outer = near.shape[0], far.shape[0]
    mine, plane = lax.rem(me, inner), lax.div(me, inner)
    rows, half_width = x.shape[1:]
    pairs = drive.shape[0]
    groups = 2 * pairs
    length = rows // SEGS
    per_tile = LANES // GROUP_CH
    tiles = groups // per_tile
    pairs_tile = per_tile // 2

    barrier = pltpu.get_barrier_semaphore()
    for hop in range(1, inner):
        target = plane * inner + lax.rem(mine + hop, inner)
        pl.semaphore_signal(barrier, inc=1, device_id={"sp": target}, device_id_type=MESH)

    @pl.when(me > 0)
    def _():
        for hop in range(1, outer):
            target = lax.rem(plane + hop, outer) * inner + mine
            target = jnp.where(target == 0, 2, target)
            pl.semaphore_signal(barrier, inc=1, device_id={"sp": target}, device_id_type=MESH)
        pl.semaphore_signal(barrier, inc=1, device_id={"sp": me - 1}, device_id_type=MESH)

    pl.semaphore_signal(barrier, inc=1, device_id={"tp": other}, device_id_type=MESH)

    pieces, _, step = acc.shape
    width = pieces * step
    half_of = lambda ref, owner: ref.at[:, pl.ds(pl.multiple_of(owner * width, LANES), width)]
    small = fetch_all((
        (sink_in, sink_ref), (or_in, orr), (oi_in, oi), (skip_in, skip), (back_in, back),
        (half_of(how_ref, tp), how), (half_of(sow_ref, tp), sow),
    ), in_sem)
    columns = [
        (ref.at[:, pl.ds(c * TILE, TILE)], w2.at[2 * i + c])
        for i, ref in enumerate((wq_ref, wg_ref, wsg_ref)) for c in range(2)
    ]
    weights = fetch_all(columns, w_sem)
    for copy in small[:5] + weights + small[5:]:
        copy.start()

    def cross(k, src, dst):
        return pltpu.make_async_remote_copy(
            src_ref=src, dst_ref=dst, send_sem=x_send.at[k], recv_sem=x_recv.at[k],
            device_id={"tp": other}, device_id_type=MESH,
        )

    crossing = [cross(0, half_of(how_ref, other), how_x), cross(1, half_of(sow_ref, other), sow_x)]
    head_cross, state_cross = cross(2, head, head_x), cross(3, state, state_x)

    def project(block):
        return (ndot(x[0], block[:half_width, :]) + ndot(x[1], block[half_width:, :])).astype(BF16)

    own_rows = pl.ds(WINDOW, rows)
    keys[own_rows, :] = project(w[2])
    values[own_rows, :] = project(w[3])
    fed = [project(w[c]) for c in range(2)]

    def halos(target):
        return [
            pltpu.make_async_remote_copy(
                src_ref=band.at[pl.ds(rows, WINDOW)], dst_ref=band.at[pl.ds(0, WINDOW)],
                send_sem=halo_send.at[k], recv_sem=halo_recv.at[k],
                device_id={"sp": target}, device_id_type=MESH,
            )
            for k, band in enumerate((keys, values))
        ]

    signals = inner + jnp.where(me < count - 1, 1, 0) + jnp.where(me > 0, outer - 2, 0)
    signals = signals + jnp.where(mine > 0, 1, 0) + jnp.where(me == 2, outer - 1, 0)

    def send_halos():
        @pl.when(me < count - 1)
        def _():
            for copy in halos(me + 1):
                copy.start()

    us = [ndot(permute[...], part) for part in fed]
    for c in range(2):
        lanes = pl.ds(c * TILE, TILE)
        u_ref[:, lanes] = us[c].astype(BF16)
        weighted = (us[c] * win[:, lanes]).astype(BF16)
        for t in range(TILE // LANES):
            tile = c * (TILE // LANES) + t
            part = weighted[:, t * LANES : (t + 1) * LANES]
            for i in range(pairs_tile):
                q = tile * pairs_tile + i
                pushed[q] = ndot(part, drive[q])

    bunch = 8

    def wide(ref, index, q):
        return jnp.broadcast_to(ref[index, q : q + 1, :], (SEGS, LANES))

    def scan(first, start, keep):
        br = [wide(base, 0, first + i) for i in range(bunch)]
        bi = [wide(base, 1, first + i) for i in range(bunch)]

        def steps(jj, carry):
            carry = list(carry)
            kept = [[] for _ in range(2 * bunch)]
            for sub in range(2):
                spot = pl.ds(pl.multiple_of((2 * jj + sub) * SEGS, SEGS), SEGS)
                for i in range(bunch):
                    r, m = carry[2 * i], carry[2 * i + 1]
                    p = pushed[first + i, spot, :]
                    new_r = br[i] * r - bi[i] * m + p[:, :LANES]
                    new_m = br[i] * m + bi[i] * r + p[:, LANES:]
                    carry[2 * i], carry[2 * i + 1] = new_r, new_m
                    kept[2 * i].append(new_r)
                    kept[2 * i + 1].append(new_m)
            if keep:
                spot = pl.ds(pl.multiple_of(jj * 2 * SEGS, 2 * SEGS), 2 * SEGS)
                for i in range(bunch):
                    for part in range(2):
                        value = jnp.concatenate(kept[2 * i + part], axis=0).astype(BF16)
                        states_ref[first + i, spot, pl.ds(part * LANES, LANES)] = value
            return tuple(carry)

        return lax.fori_loop(0, length // 2, steps, tuple(start), unroll=2 if keep else 4)

    def row(kind, q):
        return table[kind * SEGS : (kind + 1) * SEGS, q * LANES : (q + 1) * LANES]

    sub = lax.broadcasted_iota(jnp.int32, (SEGS, LANES), 0)
    near_me = near.at[mine]
    near_me[2 * pairs :, :] = pack_shift(shift_rows[...])
    for first in range(0, pairs, bunch):
        ends = scan(first, [jnp.zeros((SEGS, LANES), F32)] * (2 * bunch), False)
        for i in range(bunch):
            q = first + i
            fin = row(FIN, q)
            h_r, h_i = ends[2 * i] * fin, ends[2 * i + 1] * fin
            for d, kind in enumerate((ONE, TWO, FOUR)):
                hop = 1 << d
                weight = jnp.where(sub >= hop, row(kind, q), 0.0)
                a_r, a_i = cmul(
                    pltpu.roll(h_r, hop, 0), pltpu.roll(h_i, hop, 0),
                    wide(base, 2 + 2 * d, q), wide(base, 3 + 2 * d, q),
                )
                h_r, h_i = h_r + weight * a_r, h_i + weight * a_i
            carried[0, q : q + 1, :] = h_r[SEGS - 1 :]
            carried[1, q : q + 1, :] = h_i[SEGS - 1 :]
            ref = row(REF, q)
            entry[0, q] = jnp.where(sub >= 1, pltpu.roll(h_r, 1, 0), 0.0) * ref
            entry[1, q] = jnp.where(sub >= 1, pltpu.roll(h_i, 1, 0), 0.0) * ref

    blocks = rows // WINDOW
    group_size = Q_HEADS // KV_HEADS
    tile_heads = TILE // HEAD_DIM
    q_index = lax.broadcasted_iota(jnp.int32, (WINDOW, 2 * WINDOW), 0)
    k_index = lax.broadcasted_iota(jnp.int32, (WINDOW, 2 * WINDOW), 1)
    distance = WINDOW + q_index - k_index
    in_window = (distance >= 0) & (distance < WINDOW)

    def attend(block):
        here = pl.ds(block * WINDOW, WINDOW)
        band = pl.ds(block * WINDOW, 2 * WINDOW)
        allowed = in_window
        if block == 0:
            allowed = allowed & (k_index >= jnp.where(me == 0, WINDOW, 0))
        key, value = keys[band, :], values[band, :]
        for tile in range(2):
            query = proj[tile, here, :] * jnp.asarray(HEAD_DIM ** -0.5, BF16)
            results = []
            for j in range(tile_heads):
                head_id = tile * tile_heads + j
                kv = head_id // group_size
                k = key[:, kv * HEAD_DIM : (kv + 1) * HEAD_DIM]
                v = value[:, kv * HEAD_DIM : (kv + 1) * HEAD_DIM]
                scores = ntdot(query[:, j * HEAD_DIM : (j + 1) * HEAD_DIM], k)
                scores = jnp.where(allowed, scores, NEG_FILL)
                sink = sink_ref[head_id]
                maxima = jnp.maximum(jnp.max(scores, axis=-1, keepdims=True), sink)
                exponent = jnp.exp(scores - maxima)
                total = jnp.sum(exponent, axis=-1, keepdims=True) + jnp.exp(sink - maxima)
                results.append(ndot(exponent.astype(BF16), v) * (1.0 / total))
            gate = jax.nn.sigmoid(proj[2 + tile, here, :].astype(F32))
            head[here, pl.ds(tile * TILE, TILE)] = (gate * jnp.concatenate(results, axis=1)).astype(BF16)

    def last_part():
        for copy in weights[4:]:
            copy.wait()
        gates = [project(w2[4 + c]) for c in range(2)]
        for c in range(2):
            gate_ref[:, c * TILE : (c + 1) * TILE] = ndot(permute[...], gates[c]).astype(BF16)

    @pl.when(me == 0)
    def _():
        keys[:WINDOW, :] = jnp.zeros((WINDOW, keys.shape[1]), BF16)
        values[:WINDOW, :] = jnp.zeros((WINDOW, values.shape[1]), BF16)

    near_me[:pairs, :] = carried[0].astype(BF16)
    near_me[pairs : 2 * pairs, :] = carried[1].astype(BF16)

    def to_near(target):
        return pltpu.make_async_remote_copy(
            src_ref=near_me, dst_ref=near_me, send_sem=near_send.at[target], recv_sem=near_recv.at[mine],
            device_id={"sp": plane * inner + target}, device_id_type=MESH,
        )

    def from_near(source):
        return pltpu.make_async_remote_copy(
            src_ref=near_me, dst_ref=near.at[source], send_sem=near_send.at[source], recv_sem=near_recv.at[source],
            device_id={"sp": plane * inner + source}, device_id_type=MESH,
        )

    pl.semaphore_wait(barrier, signals)
    for hop in range(1, inner):
        to_near(lax.rem(mine + hop, inner)).start()

    crowded = mine == inner - 1
    pl.when(jnp.logical_not(crowded))(send_halos)
    for copy in weights[:4] + small[:1]:
        copy.wait()
    for n in range(4):
        proj[n] = project(w2[n])
    pl.when(crowded)(send_halos)
    for block in range(1, blocks):
        attend(block)

    for copy in small[1:4]:
        copy.wait()
    wout[...] = ndot(shrunk[...], spread[...])
    lanes_of = lax.broadcasted_iota(jnp.int32, (GROUP_CH, groups * GROUP_CH), 1) % GROUP_CH
    channel = lax.broadcasted_iota(jnp.int32, (GROUP_CH, groups * GROUP_CH), 0)
    skips = sum(ndot(piece, spread[:groups, :]) for piece in split(skip[...], 3))
    skip_row[...] = jnp.broadcast_to(
        jnp.sum(jnp.where(lanes_of == channel, skips, 0.0), axis=0, keepdims=True), skip_row.shape
    )
    row_low = lax.broadcasted_iota(jnp.int32, (2 * GROUP_CH, LANES), 0) < GROUP_CH
    lane_low = lax.broadcasted_iota(jnp.int32, (2 * GROUP_CH, LANES), 1) < LANES // 2
    own_lane = row_low == lane_low
    zero = jnp.zeros((LANES, TILE), BF16)
    for q in range(pairs):
        pick = lambda ref: jnp.concatenate([
            jnp.concatenate([ref[2 * q], ref[2 * q]], axis=1),
            jnp.concatenate([ref[2 * q + 1], ref[2 * q + 1]], axis=1),
        ], axis=0)
        readout[q] = zero
        readout[q, pl.ds((q % pairs_tile) * 2 * GROUP_CH, 2 * GROUP_CH), :] = jnp.concatenate(
            [jnp.where(own_lane, pick(orr), 0.0), jnp.where(own_lane, -pick(oi), 0.0)], axis=1
        ).astype(BF16)

    def near_arrive():
        for hop in range(1, inner):
            from_near(lax.rem(mine + hop, inner)).wait_recv()

    far_me = far.at[plane]

    @pl.when(me == 0)
    def _():
        before[...] = jnp.zeros(before.shape, F32)

    @pl.when(me > 0)
    def _():
        near_arrive()

        block_r, block_i = base[8], base[9]
        agg_r = agg_i = jnp.zeros((pairs, LANES), F32)
        agg_s = jnp.zeros((1, LANES), F32)
        pw_r, pw_i = jnp.ones((pairs, LANES), F32), jnp.zeros((pairs, LANES), F32)
        pre = [agg_r, agg_i, agg_s, pw_r, pw_i]
        for i in range(inner):
            now = [agg_r, agg_i, agg_s, pw_r, pw_i]
            if i > 0:
                pre = [jnp.where(mine == i, a, b) for a, b in zip(now, pre)]
            shift_i = unpack_shift(near[i, 2 * pairs :, :])
            a_r, a_i = cmul(agg_r, agg_i, block_r, block_i)
            factor = jnp.exp(per_pair(shift_i, pairs))
            agg_r = factor * a_r + near[i, :pairs, :].astype(F32)
            agg_i = factor * a_i + near[i, pairs : 2 * pairs, :].astype(F32)
            agg_s = agg_s + shift_i
            pw_r, pw_i = cmul(pw_r, pw_i, block_r, block_i)
        far_me[:pairs, :] = agg_r.astype(BF16)
        far_me[pairs : 2 * pairs, :] = agg_i.astype(BF16)
        far_me[2 * pairs :, :] = pack_shift(jnp.broadcast_to(agg_s, (SEGS, LANES)))
        scale = jnp.exp(per_pair(pre[2], pairs))
        for k, value in enumerate((pre[0], pre[1], scale * pre[3], scale * pre[4], pw_r, pw_i)):
            before[k] = value

    def to_far(target, place, sem):
        return pltpu.make_async_remote_copy(
            src_ref=far_me, dst_ref=far_me, send_sem=sem.at[target], recv_sem=far_recv.at[plane],
            device_id={"sp": target * inner + place}, device_id_type=MESH,
        )

    def far_sends(act):
        for target in range(1, outer):
            @pl.when(me == 2)
            def _():
                act(to_far(target, 0, first_send))

            @pl.when((plane < target) & (me > 0))
            def _():
                act(to_far(target, mine, far_send))

    def from_far(source):
        return pltpu.make_async_remote_copy(
            src_ref=far_me, dst_ref=far.at[source], send_sem=far_send.at[source], recv_sem=far_recv.at[source],
            device_id={"sp": source * inner + mine}, device_id_type=MESH,
        )

    for q in range(pairs):
        spot = pl.ds(q * SEGS, SEGS)
        scale = row(PRE, q) * row(REF, q)
        init[0, q] = power[0, spot, :] * scale
        init[1, q] = power[1, spot, :] * scale

    far_sends(lambda copy: copy.start())
    for copy in crossing:
        copy.start()

    last_part()

    def first_block():
        @pl.when(me > 0)
        def _():
            for copy in halos(me):
                copy.wait_recv()

        attend(0)

    def head_out():
        head_cross.start()
        for piece in range(pieces):
            acc[piece] = ndot(head[...], how[:, part_of(piece)])

    for copy in small[4:]:
        copy.wait()
    part_of = lambda piece: pl.ds(piece * step, step)

    soon = halo_comes_soon(me)

    @pl.when(soon)
    def _():
        first_block()
        head_out()

    carry_r = carry_i = jnp.zeros((pairs, LANES), F32)
    for z in range(outer - 1):
        @pl.when(z < plane)
        def _():
            from_far(z).wait_recv()

    for z in range(outer - 1):
        factor = jnp.exp(per_pair(unpack_shift(far[z, 2 * pairs :, :]), pairs))
        a_r, a_i = cmul(carry_r, carry_i, before[4], before[5])
        carry_r = jnp.where(z < plane, factor * a_r + far[z, :pairs, :].astype(F32), carry_r)
        carry_i = jnp.where(z < plane, factor * a_i + far[z, pairs : 2 * pairs, :].astype(F32), carry_i)
    in_r, in_i = cmul(carry_r, carry_i, before[2], before[3])
    carried[0], carried[1] = in_r + before[0], in_i + before[1]
    for first in range(0, pairs, bunch):
        start = []
        for i in range(bunch):
            q = first + i
            s_r, s_i = cmul(init[0, q], init[1, q], wide(carried, 0, q), wide(carried, 1, q))
            start += [entry[0, q] + s_r, entry[1, q] + s_i]
        scan(first, start, True)
    for tile in range(tiles):
        lanes = pl.ds(tile * LANES, LANES)
        seen = sum(
            ntdot(states_ref[q], readout[q]) for q in range(tile * pairs_tile, (tile + 1) * pairs_tile)
        )
        recurrent = wout[:, lanes] * seen + skip_row[:1, lanes] * u_ref[:, lanes].astype(F32)
        gate = jax.nn.sigmoid(gate_ref[:, lanes].astype(F32))
        mixed[:, lanes] = (gate * jax.nn.gelu(recurrent)).astype(BF16)
    state[...] = ndot(back[...], mixed[...]).astype(BF16)
    state_cross.start()

    @pl.when(jnp.logical_not(soon))
    def _():
        first_block()
        head_out()

    for piece in range(pieces):
        acc[piece] += ndot(state[...], sow[:, part_of(piece)])
    for copy in crossing:
        copy.wait()

    @pl.when(soon)
    def _():
        head_cross.wait()
        for piece in range(pieces):
            acc[piece] += ndot(head_x[...], how_x[:, part_of(piece)])
        state_cross.wait()

    @pl.when(jnp.logical_not(soon))
    def _():
        state_cross.wait()
        for piece in range(pieces):
            acc[piece] += ndot(state_x[...], sow_x[:, part_of(piece)])
        head_cross.wait()

    pl.when(me == 0)(near_arrive)
    for hop in range(1, inner):
        to_near(lax.rem(mine + hop, inner)).wait_send()
    far_sends(lambda copy: copy.wait_send())

    @pl.when(me < count - 1)
    def _():
        for copy in halos(me + 1):
            copy.wait_send()


def halo_comes_soon(me):
    return (lax.rem(me, 2) == 1) | (me == 0)


def close_kernel(acc, state_x, sow_x, head_x, how_x, out_ref, stage, sem):
    pieces, _, step = acc.shape
    copies = [
        pltpu.make_async_copy(stage.at[piece], out_ref.at[:, pl.ds(piece * step, step)], sem.at[piece])
        for piece in range(pieces)
    ]

    def close(gated, weight):
        for piece in range(pieces):
            stage[piece] = (acc[piece] + ndot(gated[...], weight[:, pl.ds(piece * step, step)])).astype(BF16)
            copies[piece].start()

    soon = halo_comes_soon(lax.axis_index("sp"))
    pl.when(soon)(lambda: close(state_x, sow_x))
    pl.when(jnp.logical_not(soon))(lambda: close(head_x, how_x))
    for copy in copies:
        copy.wait()


def on_device(
    hidden, query_weight, key_weight, value_weight, head_gate_weight, state_in_weight, state_gate_weight,
    sink_logit, decay_real, decay_frequency, log_step, input_real, input_imaginary, output_real,
    output_imaginary, skip_weight, decay_shift, head_out_weight, state_out_weight,
):
    rows, half = hidden.shape
    groups, states = decay_real.shape
    pairs = groups // 2
    channels = groups * GROUP_CH
    count = lax.axis_size("sp")
    inner = 1 << (count.bit_length() // 2)
    outer = count // inner
    permute, back, running, sums, spread, widen = constants(rows, groups, states)
    width = head_out_weight.shape[1] // 2
    pieces = 4
    like = lambda v: pltpu.VMEM(v.shape, v.dtype)
    pin = lambda v: pltpu.with_memory_space_constraint(v, pltpu.HBM)
    shaped = jax.ShapeDtypeStruct
    dma = pltpu.SemaphoreType.DMA
    mib = 1024 * 1024
    small = (
        decay_real, decay_frequency, log_step.reshape(1, groups), decay_shift, running, sums, spread, widen,
        input_real.transpose(0, 2, 1), input_imaginary.transpose(0, 2, 1), permute,
    )
    late = (output_real, output_imaginary, skip_weight.T)
    first_tiles = (state_in_weight.shape[1] + key_weight.shape[1] + value_weight.shape[1]) // TILE
    prepared = (
        shaped((2, rows, half), BF16),
        shaped((first_tiles, 2 * half, TILE), BF16),
        shaped((pairs, LANES, TILE), BF16),
        shaped((rows, channels), F32),
        shaped((rows, 2 * groups), BF16),
        shaped((10, pairs, LANES), F32),
        shaped((2, pairs * SEGS, LANES), F32),
        shaped((7 * SEGS, groups * states), F32),
        shaped((SEGS, LANES), F32),
        shaped(permute.shape, BF16),
        shaped(spread.shape, BF16),
    )
    ready = pl.pallas_call(
        prepare_kernel,
        out_shape=prepared,
        in_specs=[ANY] * (4 + len(small)),
        out_specs=(VMEM,) * len(prepared),
        scratch_shapes=[
            *[like(v) for v in small if v is not permute and v is not spread],
            pltpu.VMEM((2, pairs, LANES), F32),
            dma((1 + len(small),)), dma((first_tiles,)), dma, dma,
        ],
        compiler_params=pltpu.CompilerParams(
            vmem_limit_bytes=PREP_MIB * mib, collective_id=0, has_side_effects=True
        ),
        name="prepare",
    )(*map(pin, (hidden, state_in_weight, key_weight, value_weight, *small)))
    closing = pl.pallas_call(
        layer_kernel,
        out_shape=(
            shaped((pieces, rows, width // pieces), F32),
            shaped((rows, channels), BF16),
            shaped((state_out_weight.shape[0], width), BF16),
            shaped((rows, head_out_weight.shape[0]), BF16),
            shaped((head_out_weight.shape[0], width), BF16),
        ),
        in_specs=[VMEM] * len(prepared) + [ANY] * (7 + len(late)),
        out_specs=(VMEM,) * 5,
        scratch_shapes=[
            pltpu.VMEM((6, 2 * half, TILE), BF16),
            *[pltpu.VMEM((head_out_weight.shape[0], width), BF16)] * 2,
            like(back),
            pltpu.SMEM(sink_logit.shape, F32),
            *[like(v) for v in late],
            pltpu.VMEM((pairs, LANES, TILE), BF16),
            pltpu.VMEM((rows, channels), F32),
            pltpu.VMEM((SEGS, channels), F32),
            pltpu.VMEM((pairs, rows, TILE), F32),
            pltpu.VMEM((pairs, rows, TILE), BF16),
            pltpu.VMEM((rows, channels), BF16),
            pltpu.VMEM((rows, channels), BF16),
            pltpu.VMEM((2, pairs, LANES), F32),
            pltpu.VMEM((6, pairs, LANES), F32),
            pltpu.VMEM((2, pairs, SEGS, LANES), F32),
            pltpu.VMEM((2, pairs, SEGS, LANES), F32),
            pltpu.VMEM((4, rows, TILE), BF16),
            pltpu.VMEM((WINDOW + rows, TILE), BF16),
            pltpu.VMEM((WINDOW + rows, TILE), BF16),
            *[pltpu.VMEM((rows, channels), BF16)] * 3,
            pltpu.VMEM((inner, 2 * pairs + 2 * SEGS, LANES), BF16),
            pltpu.VMEM((outer, 2 * pairs + 2 * SEGS, LANES), BF16),
            dma((7,)), dma((6,)), dma((inner,)), dma((inner,)), *[dma((outer,))] * 3,
            dma((2,)), dma((2,)), dma((4,)), dma((4,)),
        ],
        compiler_params=pltpu.CompilerParams(
            vmem_limit_bytes=LAYER_MIB * mib, collective_id=1, has_side_effects=True
        ),
        name="layer",
    )(
        *ready,
        *map(pin, (
            query_weight, head_gate_weight, state_gate_weight, sink_logit, head_out_weight, state_out_weight,
            back, *late,
        )),
    )
    return pl.pallas_call(
        close_kernel,
        out_shape=shaped((rows, width), BF16),
        in_specs=[VMEM] * 5,
        out_specs=ANY,
        scratch_shapes=[pltpu.VMEM((pieces, rows, width // pieces), BF16), dma((pieces,))],
        compiler_params=pltpu.CompilerParams(vmem_limit_bytes=CLOSE_MIB * mib),
        name="close",
    )(*closing)


def solution(mesh):
    in_specs = (
        P("sp", "tp"),
        P(None, "tp"),
        P(None, "tp"),
        P(None, "tp"),
        P(None, "tp"),
        P(None, "tp"),
        P(None, "tp"),
        P("tp"),
        P("tp", None),
        P("tp", None),
        P("tp"),
        P("tp", None, None),
        P("tp", None, None),
        P("tp", None, None),
        P("tp", None, None),
        P("tp", None),
        P("tp", "sp"),
        P("tp", None),
        P("tp", None),
    )
    out_specs = P("sp", "tp")
    return jax.shard_map(
        on_device, mesh=mesh, in_specs=in_specs, out_specs=out_specs, check_vma=False
    )
```
